512 devices in a mesh: ep: 128 (over z, x, core), tp: 4 (over y).
Axes of the slice: x: 4, y: 4, z: 16, core: 2. Of those that a mesh axis runs over, the one named last changes fastest.
Arguments:
- hidden_in: bfloat16 [2048, 2048], P('ep'), may hold values from -6 to 6
- state_in: float32 [2048, 16, 64, 64], P('ep', 'tp'), may hold values from -6 to 6
- receptance: bfloat16 [2048, 1024], P('ep', 'tp'), may hold values from -6 to 6
- key_in: bfloat16 [2048, 1024], P('ep', 'tp'), may hold values from -1.5 to 1.5
- value_in: bfloat16 [2048, 1024], P('ep', 'tp'), may hold values from -6 to 6
- learn_in: bfloat16 [2048, 1024], P('ep', 'tp'), may hold values from -8 to 8
- decay_in: float32 [2048, 1024], P('ep', 'tp'), may hold values from -6 to 6
- decay_base: float32 [1024], P('tp'), may hold values from -3 to 1
- norm_gain: float32 [1024], P('tp'), may hold values from 0.1 to 1.9
- out_weight: bfloat16 [1024, 2048], P('tp'), may hold values from -0.1875 to 0.1875
- routed_gain: float32 [2048], replicated, may hold values from 0.1 to 1.9
- expert_gate: bfloat16 [128, 2048, 512], P('ep', None, 'tp'), may hold values from -0.125 to 0.125
- expert_up: bfloat16 [128, 2048, 512], P('ep', None, 'tp'), may hold values from -0.125 to 0.125
- expert_down: bfloat16 [128, 512, 2048], P('ep', 'tp'), may hold values from -0.25 to 0.25
- route_ids: int32 [2048, 6], P('ep'), may hold values from 0 to 127, all different within a row; in each aligned block of 16 rows (0 to 15, 16 to 31, ...) at most 2 rows name the same one
- route_weights: float32 [2048, 6], P('ep'), may hold values from 0.05 to 0.5
Outputs:
- hidden_out: bfloat16 [2048, 2048], P('ep')
- state_out: float32 [2048, 16, 64, 64], P('ep', 'tp')
The draws below stay inside these ranges and needn't reach their ends.
Inputs may be any that keep to these rules, and one draw needn't show every extreme that they name: `route_ids`: each row names 6 different experts. Among the rows of one index of ep no expert is named more than 2 times, a bound that some block reaches.
All inputs are finite; a program needn't handle non-finite values.
Results may differ from the reference program's by a relative error of at most 0.014.
Values may be sent and summed in bfloat16 or wider, within the bound.
No kernel may reach another device: no remote copies, remote signals or barrier semaphores. Data moves between devices by JAX's collectives and lax.ppermute only.
A program may use at most 128 MiB of HBM per device.

```python
import math
import jax
import jax.numpy as jnp
import numpy as np
from jax import lax

D = 2048
HEADS = 16
HEAD_DIM = 64
RD = 1024
FF = 512
EXPERTS = 128
TOP_K = 6
SEQ_DEV = 16
SEQS = 2048
CAP = 2
N_EP = 128
N_TP = 4


def level_of(own_key, dims, shards, low, largest):
    loudness, own = 1.0, jax.random.fold_in(own_key, 6)
    for dim, shards_of in shards:
        draws = jnp.exp(jax.random.uniform(jax.random.fold_in(own, dim), (shards_of,), jnp.float32, low / len(shards), largest / len(shards)))
        loudness = loudness * jnp.repeat(draws, dims[dim] // shards_of).reshape([-1 if axis == dim else 1 for axis in range(len(dims))])
    return loudness


def assign_block(rng, own, number, rows, number_of, top, most, lean):
    sequence = jax.random.permutation(rng, number_of)
    packed, ordinary = shares(number_of, rows * top, most, lean, True), shares(number_of, rows * top, most, lean, False)
    places = jnp.arange(number_of)

    def named(tallies, rotation):
        used = int((tallies > 0).sum())
        fixed = max(1, used // 4)
        shifted = fixed + (places - fixed + rotation * (used - fixed)) % max(1, number_of - fixed)
        return jnp.zeros((number_of,), jnp.int32).at[sequence[jnp.where(places < fixed, places, shifted)]].set(jnp.asarray(tallies, jnp.int32))

    tallies = jnp.where(number % 4 == 0, named(packed, number // 4), named(ordinary, number - number // 4 - 1))
    mixed = jax.random.permutation(jax.random.fold_in(own, 3), number_of)
    source_of, receiver = mixed[0:number_of // 2 * 2:2], mixed[1:number_of // 2 * 2:2]
    margin = jnp.minimum(tallies[source_of] - 1, most - tallies[receiver]) // 2
    margin = jnp.where((source_of == sequence[0]) | (receiver == sequence[0]) | (tallies[receiver] == 0), 0, jnp.maximum(margin, 0))
    shifted = jax.random.randint(jax.random.fold_in(own, 4), (number_of // 2,), 0, 1 << 20) % (margin + 1)
    tallies = tallies.at[source_of].add(-shifted).at[receiver].add(shifted)
    members = jnp.searchsorted(jnp.cumsum(tallies), jnp.arange(rows * top), side="right").astype(jnp.int32)
    listing = members.reshape(top, rows).T
    listing = listing[jax.random.permutation(jax.random.fold_in(own, 1), rows)]
    rotation = jax.random.randint(jax.random.fold_in(own, 2), (rows, 1), 0, top)
    return jnp.take_along_axis(listing, (jnp.arange(top)[None, :] + rotation) % top, axis=1)


def shares(amount, total, limit, slope, full):
    weights = [(1 << 20) // math.isqrt(grade ** slope) + 1 for grade in range(1, amount + 1)]
    largest = limit if full else min(limit, max(-(-total // amount), total * weights[0] // sum(weights)))
    least = 1 if total - largest >= amount - 1 else 0
    given, rest = [largest] + [least] * (amount - 1), total - largest - least * (amount - 1)
    while rest > 0:
        candidates = [i for i in range(1, amount) if given[i] < largest] or [i for i in range(1, amount) if given[i] < limit]
        mass, remaining = sum([weights[i] for i in candidates]), rest
        for i in candidates:
            extra = min(limit - given[i], max(1, remaining * weights[i] // mass), rest)
            given[i] = given[i] + extra
            rest = rest - extra
    return np.array(given)


def centred(key, dims, deviation, limit, cuts=(), held_as=jnp.bfloat16):
    values = jax.random.normal(key, dims, jnp.float32) * deviation
    if len(cuts) > 0:
        values = level_of(key, dims, cuts, -0.22, 0.18) * values
    return jnp.clip(values, min=-limit, max=limit).astype(held_as)


def setup_inputs(seed: int = 0) -> dict:
    seeds = jax.random.split(jax.random.key(seed), 17)
    hidden_in = centred(seeds[0], (SEQS, D), 1.0, 6.0, ((0, 128),))
    state_in = centred(seeds[1], (SEQS, HEADS, HEAD_DIM, HEAD_DIM), 1.0, 6.0, ((0, 128), (1, 4)), jnp.float32)
    receptance = centred(seeds[2], (SEQS, RD), 1.0, 6.0, ((0, 128), (1, 4)))
    key_in = centred(seeds[3], (SEQS, RD), 0.25, 1.5, ((0, 128), (1, 4)))
    value_in = centred(seeds[4], (SEQS, RD), 1.0, 6.0, ((0, 128), (1, 4)))
    learn_in = centred(seeds[5], (SEQS, RD), 2.0, 8.0, ((0, 128), (1, 4)))
    decay_in = centred(seeds[6], (SEQS, RD), 1.0, 6.0, ((0, 128), (1, 4)), jnp.float32)
    decay_base = jnp.clip(-3.0 + 4.0 * jax.random.uniform(seeds[7], (RD,), jnp.float32) ** level_of(seeds[7], (RD,), ((0, 4),), -0.2, 0.2), -3.0, 1.0)
    norm_gain = jnp.clip(1.0 + 0.18 * jax.random.normal(seeds[8], (RD,), jnp.float32), 0.1, 1.9)
    out_weight = centred(seeds[9], (RD, D), RD ** -0.5, 0.1875, ((0, 4),))
    routed_gain = jnp.clip(1.0 + 0.18 * jax.random.normal(seeds[10], (D,), jnp.float32), 0.1, 1.9)
    expert_gate = centred(seeds[11], (EXPERTS, D, FF), D ** -0.5, 0.125, ((0, 128), (2, 4)))
    expert_up = centred(seeds[12], (EXPERTS, D, FF), D ** -0.5, 0.125, ((0, 128), (2, 4)))
    expert_down = centred(seeds[13], (EXPERTS, FF, D), FF ** -0.5, 0.25, ((0, 128), (1, 4)))
    route_ids_keys = jax.random.split(jax.random.fold_in(seeds[14], 1), SEQS // SEQ_DEV)
    route_ids_turns = jax.random.permutation(jax.random.fold_in(seeds[14], 3), SEQS // SEQ_DEV)
    route_ids = jax.vmap(lambda own, number: assign_block(jax.random.fold_in(seeds[14], 2), own, number, SEQ_DEV, EXPERTS, TOP_K, CAP, 2))(route_ids_keys, route_ids_turns).reshape((SEQS, TOP_K))
    route_weights = jnp.clip(jnp.exp(math.log(0.5) - 2.3025851 * jax.random.uniform(seeds[15], (SEQS, TOP_K), jnp.float32) ** level_of(seeds[15], (SEQS, TOP_K), ((0, 128),), -0.2, 0.2)), 0.05, 0.5)
    return {"hidden_in": hidden_in, "state_in": state_in, "receptance": receptance, "key_in": key_in, "value_in": value_in, "learn_in": learn_in, "decay_in": decay_in, "decay_base": decay_base, "norm_gain": norm_gain, "out_weight": out_weight, "routed_gain": routed_gain, "expert_gate": expert_gate, "expert_up": expert_up, "expert_down": expert_down, "route_ids": route_ids, "route_weights": route_weights}


EPSILON = 1e-06
GROUP_EPSILON = 0.00064

def heads_update(state_in, receptance, key_in, value_in, learn_in, decay_in, decay_base, norm_gain):
    seq_count = receptance.shape[0]
    head_count = state_in.shape[1]
    head_size = state_in.shape[3]

    def to_heads(values):
        return values.astype(jnp.float32).reshape(seq_count, head_count, head_size)
    reading = to_heads(receptance)
    keys = to_heads(key_in)
    values = to_heads(value_in)
    learning = jax.nn.sigmoid(to_heads(learn_in))
    log_rate = -jax.nn.softplus(-(decay_base[None, :] + decay_in)) - 0.5
    decay = to_heads(jnp.exp(-jnp.exp(log_rate)))
    unit_key = keys * lax.rsqrt(lax.optimization_barrier(jnp.sum(keys * keys, axis=-1, keepdims=True)) + EPSILON)
    carried = jnp.einsum('shij,shj->shi', state_in, unit_key, precision=lax.Precision.HIGHEST)
    new_state = state_in * decay[:, :, None, :] - carried[..., None] * (unit_key * learning)[:, :, None, :] + values[..., None] * keys[:, :, None, :]
    output = jnp.einsum('shij,shj->shi', new_state, reading, precision=lax.Precision.HIGHEST)
    center = lax.optimization_barrier(jnp.mean(output, axis=-1, keepdims=True))
    spread = lax.optimization_barrier(jnp.mean(jnp.square(output - center), axis=-1, keepdims=True))
    gain = norm_gain.astype(jnp.float32).reshape(head_count, head_size)
    normed = (output - center) * lax.rsqrt(spread + GROUP_EPSILON) * gain[None]
    return (normed.reshape(seq_count, head_count * head_size).astype(jnp.bfloat16), new_state)

def expert_rows(rows, gate_weight, up_weight, down_weight):
    gate = jnp.dot(rows, gate_weight, preferred_element_type=jnp.float32)
    upward = jnp.dot(rows, up_weight, preferred_element_type=jnp.float32)
    hidden = (jax.nn.silu(gate) * upward).astype(jnp.bfloat16)
    block = hidden.shape[1] // N_TP
    partial_value = jnp.einsum('bjf,jfd->jbd', hidden.reshape(hidden.shape[0], N_TP, block).astype(jnp.float32), down_weight.reshape(N_TP, block, down_weight.shape[1]).astype(jnp.float32))
    rounded = lax.optimization_barrier(partial_value.astype(jnp.bfloat16)).astype(jnp.float32)
    return lax.optimization_barrier(jnp.sum(rounded, axis=0)).astype(jnp.bfloat16)

def reference(hidden_in, state_in, receptance, key_in, value_in, learn_in, decay_in, decay_base, norm_gain, out_weight, routed_gain, expert_gate, expert_up, expert_down, route_ids, route_weights):
    mixed, new_state = heads_update(state_in, receptance, key_in, value_in, learn_in, decay_in, decay_base, norm_gain)
    seq_total = hidden_in.shape[0]
    block = mixed.shape[1] // N_TP
    partial_value = jnp.einsum('sjg,jgd->jsd', mixed.reshape(seq_total, N_TP, block).astype(jnp.float32), out_weight.reshape(N_TP, block, out_weight.shape[1]).astype(jnp.float32))
    rounded = lax.optimization_barrier(partial_value.astype(jnp.bfloat16)).astype(jnp.float32)
    attention = lax.optimization_barrier(jnp.sum(rounded, axis=0)).astype(jnp.bfloat16)
    residual = hidden_in.astype(jnp.float32) + attention.astype(jnp.float32)
    scale = lax.rsqrt(lax.optimization_barrier(jnp.mean(residual * residual, axis=-1, keepdims=True)) + EPSILON)
    normed = (residual * scale * routed_gain[None, :]).astype(jnp.bfloat16)
    flat_ids = route_ids.reshape(-1).astype(jnp.int32)
    expert_count = expert_gate.shape[0]
    order = jnp.argsort(flat_ids, stable=True).astype(jnp.int32)
    counts = lax.optimization_barrier(jnp.sum((flat_ids[:, None] == jnp.arange(expert_count, dtype=jnp.int32)[None, :]).astype(jnp.int32), axis=0))
    starts = (jnp.cumsum(counts) - counts).astype(jnp.int32)
    window = N_EP * CAP
    padded_order = jnp.concatenate([order, jnp.zeros((window,), jnp.int32)])
    flat_weights = route_weights.reshape(-1)

    def visit(total, expert):
        chosen = lax.dynamic_slice_in_dim(padded_order, starts[expert], window, 0)
        tokens = chosen // TOP_K
        live = jnp.arange(window, dtype=jnp.int32) < counts[expert]
        result = expert_rows(normed[tokens], expert_gate[expert], expert_up[expert], expert_down[expert])
        weight = jnp.where(live, flat_weights[chosen], jnp.zeros_like(flat_weights[chosen]))
        return (total.at[tokens].add(weight[:, None] * result.astype(jnp.float32)), None)
    routed, _ = lax.scan(visit, jnp.zeros_like(residual), jnp.arange(expert_count, dtype=jnp.int32))
    return ((residual + routed).astype(jnp.bfloat16), new_state)
```

```python
import jax
import jax.numpy as jnp
import numpy as np
from jax import lax
from jax.sharding import Mesh, PartitionSpec as P

EPSILON = 1e-06
GROUP_EPSILON = 0.00064
Z_AXES = ("zq", "zp")
NEAR_AXES = ("zp", "x", "c", "y")
EP = ("zq", "zp", "x", "c")


def exchange(pieces, axes):
    return lax.all_to_all(pieces, axes, split_axis=0, concat_axis=0, tiled=True)


def heads_update(state_in, receptance, key_in, value_in, learn_in, decay_in, decay_base, norm_gain):
    seq_count = receptance.shape[0]
    head_count = state_in.shape[1]
    head_size = state_in.shape[3]

    def to_heads(values):
        return values.astype(jnp.float32).reshape(seq_count, head_count, head_size)

    reading = to_heads(receptance)
    keys = to_heads(key_in)
    values = to_heads(value_in)
    learning = jax.nn.sigmoid(to_heads(learn_in))
    log_rate = -jax.nn.softplus(-(decay_base[None, :] + decay_in)) - 0.5
    decay = to_heads(jnp.exp(-jnp.exp(log_rate)))
    unit_key = keys * lax.rsqrt(jnp.sum(keys * keys, axis=-1, keepdims=True) + EPSILON)
    carried = jnp.einsum("shij,shj->shi", state_in, unit_key)
    new_state = (
        state_in * decay[:, :, None, :]
        - carried[..., None] * (unit_key * learning)[:, :, None, :]
        + values[..., None] * keys[:, :, None, :]
    )
    output = jnp.einsum("shij,shj->shi", new_state, reading)
    center = jnp.mean(output, axis=-1, keepdims=True)
    spread = jnp.mean(jnp.square(output - center), axis=-1, keepdims=True)
    gain = norm_gain.reshape(head_count, head_size)
    normed = (output - center) * lax.rsqrt(spread + GROUP_EPSILON) * gain[None]
    return (normed.reshape(seq_count, head_count * head_size).astype(jnp.bfloat16), new_state)


def split_weights(weights):
    high = weights.astype(jnp.bfloat16)
    low = (weights - high.astype(jnp.float32)).astype(jnp.bfloat16)
    return high, low


def selection(routing, first_expert, experts, slots):
    tokens = routing.shape[0]
    senders = lax.axis_size(Z_AXES)
    per_sender = tokens // senders
    wide = routing.astype(jnp.float32)
    named = first_expert + jnp.arange(experts, dtype=jnp.int32)
    ids = wide[:, 0:6].astype(jnp.int32)
    hit = ids[:, :, None] == named[None, None, :]
    member = jnp.any(hit, axis=1).astype(jnp.float32)
    high = jnp.sum(jnp.where(hit, wide[:, 6:12, None], 0.0), axis=1)
    low = jnp.sum(jnp.where(hit, wide[:, 12:18, None], 0.0), axis=1)
    at = np.arange(tokens)
    earlier = (at[:, None] // per_sender == at[None, :] // per_sender) & (at[:, None] < at[None, :])
    rank = jnp.einsum("te,tu->eu", member.astype(jnp.bfloat16), jnp.asarray(earlier, jnp.bfloat16), preferred_element_type=jnp.float32)
    sender = jnp.asarray(at // per_sender, jnp.float32)
    row = jnp.where(member.T > 0, sender[None, :] * slots + rank, -1.0)
    choice = row[:, None, :] == jnp.arange(senders * slots, dtype=jnp.float32)[None, :, None]
    weights = [jnp.where(choice, part.T[:, None, :], 0.0).astype(jnp.bfloat16).reshape(-1, tokens) for part in (high, low)]
    return choice.astype(jnp.bfloat16).reshape(-1, tokens), weights


def on_device(
    hidden_in,
    state_in,
    receptance,
    key_in,
    value_in,
    learn_in,
    decay_in,
    decay_base,
    norm_gain,
    out_weight,
    routed_gain,
    expert_gate,
    expert_up,
    expert_down,
    route_ids,
    route_weights,
):
    bf16, f32 = jnp.bfloat16, jnp.float32
    n_y, n_z, n_zp = lax.axis_size("y"), lax.axis_size(Z_AXES), lax.axis_size("zp")
    near = lax.axis_size(("zp", "x", "c"))
    seqs, width = hidden_in.shape
    quarter = width // n_y
    piece = quarter // n_zp
    slots = 2
    y = lax.axis_index("y")

    mixed, new_state = heads_update(
        state_in, receptance, key_in, value_in, learn_in, decay_in, decay_base, norm_gain
    )
    product = jnp.dot(mixed, out_weight, preferred_element_type=f32).astype(bf16)
    arrived = exchange(jnp.broadcast_to(product, (n_y, seqs, width)), "y")
    attention = arrived.astype(f32).sum(axis=0).astype(bf16)
    residual = hidden_in.astype(f32) + attention.astype(f32)
    scale = lax.rsqrt(jnp.mean(residual * residual, axis=-1, keepdims=True) + EPSILON)
    normed = (residual * scale * routed_gain[None, :]).astype(bf16)
    own = lax.dynamic_slice_in_dim(normed, y * quarter, quarter, 1)
    own_residual = lax.dynamic_slice_in_dim(residual, y * quarter, quarter, 1)

    high, low = split_weights(route_weights)
    routing = jnp.concatenate([route_ids.astype(bf16), high, low], axis=1)
    routing = jnp.pad(routing, ((0, 0), (0, 128 - routing.shape[1])))
    halves = own.reshape(seqs, n_zp, piece).transpose(1, 0, 2)
    parcel = jnp.concatenate([halves, jnp.broadcast_to(routing, (n_zp, seqs, 128))], axis=2)
    parcels = jnp.broadcast_to(parcel, (n_z // n_zp, *parcel.shape)).reshape(n_z, seqs, piece + 128)
    rows = exchange(parcels, Z_AXES).reshape(n_z * seqs, piece + 128)

    choice, (weight_high, weight_low) = selection(rows[:, piece:], lax.axis_index("zq") * near, near, slots)
    chosen = jnp.dot(choice, rows[:, :piece], preferred_element_type=f32).astype(bf16)
    per_expert = n_z * slots
    chosen = chosen.reshape(near, 1, per_expert, piece)
    outgoing = jnp.broadcast_to(chosen, (near, n_y, per_expert, piece)).reshape(near * n_y, per_expert, piece)
    got = exchange(outgoing, NEAR_AXES)

    n_xc = near // n_zp
    flat = got.reshape(n_zp, n_xc, n_y, per_expert, piece).transpose(1, 3, 2, 0, 4).reshape(n_xc * per_expert, width)
    gate = jnp.dot(flat, expert_gate[0], preferred_element_type=f32)
    upward = jnp.dot(flat, expert_up[0], preferred_element_type=f32)
    hidden = (jax.nn.silu(gate) * upward).astype(bf16)
    partial_out = jnp.dot(hidden, expert_down[0], preferred_element_type=f32).astype(bf16)
    back = partial_out.reshape(n_xc, per_expert, n_y, n_zp, piece).transpose(3, 0, 2, 1, 4)
    returned = exchange(back.reshape(near * n_y, per_expert, piece), NEAR_AXES)

    summed = returned.reshape(near, n_y, per_expert, piece).astype(f32).sum(axis=1).astype(bf16)
    summed = summed.reshape(near * per_expert, piece)

    def weighed(weight):
        return lax.dot_general(weight, summed, (((0,), (0,)), ((), ())), preferred_element_type=f32)

    combined = (weighed(weight_high) + weighed(weight_low)).astype(bf16)
    parts = exchange(combined.reshape(n_z, seqs, piece), Z_AXES)
    routed = parts.reshape(n_z // n_zp, n_zp, seqs, piece).astype(f32).sum(axis=0)
    routed = routed.transpose(1, 0, 2).reshape(seqs, quarter)
    result = (own_residual + routed).astype(bf16)
    spread = exchange(jnp.broadcast_to(result, (n_y, seqs, quarter)), "y")
    return (spread.transpose(1, 0, 2).reshape(seqs, width), new_state)


def solution(mesh):
    near_mesh = Mesh(mesh.devices.reshape(8, 2, 4, 2, 4), ("zq", "zp", "x", "c", "y"))
    in_specs = (
        P(EP, None),
        P(EP, "y", None, None),
        P(EP, "y"),
        P(EP, "y"),
        P(EP, "y"),
        P(EP, "y"),
        P(EP, "y"),
        P("y"),
        P("y"),
        P("y", None),
        P(),
        P(EP, None, "y"),
        P(EP, None, "y"),
        P(EP, "y", None),
        P(EP, None),
        P(EP, None),
    )
    out_specs = (P(EP, None), P(EP, "y", None, None))
    return jax.shard_map(
        on_device, mesh=near_mesh, in_specs=in_specs, out_specs=out_specs, check_vma=False
    )
```

```python
import functools
import math
import jax
import jax.numpy as jnp
import numpy as np
from jax import lax
from jax.experimental import pallas as pl
from jax.experimental.pallas import tpu as pltpu
from jax.sharding import Mesh, PartitionSpec as P

EPSILON = 1e-06
GROUP_EPSILON = 0.00064
SEQ_STEP = 4
Z_AXES = ("zq", "zp")
NEAR_AXES = ("zp", "x", "c", "y")
EP = ("zq", "zp", "x", "c")


def exchange(pieces, axes):
    return lax.all_to_all(pieces, axes, split_axis=0, concat_axis=0, tiled=True)


def heads_kernel(
    copies,
    state_ref,
    reading_ref,
    key_ref,
    value_ref,
    learn_ref,
    decay_ref,
    base_ref,
    gain_ref,
    weight_ref,
    new_state_ref,
    out_ref,
    rows,
    values_across,
    read,
):
    f32 = jnp.float32
    step = pl.program_id(0)
    seqs = reading_ref.shape[0]
    per_step, heads, size, _ = state_ref.shape
    lanes = lax.broadcasted_iota(jnp.int32, (size, 128), 1)

    @pl.when(step == 0)
    def _():
        keys = key_ref[...].astype(f32)
        values = value_ref[...].astype(f32)
        learning = jax.nn.sigmoid(learn_ref[...].astype(f32))
        decay = jnp.exp(-math.exp(-0.5) * jax.nn.sigmoid(base_ref[...] + decay_ref[...]))
        reading = reading_ref[...].astype(f32)
        values_across[...] = jnp.zeros_like(values_across)
        read[...] = jnp.zeros_like(read)
        for head in range(heads):
            at = slice(head * size, (head + 1) * size)
            key = keys[:, at]
            unit = key * lax.rsqrt(jnp.sum(key * key, axis=1, keepdims=True) + EPSILON)
            rows[0, head] = unit
            rows[1, head] = decay[:, at]
            rows[2, head] = unit * learning[:, at]
            rows[3, head] = key
            rows[4, head] = reading[:, at]
            values_across[head * seqs : (head + 1) * seqs, 0:size] = values[:, at]
        values_across[...] = values_across[...].T

    shifted = pltpu.roll(values_across[0:size, :], 128 - step * per_step, 1)
    found = jnp.zeros((size, 128), f32)
    for local in range(per_step):
        seq = step * per_step + local
        for head in range(heads):
            column = head * seqs + local
            state = state_ref[local, head]

            def row(which):
                return rows[which, head, pl.ds(seq, 1), :]

            carried = jnp.sum(state * row(0), axis=1, keepdims=True)
            new = (
                state * row(1)
                - carried * row(2)
                + shifted[:, column : column + 1] * row(3)
            )
            new_state_ref[local, head] = new
            found = jnp.where(lanes == column, jnp.sum(new * row(4), axis=1, keepdims=True), found)
    read[0:size, :] += pltpu.roll(found, step * per_step, 1)

    @pl.when(step == pl.num_programs(0) - 1)
    def _():
        output = read[...]
        live = output[0:size]
        center = jnp.mean(live, axis=0, keepdims=True)
        spread = jnp.mean(jnp.square(live - center), axis=0, keepdims=True)
        read[...] = (output - center) * lax.rsqrt(spread + GROUP_EPSILON)
        across = read[...].T
        gain = gain_ref[...]
        mixed = jnp.concatenate(
            [
                across[head * seqs : (head + 1) * seqs, 0:size]
                * gain[:, head * size : (head + 1) * size]
                for head in range(heads)
            ],
            axis=1,
        ).astype(jnp.bfloat16)
        product = jnp.dot(mixed, weight_ref[...], preferred_element_type=f32).astype(jnp.bfloat16)
        for copy in range(copies):
            out_ref[copy] = product


def heads_update(copies, state_in, receptance, key_in, value_in, learn_in, decay_in, decay_base, norm_gain, out_weight):
    seqs, heads, size, _ = state_in.shape
    width = out_weight.shape[1]
    channels = heads * size
    block = pl.BlockSpec((SEQ_STEP, heads, size, size), lambda s: (s, 0, 0, 0))

    def whole(shape):
        return pl.BlockSpec(shape, lambda s: (0,) * len(shape))

    tall = whole((seqs, channels))
    flat = whole((1, channels))
    new_state, product = pl.pallas_call(
        functools.partial(heads_kernel, copies),
        grid=(seqs // SEQ_STEP,),
        in_specs=[block, tall, tall, tall, tall, tall, flat, flat, whole((channels, width))],
        out_specs=[block, whole((copies, seqs, width))],
        out_shape=[
            jax.ShapeDtypeStruct(state_in.shape, jnp.float32),
            jax.ShapeDtypeStruct((copies, seqs, width), jnp.bfloat16),
        ],
        scratch_shapes=[
            pltpu.VMEM((5, heads, seqs, size), jnp.float32),
            pltpu.VMEM((128, 128), jnp.float32),
            pltpu.VMEM((128, 128), jnp.float32),
        ],
        cost_estimate=pl.CostEstimate(flops=20_000_000, bytes_accessed=5_000_000, transcendentals=20_000),
    )(
        state_in,
        receptance,
        key_in,
        value_in,
        learn_in,
        decay_in,
        decay_base.reshape(1, channels),
        norm_gain.reshape(1, channels),
        out_weight,
    )
    return product, new_state


def expert_kernel(got_ref, gate_ref, up_ref, down_ref, out_ref, flat):
    f32 = jnp.float32
    n_zp, n_xc, n_y, rows, piece = got_ref.shape
    total = n_xc * rows
    for y in range(n_y):
        for zp in range(n_zp):
            at = (y * n_zp + zp) * piece
            flat[:, at : at + piece] = got_ref[zp, :, y].reshape(total, piece)
    arrived = flat[...]
    gate = jnp.dot(arrived, gate_ref[0], preferred_element_type=f32)
    upward = jnp.dot(arrived, up_ref[0], preferred_element_type=f32)
    hidden = (gate * jax.nn.sigmoid(gate) * upward).astype(jnp.bfloat16)
    for y in range(n_y):
        for zp in range(n_zp):
            at = (y * n_zp + zp) * piece
            partial = jnp.dot(hidden, down_ref[0, :, at : at + piece], preferred_element_type=f32)
            out_ref[zp, :, y] = partial.astype(jnp.bfloat16).reshape(n_xc, rows, piece)


def experts(got, expert_gate, expert_up, expert_down):
    n_zp, n_xc, n_y, rows, piece = got.shape
    vmem = pl.BlockSpec(memory_space=pltpu.VMEM)
    return pl.pallas_call(
        expert_kernel,
        in_specs=[vmem] * 4,
        out_specs=vmem,
        out_shape=jax.ShapeDtypeStruct(got.shape, jnp.bfloat16),
        scratch_shapes=[pltpu.VMEM((n_xc * rows, n_zp * n_y * piece), jnp.bfloat16)],
        cost_estimate=pl.CostEstimate(flops=400_000_000, bytes_accessed=4_000_000, transcendentals=40_000),
    )(got, expert_gate, expert_up, expert_down)


def split_weights(weights):
    high = weights.astype(jnp.bfloat16)
    low = (weights - high.astype(jnp.float32)).astype(jnp.bfloat16)
    return high, low


def selection(routing, first_expert, experts, slots):
    tokens = routing.shape[0]
    senders = lax.axis_size(Z_AXES)
    per_sender = tokens // senders
    wide = routing.astype(jnp.float32)
    named = first_expert + jnp.arange(experts, dtype=jnp.int32)
    ids = wide[:, 0:6].astype(jnp.int32)
    hit = ids[:, :, None] == named[None, None, :]
    member = jnp.any(hit, axis=1).astype(jnp.float32)
    high = jnp.sum(jnp.where(hit, wide[:, 6:12, None], 0.0), axis=1)
    low = jnp.sum(jnp.where(hit, wide[:, 12:18, None], 0.0), axis=1)
    at = np.arange(tokens)
    earlier = (at[:, None] // per_sender == at[None, :] // per_sender) & (at[:, None] < at[None, :])
    rank = jnp.einsum("te,tu->eu", member.astype(jnp.bfloat16), jnp.asarray(earlier, jnp.bfloat16), preferred_element_type=jnp.float32)
    sender = jnp.asarray(at // per_sender, jnp.float32)
    row = jnp.where(member.T > 0, sender[None, :] * slots + rank, -1.0)
    choice = row[:, None, :] == jnp.arange(senders * slots, dtype=jnp.float32)[None, :, None]
    weights = [jnp.where(choice, part.T[:, None, :], 0.0).astype(jnp.bfloat16).reshape(-1, tokens) for part in (high, low)]
    return choice.astype(jnp.bfloat16).reshape(-1, tokens), weights


def on_device(
    hidden_in,
    state_in,
    receptance,
    key_in,
    value_in,
    learn_in,
    decay_in,
    decay_base,
    norm_gain,
    out_weight,
    routed_gain,
    expert_gate,
    expert_up,
    expert_down,
    route_ids,
    route_weights,
):
    bf16, f32 = jnp.bfloat16, jnp.float32
    n_y, n_z, n_zp = lax.axis_size("y"), lax.axis_size(Z_AXES), lax.axis_size("zp")
    near = lax.axis_size(("zp", "x", "c"))
    seqs, width = hidden_in.shape
    quarter = width // n_y
    piece = quarter // n_zp
    slots = 2
    y = lax.axis_index("y")

    product, new_state = heads_update(
        n_y, state_in, receptance, key_in, value_in, learn_in, decay_in, decay_base, norm_gain, out_weight
    )
    arrived = exchange(product, "y")
    attention = arrived.astype(f32).sum(axis=0).astype(bf16)
    residual = hidden_in.astype(f32) + attention.astype(f32)
    scale = lax.rsqrt(jnp.mean(residual * residual, axis=-1, keepdims=True) + EPSILON)
    normed = (residual * scale * routed_gain[None, :]).astype(bf16)
    own = lax.dynamic_slice_in_dim(normed, y * quarter, quarter, 1)
    own_residual = lax.dynamic_slice_in_dim(residual, y * quarter, quarter, 1)

    high, low = split_weights(route_weights)
    routing = jnp.concatenate([route_ids.astype(bf16), high, low], axis=1)
    routing = jnp.pad(routing, ((0, 0), (0, 128 - routing.shape[1])))
    halves = own.reshape(seqs, n_zp, piece).transpose(1, 0, 2)
    parcel = jnp.concatenate([halves, jnp.broadcast_to(routing, (n_zp, seqs, 128))], axis=2)
    parcels = jnp.broadcast_to(parcel, (n_z // n_zp, *parcel.shape)).reshape(n_z, seqs, piece + 128)
    rows = exchange(parcels, Z_AXES).reshape(n_z * seqs, piece + 128)

    choice, (weight_high, weight_low) = selection(rows[:, piece:], lax.axis_index("zq") * near, near, slots)
    chosen = jnp.dot(choice, rows[:, :piece], preferred_element_type=f32).astype(bf16)
    per_expert = n_z * slots
    chosen = chosen.reshape(near, 1, per_expert, piece)
    outgoing = jnp.broadcast_to(chosen, (near, n_y, per_expert, piece)).reshape(near * n_y, per_expert, piece)
    got = exchange(outgoing, NEAR_AXES)

    n_xc = near // n_zp
    back = experts(
        got.reshape(n_zp, n_xc, n_y, per_expert, piece), expert_gate, expert_up, expert_down
    )
    returned = exchange(back.reshape(near * n_y, per_expert, piece), NEAR_AXES)

    summed = returned.reshape(near, n_y, per_expert, piece).astype(f32).sum(axis=1).astype(bf16)
    summed = summed.reshape(near * per_expert, piece)

    def weighed(weight):
        return lax.dot_general(weight, summed, (((0,), (0,)), ((), ())), preferred_element_type=f32)

    combined = (weighed(weight_high) + weighed(weight_low)).astype(bf16)
    parts = exchange(combined.reshape(n_z, seqs, piece), Z_AXES)
    routed = parts.reshape(n_z // n_zp, n_zp, seqs, piece).astype(f32).sum(axis=0)
    routed = routed.transpose(1, 0, 2).reshape(seqs, quarter)
    result = (own_residual + routed).astype(bf16)
    spread = exchange(jnp.broadcast_to(result, (n_y, seqs, quarter)), "y")
    return (spread.transpose(1, 0, 2).reshape(seqs, width), new_state)


def solution(mesh):
    near_mesh = Mesh(mesh.devices.reshape(8, 2, 4, 2, 4), ("zq", "zp", "x", "c", "y"))
    in_specs = (
        P(EP, None),
        P(EP, "y", None, None),
        P(EP, "y"),
        P(EP, "y"),
        P(EP, "y"),
        P(EP, "y"),
        P(EP, "y"),
        P("y"),
        P("y"),
        P("y", None),
        P(),
        P(EP, None, "y"),
        P(EP, None, "y"),
        P(EP, "y", None),
        P(EP, None),
        P(EP, None),
    )
    out_specs = (P(EP, None), P(EP, "y", None, None))
    return jax.shard_map(
        on_device, mesh=near_mesh, in_specs=in_specs, out_specs=out_specs, check_vma=False
    )
```

```python
import functools
import math
import jax
import jax.numpy as jnp
import numpy as np
from jax import lax
from jax.experimental import pallas as pl
from jax.experimental.pallas import tpu as pltpu
from jax.sharding import Mesh, PartitionSpec as P

EPSILON = 1e-06
GROUP_EPSILON = 0.00064
SEQ_STEP = 4
SLOTS = 2
Z_AXES = ("zq", "zp")
NEAR_AXES = ("zp", "x", "c", "y")
EP = ("zq", "zp", "x", "c")


def exchange(pieces, axes):
    return lax.all_to_all(pieces, axes, split_axis=0, concat_axis=0, tiled=True)


def split_dot(product, ones, contract):
    high = product.astype(jnp.bfloat16)
    low = (product - high.astype(jnp.float32)).astype(jnp.bfloat16)
    return contract(high, ones) + contract(low, ones)


def sum_across(product, ones):
    return jnp.dot(product, ones, preferred_element_type=jnp.float32)


def sum_to_row(product, ones):
    return lax.dot_general(
        ones, product, (((1,), (1,)), ((), ())), preferred_element_type=jnp.float32
    )


def heads_kernel(
    copies,
    state_ref,
    reading_ref,
    key_ref,
    value_ref,
    learn_ref,
    decay_ref,
    base_ref,
    gain_ref,
    weight_ref,
    new_state_ref,
    out_ref,
    rows,
    read,
):
    f32, bf16 = jnp.float32, jnp.bfloat16
    step = pl.program_id(0)
    seqs, channels = reading_ref.shape
    per_step, heads, size, _ = state_ref.shape

    @pl.when(step == 0)
    def _():
        keys = key_ref[...].astype(f32)
        values = value_ref[...].astype(f32)
        learning = jax.nn.sigmoid(learn_ref[...].astype(f32))
        decay = jnp.exp(-math.exp(-0.5) * jax.nn.sigmoid(base_ref[...] + decay_ref[...]))
        reading = reading_ref[...].astype(f32)
        read[...] = jnp.zeros_like(read)
        for head in range(heads):
            at = slice(head * size, (head + 1) * size)
            key = keys[:, at]
            unit = key * lax.rsqrt(jnp.sum(key * key, axis=1, keepdims=True) + EPSILON)
            rows[0, head] = unit
            rows[1, head] = decay[:, at]
            rows[2, head] = unit * learning[:, at]
            rows[3, head] = key
            rows[4, head] = reading[:, at]
            rows[5, head] = values[:, at]

    square = (size, size)
    diagonal = lax.broadcasted_iota(jnp.int32, square, 0) == lax.broadcasted_iota(jnp.int32, square, 1)
    ones = jnp.ones(square, bf16)
    tall_ones = jnp.ones((seqs, size), bf16)
    seq_of = lax.broadcasted_iota(jnp.int32, (seqs, channels), 0)
    found = read[...]
    for local in range(per_step):
        seq = step * per_step + local

        def row(which, head):
            return rows[which, head, pl.ds(seq, 1), :]

        carried = split_dot(
            jnp.concatenate([state_ref[local, head] * row(0, head) for head in range(heads)], axis=0),
            ones,
            sum_across,
        )
        value = sum_across(
            jnp.concatenate(
                [jnp.where(diagonal, row(5, head), 0.0).astype(bf16) for head in range(heads)], axis=0
            ),
            ones,
        )
        news = []
        for head in range(heads):
            at = slice(head * size, (head + 1) * size)
            new = (
                state_ref[local, head] * row(1, head)
                - carried[at] * row(2, head)
                + value[at] * row(3, head)
            )
            new_state_ref[local, head] = new
            news.append(new * row(4, head))
        found = jnp.where(
            seq_of == seq, split_dot(jnp.concatenate(news, axis=0), tall_ones, sum_to_row), found
        )
    read[...] = found

    @pl.when(step == pl.num_programs(0) - 1)
    def _():
        output = read[...]
        gain = gain_ref[...]
        mixed = []
        for head in range(heads):
            at = slice(head * size, (head + 1) * size)
            live = output[:, at]
            live = live - jnp.mean(live, axis=1, keepdims=True)
            spread = jnp.mean(jnp.square(live), axis=1, keepdims=True)
            mixed.append(live * lax.rsqrt(spread + GROUP_EPSILON) * gain[:, at])
        mixed = jnp.concatenate(mixed, axis=1).astype(bf16)
        product = jnp.dot(mixed, weight_ref[...], preferred_element_type=f32).astype(bf16)
        for copy in range(copies):
            out_ref[copy] = product


def heads_update(copies, state_in, receptance, key_in, value_in, learn_in, decay_in, decay_base, norm_gain, out_weight):
    seqs, heads, size, _ = state_in.shape
    width = out_weight.shape[1]
    channels = heads * size
    block = pl.BlockSpec((SEQ_STEP, heads, size, size), lambda s: (s, 0, 0, 0))

    def whole(shape):
        return pl.BlockSpec(shape, lambda s: (0,) * len(shape))

    tall = whole((seqs, channels))
    flat = whole((1, channels))
    new_state, product = pl.pallas_call(
        functools.partial(heads_kernel, copies),
        grid=(seqs // SEQ_STEP,),
        in_specs=[block, tall, tall, tall, tall, tall, flat, flat, whole((channels, width))],
        out_specs=[block, whole((copies, seqs, width))],
        out_shape=[
            jax.ShapeDtypeStruct(state_in.shape, jnp.float32),
            jax.ShapeDtypeStruct((copies, seqs, width), jnp.bfloat16),
        ],
        scratch_shapes=[
            pltpu.VMEM((6, heads, seqs, size), jnp.float32),
            pltpu.VMEM((seqs, channels), jnp.float32),
        ],
        compiler_params=pltpu.CompilerParams(vmem_limit_bytes=60 << 20),
        cost_estimate=pl.CostEstimate(flops=20_000_000, bytes_accessed=5_000_000, transcendentals=20_000),
    )(
        state_in,
        receptance,
        key_in,
        value_in,
        learn_in,
        decay_in,
        decay_base.reshape(1, channels),
        norm_gain.reshape(1, channels),
        out_weight,
    )
    return product, new_state


def expert_kernel(got_ref, gate_ref, up_ref, down_ref, out_ref, flat):
    f32 = jnp.float32
    n_zp, n_xc, n_y, rows, piece = got_ref.shape
    total = n_xc * rows
    for y in range(n_y):
        for zp in range(n_zp):
            at = (y * n_zp + zp) * piece
            flat[:, at : at + piece] = got_ref[zp, :, y].reshape(total, piece)
    arrived = flat[...]
    gate = jnp.dot(arrived, gate_ref[0], preferred_element_type=f32)
    upward = jnp.dot(arrived, up_ref[0], preferred_element_type=f32)
    hidden = (gate * jax.nn.sigmoid(gate) * upward).astype(jnp.bfloat16)
    for y in range(n_y):
        for zp in range(n_zp):
            at = (y * n_zp + zp) * piece
            partial = jnp.dot(hidden, down_ref[0, :, at : at + piece], preferred_element_type=f32)
            out_ref[zp, :, y] = partial.astype(jnp.bfloat16).reshape(n_xc, rows, piece)


def experts(got, expert_gate, expert_up, expert_down):
    n_zp, n_xc, n_y, rows, piece = got.shape
    vmem = pl.BlockSpec(memory_space=pltpu.VMEM)
    return pl.pallas_call(
        expert_kernel,
        in_specs=[vmem] * 4,
        out_specs=vmem,
        out_shape=jax.ShapeDtypeStruct(got.shape, jnp.bfloat16),
        scratch_shapes=[pltpu.VMEM((n_xc * rows, n_zp * n_y * piece), jnp.bfloat16)],
        compiler_params=pltpu.CompilerParams(vmem_limit_bytes=12 << 20),
        cost_estimate=pl.CostEstimate(flops=400_000_000, bytes_accessed=4_000_000, transcendentals=40_000),
    )(got, expert_gate, expert_up, expert_down)


def pack_kernel(
    n_zp, arrived_ref, hidden_ref, gain_ref, ids_ref, weights_ref, parcels_ref, own_ref
):
    f32, bf16 = jnp.float32, jnp.bfloat16
    seqs, width = hidden_ref.shape
    quarter = own_ref.shape[1]
    top = ids_ref.shape[0]
    attention = jnp.sum(arrived_ref[...].astype(f32), axis=0).astype(bf16)
    residual = hidden_ref[...].astype(f32) + attention.astype(f32)
    scale = lax.rsqrt(jnp.mean(residual * residual, axis=1, keepdims=True) + EPSILON)
    at = pl.ds(pl.multiple_of(lax.axis_index("y") * quarter, quarter), quarter)
    attention = jnp.sum(arrived_ref[:, :, at].astype(f32), axis=0).astype(bf16)
    residual = hidden_ref[:, at].astype(f32) + attention.astype(f32)
    own_ref[...] = residual
    normed = (residual * scale * gain_ref[:, at]).astype(bf16)

    weights = weights_ref[...]
    routing = jnp.zeros((8, 128), f32)
    parts = [ids_ref[...].astype(f32)]
    for _ in range(3):
        part = weights.astype(bf16).astype(f32)
        parts.append(part)
        weights = weights - part
    routing = jnp.concatenate(
        [jnp.pad(part, ((0, 8 - top), (0, 0))) for part in parts]
        + [jnp.zeros((8, 128 - len(parts) * seqs), f32)],
        axis=1,
    ).astype(bf16)
    n_z = parcels_ref.shape[0]
    chunks = quarter // n_zp // 128
    for z in range(n_z):
        first = (z % n_zp) * chunks
        for chunk in range(chunks):
            lanes = slice((first + chunk) * 128, (first + chunk + 1) * 128)
            parcels_ref[z, chunk * seqs : (chunk + 1) * seqs, :] = normed[:, lanes]
        parcels_ref[z, chunks * seqs : chunks * seqs + 8, :] = routing


def pack(arrived, hidden_in, routed_gain, route_ids, route_weights, n_z, n_zp):
    n_y, seqs, width = arrived.shape
    quarter = width // n_y
    vmem = pl.BlockSpec(memory_space=pltpu.VMEM)
    return pl.pallas_call(
        functools.partial(pack_kernel, n_zp),
        in_specs=[vmem] * 5,
        out_specs=[vmem] * 2,
        out_shape=[
            jax.ShapeDtypeStruct((n_z, quarter // n_zp // 128 * seqs + 8, 128), jnp.bfloat16),
            jax.ShapeDtypeStruct((seqs, quarter), jnp.float32),
        ],
        compiler_params=pltpu.CompilerParams(vmem_limit_bytes=8 << 20),
    )(arrived, hidden_in, routed_gain.reshape(1, width), route_ids.T, route_weights.T)


def choose_kernel(top, slots, rows_ref, chosen_ref, place_ref, weight_ref, flat, choice):
    f32, bf16 = jnp.float32, jnp.bfloat16
    n_z = rows_ref.shape[0]
    seqs = flat.shape[0] // n_z
    near, n_y, per_expert, piece = chosen_ref.shape
    tokens = n_z * seqs
    chunks = piece // 128
    sender_of = lax.broadcasted_iota(jnp.int32, (8, 128), 1) // seqs
    groups = tokens // 128
    per_group = 128 // seqs
    spread = [[jnp.zeros((8, 128), f32) for _ in range(groups)] for _ in range(4)]
    for z in range(n_z):
        for chunk in range(chunks):
            flat[z * seqs : (z + 1) * seqs, chunk * 128 : (chunk + 1) * 128] = rows_ref[
                z, chunk * seqs : (chunk + 1) * seqs, :
            ]
        routing = rows_ref[z, chunks * seqs : chunks * seqs + 8, :].astype(f32)
        group, place = divmod(z, per_group)
        for which in range(4):
            turn = (place - which) * seqs % 128
            moved = routing if turn == 0 else pltpu.roll(routing, turn, 1)
            spread[which][group] = jnp.where(sender_of == place, moved, spread[which][group])
    ids, high, middle, low = [jnp.concatenate(part, axis=1) for part in spread]
    weights = high + middle + low
    named = (
        lax.axis_index("zq") * near + lax.broadcasted_iota(jnp.int32, (near, tokens), 0)
    ).astype(f32)
    member = jnp.zeros((near, tokens), f32)
    weight = jnp.zeros((near, tokens), f32)
    for k in range(top):
        hit = named == ids[k : k + 1, :]
        member = jnp.where(hit, 1.0, member)
        weight = jnp.where(hit, weights[k : k + 1, :], weight)
    token = lax.broadcasted_iota(jnp.int32, (tokens, tokens), 0)
    other = lax.broadcasted_iota(jnp.int32, (tokens, tokens), 1)
    earlier = (token // seqs == other // seqs) & (token < other)
    rank = jnp.dot(member.astype(bf16), jnp.where(earlier, 1.0, 0.0).astype(bf16), preferred_element_type=f32)
    sender = (lax.broadcasted_iota(jnp.int32, (near, tokens), 1) // seqs * slots).astype(f32)
    place = jnp.where(member > 0, sender + rank, -1.0)
    place_ref[...] = place
    weight_ref[...] = weight
    row = lax.broadcasted_iota(jnp.int32, (per_expert, tokens), 0).astype(f32)
    for expert in range(near):
        choice[expert * per_expert : (expert + 1) * per_expert, :] = jnp.where(
            row == place[expert : expert + 1, :], 1.0, 0.0
        ).astype(bf16)
    chosen = jnp.dot(choice[...], flat[...], preferred_element_type=f32).astype(bf16)
    chosen = chosen.reshape(near, per_expert, piece)
    for y in range(n_y):
        chosen_ref[:, y] = chosen


def choose(rows, near, n_y, slots, top, seqs):
    n_z, depth, _ = rows.shape
    piece = (depth - 8) // seqs * 128
    tokens = n_z * seqs
    vmem = pl.BlockSpec(memory_space=pltpu.VMEM)
    return pl.pallas_call(
        functools.partial(choose_kernel, top, slots),
        in_specs=[vmem],
        out_specs=[vmem] * 3,
        out_shape=[
            jax.ShapeDtypeStruct((near, n_y, n_z * slots, piece), jnp.bfloat16),
            jax.ShapeDtypeStruct((near, tokens), jnp.float32),
            jax.ShapeDtypeStruct((near, tokens), jnp.float32),
        ],
        scratch_shapes=[
            pltpu.VMEM((tokens, piece), jnp.bfloat16),
            pltpu.VMEM((near * n_z * slots, tokens), jnp.bfloat16),
        ],
        compiler_params=pltpu.CompilerParams(vmem_limit_bytes=12 << 20),
    )(rows)


def combine_kernel(returned_ref, place_ref, weight_ref, out_ref, summed, choice):
    f32, bf16 = jnp.float32, jnp.bfloat16
    near, n_y, per_expert, piece = returned_ref.shape
    n_z, seqs, _ = out_ref.shape
    tokens = n_z * seqs
    total = near * per_expert
    row = lax.broadcasted_iota(jnp.int32, (per_expert, tokens), 0).astype(f32)
    for expert in range(near):
        at = slice(expert * per_expert, (expert + 1) * per_expert)
        result = jnp.sum(returned_ref[expert].astype(f32), axis=0).astype(bf16)
        summed[at, :] = result
        summed[total + expert * per_expert : total + (expert + 1) * per_expert, :] = result
        weight = jnp.where(
            row == place_ref[expert : expert + 1, :], weight_ref[expert : expert + 1, :], 0.0
        )
        high = weight.astype(bf16)
        choice[at, :] = high
        choice[total + expert * per_expert : total + (expert + 1) * per_expert, :] = (
            weight - high.astype(f32)
        ).astype(bf16)
    combined = lax.dot_general(
        choice[...], summed[...], (((0,), (0,)), ((), ())), preferred_element_type=f32
    )
    out_ref[...] = combined.astype(bf16).reshape(n_z, seqs, piece)


def combine(returned, place, weight, n_z):
    near, n_y, per_expert, piece = returned.shape
    tokens = place.shape[1]
    vmem = pl.BlockSpec(memory_space=pltpu.VMEM)
    return pl.pallas_call(
        combine_kernel,
        in_specs=[vmem] * 3,
        out_specs=vmem,
        out_shape=jax.ShapeDtypeStruct((n_z, tokens // n_z, piece), jnp.bfloat16),
        scratch_shapes=[
            pltpu.VMEM((2 * near * per_expert, piece), jnp.bfloat16),
            pltpu.VMEM((2 * near * per_expert, tokens), jnp.bfloat16),
        ],
        compiler_params=pltpu.CompilerParams(vmem_limit_bytes=12 << 20),
    )(returned, place, weight)


def on_device(
    hidden_in,
    state_in,
    receptance,
    key_in,
    value_in,
    learn_in,
    decay_in,
    decay_base,
    norm_gain,
    out_weight,
    routed_gain,
    expert_gate,
    expert_up,
    expert_down,
    route_ids,
    route_weights,
):
    n_y, n_z, n_zp = lax.axis_size("y"), lax.axis_size(Z_AXES), lax.axis_size("zp")
    near = lax.axis_size(("zp", "x", "c"))
    seqs, width = hidden_in.shape
    quarter = width // n_y
    piece = quarter // n_zp
    per_expert = n_z * SLOTS

    product, new_state = heads_update(
        n_y, state_in, receptance, key_in, value_in, learn_in, decay_in, decay_base, norm_gain, out_weight
    )
    arrived = exchange(product, "y")
    parcels, own_residual = pack(arrived, hidden_in, routed_gain, route_ids, route_weights, n_z, n_zp)
    rows = exchange(parcels, Z_AXES)
    chosen, place, weight = choose(rows, near, n_y, SLOTS, route_ids.shape[1], seqs)
    got = exchange(chosen.reshape(near * n_y, per_expert, piece), NEAR_AXES)
    got = got.reshape(n_zp, near // n_zp, n_y, per_expert, piece)
    back = experts(got, expert_gate, expert_up, expert_down)
    returned = exchange(back.reshape(near * n_y, per_expert, piece), NEAR_AXES)
    combined = combine(returned.reshape(near, n_y, per_expert, piece), place, weight, n_z)
    parts = exchange(combined, Z_AXES)
    routed = parts.reshape(n_z // n_zp, n_zp, seqs, piece).astype(jnp.float32).sum(axis=0)
    routed = routed.transpose(1, 0, 2).reshape(seqs, quarter)
    result = (own_residual + routed).astype(jnp.bfloat16)
    spread = exchange(jnp.broadcast_to(result, (n_y, seqs, quarter)), "y")
    return (spread.transpose(1, 0, 2).reshape(seqs, width), new_state)


def solution(mesh):
    near_mesh = Mesh(mesh.devices.reshape(8, 2, 4, 2, 4), ("zq", "zp", "x", "c", "y"))
    in_specs = (
        P(EP, None),
        P(EP, "y", None, None),
        P(EP, "y"),
        P(EP, "y"),
        P(EP, "y"),
        P(EP, "y"),
        P(EP, "y"),
        P("y"),
        P("y"),
        P("y", None),
        P(),
        P(EP, None, "y"),
        P(EP, None, "y"),
        P(EP, "y", None),
        P(EP, None),
        P(EP, None),
    )
    out_specs = (P(EP, None), P(EP, "y", None, None))
    return jax.shard_map(
        on_device, mesh=near_mesh, in_specs=in_specs, out_specs=out_specs, check_vma=False
    )
```

```python
import functools
import math
import jax
import jax.numpy as jnp
import numpy as np
from jax import lax
from jax.experimental import pallas as pl
from jax.experimental.pallas import tpu as pltpu
from jax.sharding import Mesh, PartitionSpec as P

EPSILON = 1e-06
GROUP_EPSILON = 0.00064
SEQ_STEP = 8
SLOTS = 2
NEAR_AXES = ("zp", "x", "c", "y")
EP = ("zq", "zp", "x", "c")


def exchange(pieces, axes):
    return lax.all_to_all(pieces, axes, split_axis=0, concat_axis=0, tiled=True)


def two_parts(values):
    high = values.astype(jnp.bfloat16)
    return high, (values - high.astype(jnp.float32)).astype(jnp.bfloat16)


def heads_kernel(
    copies,
    state_ref,
    reading_ref,
    key_ref,
    value_ref,
    learn_ref,
    decay_ref,
    base_ref,
    gain_ref,
    weight_ref,
    new_state_ref,
    out_ref,
    rows,
    read,
    joined,
    parts,
    sums,
):
    f32, bf16 = jnp.float32, jnp.bfloat16
    step = pl.program_id(0)
    seqs, channels = reading_ref.shape
    per_step, heads, size, _ = state_ref.shape
    pairs = heads // 2
    pair_width = 2 * size
    square = (pair_width, pair_width)
    same_head = (
        lax.broadcasted_iota(jnp.int32, square, 0) // size
        == lax.broadcasted_iota(jnp.int32, square, 1) // size
    )
    ones = jnp.where(same_head, 1.0, 0.0).astype(bf16)

    def head_sums(values):
        return sum(jnp.dot(part, ones, preferred_element_type=f32) for part in two_parts(values))

    @pl.when(step == 0)
    def _():
        learning = jax.nn.sigmoid(learn_ref[...].astype(f32))
        decay = jnp.exp(-math.exp(-0.5) * jax.nn.sigmoid(base_ref[...] + decay_ref[...]))
        keys = key_ref[...].astype(f32)
        read[...] = jnp.zeros_like(read)
        for pair in range(pairs):
            at = slice(pair * pair_width, (pair + 1) * pair_width)
            key = keys[:, at]
            unit = key * lax.rsqrt(head_sums(key * key) + EPSILON)
            rows[0, pair] = unit
            rows[1, pair] = decay[:, at]
            rows[2, pair] = unit * learning[:, at]
            rows[3, pair] = key
            rows[4, pair] = reading_ref[:, at].astype(f32)
            rows[5, pair] = value_ref[:, at].astype(f32)

    blocks = [
        (local, pair, slice((local * pairs + pair) * size, (local * pairs + pair + 1) * size))
        for local in range(per_step)
        for pair in range(pairs)
    ]

    def row(which, local, pair):
        return rows[which, pair, pl.ds(step * per_step + local, 1), :]

    on_diagonal = lax.broadcasted_iota(jnp.int32, (size, pair_width), 0) == (
        lax.broadcasted_iota(jnp.int32, (size, pair_width), 1) % size
    )
    for local, pair, at in blocks:
        state = jnp.concatenate([state_ref[local, 2 * pair], state_ref[local, 2 * pair + 1]], axis=1)
        joined[at, :] = state
        parts[0, at, :], parts[1, at, :] = two_parts(state * row(0, local, pair))
        parts[2, at, :] = jnp.where(on_diagonal, row(5, local, pair), 0.0).astype(bf16)
    sums[0] = jnp.dot(parts[0], ones, preferred_element_type=f32) + jnp.dot(
        parts[1], ones, preferred_element_type=f32
    )
    sums[1] = jnp.dot(parts[2], ones, preferred_element_type=f32)
    for local, pair, at in blocks:
        new = (
            joined[at, :] * row(1, local, pair)
            - sums[0, at, :] * row(2, local, pair)
            + sums[1, at, :] * row(3, local, pair)
        )
        new_state_ref[local, 2 * pair] = new[:, 0:size]
        new_state_ref[local, 2 * pair + 1] = new[:, size:pair_width]
        parts[0, at, :], parts[1, at, :] = two_parts(new * row(4, local, pair))
    head_of = lax.broadcasted_iota(jnp.int32, (2 * 8, pair_width), 0) // 8
    pick = jnp.where(
        head_of == lax.broadcasted_iota(jnp.int32, (2 * 8, pair_width), 1) // size, 1.0, 0.0
    ).astype(bf16)
    dims = (((1,), (1,)), ((), ()))
    found = lax.dot_general(pick, parts[0], dims, preferred_element_type=f32) + lax.dot_general(
        pick, parts[1], dims, preferred_element_type=f32
    )
    seq_of = lax.broadcasted_iota(jnp.int32, (seqs, pairs * size), 0)
    for which in range(2):
        latest = read[which]
        for local in range(per_step):
            line = found[which * 8 : which * 8 + 1, local * pairs * size : (local + 1) * pairs * size]
            latest = jnp.where(seq_of == step * per_step + local, line, latest)
        read[which] = latest

    @pl.when(step == pl.num_programs(0) - 1)
    def _():
        mixed = []
        for pair in range(pairs):
            at = slice(pair * size, (pair + 1) * size)
            live = jnp.concatenate([read[0, :, at], read[1, :, at]], axis=1)
            live = live - head_sums(live) * (1.0 / size)
            spread = head_sums(jnp.square(live)) * (1.0 / size)
            gain = gain_ref[:, pair * pair_width : (pair + 1) * pair_width]
            mixed.append(live * lax.rsqrt(spread + GROUP_EPSILON) * gain)
        mixed = jnp.concatenate(mixed, axis=1).astype(bf16)
        product = jnp.dot(mixed, weight_ref[...], preferred_element_type=f32).astype(bf16)
        for copy in range(copies):
            out_ref[copy] = product


def heads_update(copies, state_in, receptance, key_in, value_in, learn_in, decay_in, decay_base, norm_gain, out_weight):
    seqs, heads, size, _ = state_in.shape
    width = out_weight.shape[1]
    channels = heads * size
    block = pl.BlockSpec((SEQ_STEP, heads, size, size), lambda s: (s, 0, 0, 0))

    def whole(shape):
        return pl.BlockSpec(shape, lambda s: (0,) * len(shape))

    tall = whole((seqs, channels))
    flat = whole((1, channels))
    new_state, product = pl.pallas_call(
        functools.partial(heads_kernel, copies),
        grid=(seqs // SEQ_STEP,),
        in_specs=[block, tall, tall, tall, tall, tall, flat, flat, whole((channels, width))],
        out_specs=[block, whole((copies, seqs, width))],
        out_shape=[
            jax.ShapeDtypeStruct(state_in.shape, jnp.float32),
            pltpu.VMEM((copies, seqs, width), jnp.bfloat16),
        ],
        scratch_shapes=[
            pltpu.VMEM((6, heads // 2, seqs, 2 * size), jnp.float32),
            pltpu.VMEM((2, seqs, channels // 2), jnp.float32),
            pltpu.VMEM((SEQ_STEP * heads // 2 * size, 2 * size), jnp.float32),
            pltpu.VMEM((3, SEQ_STEP * heads // 2 * size, 2 * size), jnp.bfloat16),
            pltpu.VMEM((2, SEQ_STEP * heads // 2 * size, 2 * size), jnp.float32),
        ],
        compiler_params=pltpu.CompilerParams(vmem_limit_bytes=60 << 20),
        cost_estimate=pl.CostEstimate(flops=20_000_000, bytes_accessed=5_000_000, transcendentals=20_000),
    )(
        state_in,
        receptance,
        key_in,
        value_in,
        learn_in,
        decay_in,
        decay_base.reshape(1, channels),
        norm_gain.reshape(1, channels),
        out_weight,
    )
    return product, new_state


def expert_kernel(got_ref, gate_ref, up_ref, down_ref, out_ref, flat):
    f32 = jnp.float32
    senders, n_y, rows, quarter = got_ref.shape
    for y in range(n_y):
        flat[:, y * quarter : (y + 1) * quarter] = got_ref[:, y].reshape(senders * rows, quarter)
    arrived = flat[...]
    gate = jnp.dot(arrived, gate_ref[0], preferred_element_type=f32)
    upward = jnp.dot(arrived, up_ref[0], preferred_element_type=f32)
    hidden = (gate * jax.nn.sigmoid(gate) * upward).astype(jnp.bfloat16)
    for y in range(n_y):
        partial = jnp.dot(
            hidden, down_ref[0, :, y * quarter : (y + 1) * quarter], preferred_element_type=f32
        )
        out_ref[:, y] = partial.astype(jnp.bfloat16).reshape(senders, rows, quarter)


def experts(got, expert_gate, expert_up, expert_down):
    senders, n_y, rows, quarter = got.shape
    vmem = pl.BlockSpec(memory_space=pltpu.VMEM)
    return pl.pallas_call(
        expert_kernel,
        in_specs=[vmem] * 4,
        out_specs=vmem,
        out_shape=jax.ShapeDtypeStruct(got.shape, jnp.bfloat16),
        scratch_shapes=[pltpu.VMEM((senders * rows, n_y * quarter), jnp.bfloat16)],
        compiler_params=pltpu.CompilerParams(vmem_limit_bytes=12 << 20),
        cost_estimate=pl.CostEstimate(flops=400_000_000, bytes_accessed=4_000_000, transcendentals=40_000),
    )(got, expert_gate, expert_up, expert_down)


def pack_kernel(
    arrived_ref, hidden_ref, gain_ref, ids_ref, weights_ref, parcels_ref, own_ref
):
    f32, bf16 = jnp.float32, jnp.bfloat16
    seqs, width = hidden_ref.shape
    quarter = own_ref.shape[1]
    top = ids_ref.shape[0]
    attention = jnp.sum(arrived_ref[...].astype(f32), axis=0).astype(bf16)
    residual = hidden_ref[...].astype(f32) + attention.astype(f32)
    scale = lax.rsqrt(jnp.mean(residual * residual, axis=1, keepdims=True) + EPSILON)
    at = pl.ds(pl.multiple_of(lax.axis_index("y") * quarter, quarter), quarter)
    attention = jnp.sum(arrived_ref[:, :, at].astype(f32), axis=0).astype(bf16)
    residual = hidden_ref[:, at].astype(f32) + attention.astype(f32)
    own_ref[...] = residual
    normed = (residual * scale * gain_ref[:, at]).astype(bf16)

    weights = weights_ref[...]
    routing = jnp.zeros((8, 128), f32)
    parts = [ids_ref[...].astype(f32)]
    for _ in range(3):
        part = weights.astype(bf16).astype(f32)
        parts.append(part)
        weights = weights - part
    routing = jnp.concatenate(
        [jnp.pad(part, ((0, 8 - top), (0, 0))) for part in parts]
        + [jnp.zeros((8, 128 - len(parts) * seqs), f32)],
        axis=1,
    ).astype(bf16)
    chunks = quarter // 128
    for z in range(parcels_ref.shape[0]):
        for chunk in range(chunks):
            parcels_ref[z, chunk * seqs : (chunk + 1) * seqs, :] = normed[
                :, chunk * 128 : (chunk + 1) * 128
            ]
        parcels_ref[z, chunks * seqs : chunks * seqs + 8, :] = routing


def pack(arrived, hidden_in, routed_gain, route_ids, route_weights, n_z):
    n_y, seqs, width = arrived.shape
    quarter = width // n_y
    vmem = pl.BlockSpec(memory_space=pltpu.VMEM)
    return pl.pallas_call(
        pack_kernel,
        in_specs=[vmem] * 5,
        out_specs=[vmem] * 2,
        out_shape=[
            jax.ShapeDtypeStruct((n_z, quarter // 128 * seqs + 8, 128), jnp.bfloat16),
            jax.ShapeDtypeStruct((seqs, quarter), jnp.float32),
        ],
        compiler_params=pltpu.CompilerParams(vmem_limit_bytes=8 << 20),
    )(arrived, hidden_in, routed_gain.reshape(1, width), route_ids.T, route_weights.T)


def choose_kernel(top, slots, rows_ref, chosen_ref, place_ref, weight_ref, flat, choice):
    f32, bf16 = jnp.float32, jnp.bfloat16
    n_z = rows_ref.shape[0]
    seqs = flat.shape[0] // n_z
    near, n_y, per_expert, piece = chosen_ref.shape
    tokens = n_z * seqs
    chunks = piece // 128
    sender_of = lax.broadcasted_iota(jnp.int32, (8, 128), 1) // seqs
    groups = tokens // 128
    per_group = 128 // seqs
    spread = [[jnp.zeros((8, 128), f32) for _ in range(groups)] for _ in range(4)]
    for z in range(n_z):
        for chunk in range(chunks):
            flat[z * seqs : (z + 1) * seqs, chunk * 128 : (chunk + 1) * 128] = rows_ref[
                z, chunk * seqs : (chunk + 1) * seqs, :
            ]
        routing = rows_ref[z, chunks * seqs : chunks * seqs + 8, :].astype(f32)
        group, place = divmod(z, per_group)
        for which in range(4):
            turn = (place - which) * seqs % 128
            moved = routing if turn == 0 else pltpu.roll(routing, turn, 1)
            spread[which][group] = jnp.where(sender_of == place, moved, spread[which][group])
    ids, high, middle, low = [jnp.concatenate(part, axis=1) for part in spread]
    weights = high + middle + low
    named = (
        lax.axis_index("zq") * near + lax.broadcasted_iota(jnp.int32, (near, tokens), 0)
    ).astype(f32)
    member = jnp.zeros((near, tokens), f32)
    weight = jnp.zeros((near, tokens), f32)
    for k in range(top):
        hit = named == ids[k : k + 1, :]
        member = jnp.where(hit, 1.0, member)
        weight = jnp.where(hit, weights[k : k + 1, :], weight)
    token = lax.broadcasted_iota(jnp.int32, (tokens, tokens), 0)
    other = lax.broadcasted_iota(jnp.int32, (tokens, tokens), 1)
    earlier = (token // seqs == other // seqs) & (token < other)
    rank = jnp.dot(member.astype(bf16), jnp.where(earlier, 1.0, 0.0).astype(bf16), preferred_element_type=f32)
    sender = (lax.broadcasted_iota(jnp.int32, (near, tokens), 1) // seqs * slots).astype(f32)
    place = jnp.where(member > 0, sender + rank, -1.0)
    place_ref[...] = place
    weight_ref[...] = weight
    row = lax.broadcasted_iota(jnp.int32, (per_expert, tokens), 0).astype(f32)
    for expert in range(near):
        choice[expert * per_expert : (expert + 1) * per_expert, :] = jnp.where(
            row == place[expert : expert + 1, :], 1.0, 0.0
        ).astype(bf16)
    chosen = jnp.dot(choice[...], flat[...], preferred_element_type=f32).astype(bf16)
    chosen = chosen.reshape(near, per_expert, piece)
    for y in range(n_y):
        chosen_ref[:, y] = chosen


def choose(rows, near, n_y, slots, top, seqs):
    n_z, depth, _ = rows.shape
    piece = (depth - 8) // seqs * 128
    tokens = n_z * seqs
    vmem = pl.BlockSpec(memory_space=pltpu.VMEM)
    return pl.pallas_call(
        functools.partial(choose_kernel, top, slots),
        in_specs=[vmem],
        out_specs=[vmem] * 3,
        out_shape=[
            jax.ShapeDtypeStruct((near, n_y, n_z * slots, piece), jnp.bfloat16),
            jax.ShapeDtypeStruct((near, tokens), jnp.float32),
            jax.ShapeDtypeStruct((near, tokens), jnp.float32),
        ],
        scratch_shapes=[
            pltpu.VMEM((tokens, piece), jnp.bfloat16),
            pltpu.VMEM((near * n_z * slots, tokens), jnp.bfloat16),
        ],
        compiler_params=pltpu.CompilerParams(vmem_limit_bytes=12 << 20),
    )(rows)


def combine_kernel(returned_ref, place_ref, weight_ref, out_ref, summed, choice):
    f32, bf16 = jnp.float32, jnp.bfloat16
    near, n_y, per_expert, piece = returned_ref.shape
    n_z, seqs, _ = out_ref.shape
    tokens = n_z * seqs
    total = near * per_expert
    row = lax.broadcasted_iota(jnp.int32, (per_expert, tokens), 0).astype(f32)
    for expert in range(near):
        at = slice(expert * per_expert, (expert + 1) * per_expert)
        result = jnp.sum(returned_ref[expert].astype(f32), axis=0).astype(bf16)
        summed[at, :] = result
        summed[total + expert * per_expert : total + (expert + 1) * per_expert, :] = result
        weight = jnp.where(
            row == place_ref[expert : expert + 1, :], weight_ref[expert : expert + 1, :], 0.0
        )
        high = weight.astype(bf16)
        choice[at, :] = high
        choice[total + expert * per_expert : total + (expert + 1) * per_expert, :] = (
            weight - high.astype(f32)
        ).astype(bf16)
    combined = lax.dot_general(
        choice[...], summed[...], (((0,), (0,)), ((), ())), preferred_element_type=f32
    )
    out_ref[...] = combined.astype(bf16).reshape(n_z, seqs, piece)


def combine(returned, place, weight, n_z):
    near, n_y, per_expert, piece = returned.shape
    tokens = place.shape[1]
    vmem = pl.BlockSpec(memory_space=pltpu.VMEM)
    return pl.pallas_call(
        combine_kernel,
        in_specs=[vmem] * 3,
        out_specs=vmem,
        out_shape=jax.ShapeDtypeStruct((n_z, tokens // n_z, piece), jnp.bfloat16),
        scratch_shapes=[
            pltpu.VMEM((2 * near * per_expert, piece), jnp.bfloat16),
            pltpu.VMEM((2 * near * per_expert, tokens), jnp.bfloat16),
        ],
        compiler_params=pltpu.CompilerParams(vmem_limit_bytes=12 << 20),
    )(returned, place, weight)


def on_device(
    hidden_in,
    state_in,
    receptance,
    key_in,
    value_in,
    learn_in,
    decay_in,
    decay_base,
    norm_gain,
    out_weight,
    routed_gain,
    expert_gate,
    expert_up,
    expert_down,
    route_ids,
    route_weights,
):
    n_y, n_zq = lax.axis_size("y"), lax.axis_size("zq")
    near = lax.axis_size(("zp", "x", "c"))
    seqs, width = hidden_in.shape
    quarter = width // n_y
    per_expert = n_zq * SLOTS

    product, new_state = heads_update(
        n_y, state_in, receptance, key_in, value_in, learn_in, decay_in, decay_base, norm_gain, out_weight
    )
    arrived = exchange(product, "y")
    parcels, own_residual = pack(arrived, hidden_in, routed_gain, route_ids, route_weights, n_zq)
    rows = exchange(parcels, "zq")
    chosen, place, weight = choose(rows, near, n_y, SLOTS, route_ids.shape[1], seqs)
    got = exchange(chosen.reshape(near * n_y, per_expert, quarter), NEAR_AXES)
    back = experts(got.reshape(near, n_y, per_expert, quarter), expert_gate, expert_up, expert_down)
    returned = exchange(back.reshape(near * n_y, per_expert, quarter), NEAR_AXES)
    combined = combine(returned.reshape(near, n_y, per_expert, quarter), place, weight, n_zq)
    routed = exchange(combined, "zq").astype(jnp.float32).sum(axis=0)
    result = (own_residual + routed).astype(jnp.bfloat16)
    spread = exchange(jnp.broadcast_to(result, (n_y, seqs, quarter)), "y")
    return (spread.transpose(1, 0, 2).reshape(seqs, width), new_state)


def solution(mesh):
    near_mesh = Mesh(mesh.devices.reshape(8, 2, 4, 2, 4), ("zq", "zp", "x", "c", "y"))
    in_specs = (
        P(EP, None),
        P(EP, "y", None, None),
        P(EP, "y"),
        P(EP, "y"),
        P(EP, "y"),
        P(EP, "y"),
        P(EP, "y"),
        P("y"),
        P("y"),
        P("y", None),
        P(),
        P(EP, None, "y"),
        P(EP, None, "y"),
        P(EP, "y", None),
        P(EP, None),
        P(EP, None),
    )
    out_specs = (P(EP, None), P(EP, "y", None, None))
    return jax.shard_map(
        on_device, mesh=near_mesh, in_specs=in_specs, out_specs=out_specs, check_vma=False
    )
```

```python
import functools
import math
import jax
import jax.numpy as jnp
import numpy as np
from jax import lax
from jax.experimental import pallas as pl
from jax.experimental.pallas import tpu as pltpu
from jax.sharding import Mesh, PartitionSpec as P

EPSILON = 1e-06
GROUP_EPSILON = 0.00064
SEQ_STEP = 8
SLOTS = 2
NEAR_AXES = ("zp", "x", "c", "y")
EP = ("zq", "zp", "x", "c")


def exchange(pieces, axes):
    return lax.all_to_all(pieces, axes, split_axis=0, concat_axis=0, tiled=True)


def two_parts(values):
    high = values.astype(jnp.bfloat16)
    return high, (values - high.astype(jnp.float32)).astype(jnp.bfloat16)


def heads_kernel(
    copies,
    state_ref,
    reading_ref,
    key_ref,
    value_ref,
    learn_ref,
    decay_ref,
    base_ref,
    gain_ref,
    weight_ref,
    new_state_ref,
    out_ref,
    state_here,
    new_here,
    inputs,
    decay_here,
    vectors,
    weight_here,
    rows,
    read,
    joined,
    parts,
    sums,
    arrived,
    stored,
):
    f32, bf16 = jnp.float32, jnp.bfloat16
    seqs, heads, size, _ = state_here.shape
    channels = heads * size
    pairs = heads // 2
    pair_width = 2 * size
    steps = seqs // SEQ_STEP

    def state_load(step):
        at = pl.ds(step * SEQ_STEP, SEQ_STEP)
        return pltpu.make_async_copy(state_ref.at[at], state_here.at[at], arrived.at[step])

    def state_store(step):
        at = pl.ds(step * SEQ_STEP, SEQ_STEP)
        return pltpu.make_async_copy(new_here.at[at], new_state_ref.at[at], stored.at[step])

    small = [
        pltpu.make_async_copy(source, target, arrived.at[steps + number])
        for number, (source, target) in enumerate(
            (
                (key_ref, inputs.at[0]),
                (learn_ref, inputs.at[1]),
                (decay_ref, decay_here),
                (base_ref, vectors.at[0]),
                (reading_ref, inputs.at[2]),
                (value_ref, inputs.at[3]),
                (gain_ref, vectors.at[1]),
            )
        )
    ]
    weight_load = pltpu.make_async_copy(weight_ref, weight_here, arrived.at[steps + len(small)])
    for load in small:
        load.start()
    for step in range(steps):
        state_load(step).start()
    weight_load.start()

    square = (pair_width, pair_width)
    same_head = (
        lax.broadcasted_iota(jnp.int32, square, 0) // size
        == lax.broadcasted_iota(jnp.int32, square, 1) // size
    )
    ones = jnp.where(same_head, 1.0, 0.0).astype(bf16)

    def head_sums(values):
        return sum(jnp.dot(part, ones, preferred_element_type=f32) for part in two_parts(values))

    for load in small:
        load.wait()
    keys = inputs[0].astype(f32)
    learning = jax.nn.sigmoid(inputs[1].astype(f32))
    decay = jnp.exp(-math.exp(-0.5) * jax.nn.sigmoid(vectors[0] + decay_here[...]))
    read[...] = jnp.zeros_like(read)
    for pair in range(pairs):
        at = slice(pair * pair_width, (pair + 1) * pair_width)
        key = keys[:, at]
        unit = key * lax.rsqrt(head_sums(key * key) + EPSILON)
        rows[0, pair] = unit
        rows[1, pair] = decay[:, at]
        rows[2, pair] = unit * learning[:, at]
        rows[3, pair] = key
        rows[4, pair] = inputs[2, :, at].astype(f32)
        rows[5, pair] = inputs[3, :, at].astype(f32)

    blocks = [
        (local, pair, slice((local * pairs + pair) * size, (local * pairs + pair + 1) * size))
        for local in range(SEQ_STEP)
        for pair in range(pairs)
    ]
    on_diagonal = lax.broadcasted_iota(jnp.int32, (size, pair_width), 0) == (
        lax.broadcasted_iota(jnp.int32, (size, pair_width), 1) % size
    )
    head_of = lax.broadcasted_iota(jnp.int32, (2 * 8, pair_width), 0) // 8
    pick = jnp.where(
        head_of == lax.broadcasted_iota(jnp.int32, (2 * 8, pair_width), 1) // size, 1.0, 0.0
    ).astype(bf16)
    seq_of = lax.broadcasted_iota(jnp.int32, (seqs, pairs * size), 0)

    @pl.loop(0, steps)
    def _(step):
        first = step * SEQ_STEP

        def row(which, local, pair):
            return rows[which, pair, pl.ds(first + local, 1), :]

        state_load(step).wait()
        for local, pair, at in blocks:
            parts[2, at, :] = jnp.where(on_diagonal, row(5, local, pair), 0.0).astype(bf16)
            state = jnp.concatenate(
                [state_here[first + local, 2 * pair], state_here[first + local, 2 * pair + 1]], axis=1
            )
            joined[at, :] = state
            parts[0, at, :], parts[1, at, :] = two_parts(state * row(0, local, pair))
        sums[0] = jnp.dot(parts[0], ones, preferred_element_type=f32) + jnp.dot(
            parts[1], ones, preferred_element_type=f32
        )
        sums[1] = jnp.dot(parts[2], ones, preferred_element_type=f32)
        for local, pair, at in blocks:
            new = (
                joined[at, :] * row(1, local, pair)
                - sums[0, at, :] * row(2, local, pair)
                + sums[1, at, :] * row(3, local, pair)
            )
            new_here[first + local, 2 * pair] = new[:, 0:size]
            new_here[first + local, 2 * pair + 1] = new[:, size:pair_width]
            parts[0, at, :], parts[1, at, :] = two_parts(new * row(4, local, pair))
        state_store(step).start()
        dims = (((1,), (1,)), ((), ()))
        found = lax.dot_general(pick, parts[0], dims, preferred_element_type=f32) + lax.dot_general(
            pick, parts[1], dims, preferred_element_type=f32
        )
        for which in range(2):
            latest = read[which]
            for local in range(SEQ_STEP):
                line = found[
                    which * 8 : which * 8 + 1, local * pairs * size : (local + 1) * pairs * size
                ]
                latest = jnp.where(seq_of == first + local, line, latest)
            read[which] = latest

    mixed = []
    for pair in range(pairs):
        at = slice(pair * size, (pair + 1) * size)
        live = jnp.concatenate([read[0, :, at], read[1, :, at]], axis=1)
        live = live - head_sums(live) * (1.0 / size)
        spread = head_sums(jnp.square(live)) * (1.0 / size)
        gain = vectors[1, :, pair * pair_width : (pair + 1) * pair_width]
        mixed.append(live * lax.rsqrt(spread + GROUP_EPSILON) * gain)
    mixed = jnp.concatenate(mixed, axis=1).astype(bf16)
    weight_load.wait()
    product = jnp.dot(mixed, weight_here[...], preferred_element_type=f32).astype(bf16)
    for copy in range(copies):
        out_ref[copy] = product
    for step in range(steps):
        state_store(step).wait()


def heads_update(copies, state_in, receptance, key_in, value_in, learn_in, decay_in, decay_base, norm_gain, out_weight):
    seqs, heads, size, _ = state_in.shape
    width = out_weight.shape[1]
    channels = heads * size
    steps = seqs // SEQ_STEP
    step_rows = SEQ_STEP * heads // 2 * size
    any_space = pl.BlockSpec(memory_space=pl.ANY)
    new_state, product = pl.pallas_call(
        functools.partial(heads_kernel, copies),
        in_specs=[any_space] * 9,
        out_specs=[any_space, pl.BlockSpec(memory_space=pltpu.VMEM)],
        out_shape=[
            jax.ShapeDtypeStruct(state_in.shape, jnp.float32),
            pltpu.VMEM((copies, seqs, width), jnp.bfloat16),
        ],
        scratch_shapes=[
            pltpu.VMEM(state_in.shape, jnp.float32),
            pltpu.VMEM(state_in.shape, jnp.float32),
            pltpu.VMEM((4, seqs, channels), jnp.bfloat16),
            pltpu.VMEM((seqs, channels), jnp.float32),
            pltpu.VMEM((2, 1, channels), jnp.float32),
            pltpu.VMEM((channels, width), jnp.bfloat16),
            pltpu.VMEM((6, heads // 2, seqs, 2 * size), jnp.float32),
            pltpu.VMEM((2, seqs, channels // 2), jnp.float32),
            pltpu.VMEM((step_rows, 2 * size), jnp.float32),
            pltpu.VMEM((3, step_rows, 2 * size), jnp.bfloat16),
            pltpu.VMEM((2, step_rows, 2 * size), jnp.float32),
            pltpu.SemaphoreType.DMA((steps + 8,)),
            pltpu.SemaphoreType.DMA((steps,)),
        ],
        compiler_params=pltpu.CompilerParams(vmem_limit_bytes=60 << 20),
        cost_estimate=pl.CostEstimate(flops=20_000_000, bytes_accessed=5_000_000, transcendentals=20_000),
    )(
        state_in,
        receptance,
        key_in,
        value_in,
        learn_in,
        decay_in,
        decay_base.reshape(1, channels),
        norm_gain.reshape(1, channels),
        out_weight,
    )
    return product, new_state


def expert_kernel(got_ref, gate_ref, up_ref, down_ref, out_ref, flat):
    f32 = jnp.float32
    senders, n_y, rows, quarter = got_ref.shape
    for y in range(n_y):
        flat[:, y * quarter : (y + 1) * quarter] = got_ref[:, y].reshape(senders * rows, quarter)
    arrived = flat[...]
    gate = jnp.dot(arrived, gate_ref[0], preferred_element_type=f32)
    upward = jnp.dot(arrived, up_ref[0], preferred_element_type=f32)
    hidden = (gate * jax.nn.sigmoid(gate) * upward).astype(jnp.bfloat16)
    for y in range(n_y):
        partial = jnp.dot(
            hidden, down_ref[0, :, y * quarter : (y + 1) * quarter], preferred_element_type=f32
        )
        out_ref[:, y] = partial.astype(jnp.bfloat16).reshape(senders, rows, quarter)


def experts(got, expert_gate, expert_up, expert_down):
    senders, n_y, rows, quarter = got.shape
    vmem = pl.BlockSpec(memory_space=pltpu.VMEM)
    return pl.pallas_call(
        expert_kernel,
        in_specs=[vmem] * 4,
        out_specs=vmem,
        out_shape=jax.ShapeDtypeStruct(got.shape, jnp.bfloat16),
        scratch_shapes=[pltpu.VMEM((senders * rows, n_y * quarter), jnp.bfloat16)],
        compiler_params=pltpu.CompilerParams(vmem_limit_bytes=12 << 20),
        cost_estimate=pl.CostEstimate(flops=400_000_000, bytes_accessed=4_000_000, transcendentals=40_000),
    )(got, expert_gate, expert_up, expert_down)


def pack_kernel(
    arrived_ref, hidden_ref, gain_ref, ids_ref, weights_ref, parcels_ref, own_ref
):
    f32, bf16 = jnp.float32, jnp.bfloat16
    seqs, width = hidden_ref.shape
    quarter = own_ref.shape[1]
    top = ids_ref.shape[0]
    attention = jnp.sum(arrived_ref[...].astype(f32), axis=0).astype(bf16)
    residual = hidden_ref[...].astype(f32) + attention.astype(f32)
    scale = lax.rsqrt(jnp.mean(residual * residual, axis=1, keepdims=True) + EPSILON)
    at = pl.ds(pl.multiple_of(lax.axis_index("y") * quarter, quarter), quarter)
    attention = jnp.sum(arrived_ref[:, :, at].astype(f32), axis=0).astype(bf16)
    residual = hidden_ref[:, at].astype(f32) + attention.astype(f32)
    own_ref[...] = residual
    normed = (residual * scale * gain_ref[:, at]).astype(bf16)

    weights = weights_ref[...]
    routing = jnp.zeros((8, 128), f32)
    parts = [ids_ref[...].astype(f32)]
    for _ in range(3):
        part = weights.astype(bf16).astype(f32)
        parts.append(part)
        weights = weights - part
    routing = jnp.concatenate(
        [jnp.pad(part, ((0, 8 - top), (0, 0))) for part in parts]
        + [jnp.zeros((8, 128 - len(parts) * seqs), f32)],
        axis=1,
    ).astype(bf16)
    chunks = quarter // 128
    for z in range(parcels_ref.shape[0]):
        for chunk in range(chunks):
            parcels_ref[z, chunk * seqs : (chunk + 1) * seqs, :] = normed[
                :, chunk * 128 : (chunk + 1) * 128
            ]
        parcels_ref[z, chunks * seqs : chunks * seqs + 8, :] = routing


def pack(arrived, hidden_in, routed_gain, route_ids, route_weights, n_z):
    n_y, seqs, width = arrived.shape
    quarter = width // n_y
    vmem = pl.BlockSpec(memory_space=pltpu.VMEM)
    return pl.pallas_call(
        pack_kernel,
        in_specs=[vmem] * 5,
        out_specs=[vmem] * 2,
        out_shape=[
            jax.ShapeDtypeStruct((n_z, quarter // 128 * seqs + 8, 128), jnp.bfloat16),
            jax.ShapeDtypeStruct((seqs, quarter), jnp.float32),
        ],
        compiler_params=pltpu.CompilerParams(vmem_limit_bytes=8 << 20),
    )(arrived, hidden_in, routed_gain.reshape(1, width), route_ids.T, route_weights.T)


def choose_kernel(top, slots, rows_ref, chosen_ref, place_ref, weight_ref, flat, choice):
    f32, bf16 = jnp.float32, jnp.bfloat16
    n_z = rows_ref.shape[0]
    seqs = flat.shape[0] // n_z
    near, n_y, per_expert, piece = chosen_ref.shape
    tokens = n_z * seqs
    chunks = piece // 128
    sender_of = lax.broadcasted_iota(jnp.int32, (8, 128), 1) // seqs
    groups = tokens // 128
    per_group = 128 // seqs
    spread = [[jnp.zeros((8, 128), f32) for _ in range(groups)] for _ in range(4)]
    for z in range(n_z):
        for chunk in range(chunks):
            flat[z * seqs : (z + 1) * seqs, chunk * 128 : (chunk + 1) * 128] = rows_ref[
                z, chunk * seqs : (chunk + 1) * seqs, :
            ]
        routing = rows_ref[z, chunks * seqs : chunks * seqs + 8, :].astype(f32)
        group, place = divmod(z, per_group)
        for which in range(4):
            turn = (place - which) * seqs % 128
            moved = routing if turn == 0 else pltpu.roll(routing, turn, 1)
            spread[which][group] = jnp.where(sender_of == place, moved, spread[which][group])
    ids, high, middle, low = [jnp.concatenate(part, axis=1) for part in spread]
    weights = high + middle + low
    named = (
        lax.axis_index("zq") * near + lax.broadcasted_iota(jnp.int32, (near, tokens), 0)
    ).astype(f32)
    member = jnp.zeros((near, tokens), f32)
    weight = jnp.zeros((near, tokens), f32)
    for k in range(top):
        hit = named == ids[k : k + 1, :]
        member = jnp.where(hit, 1.0, member)
        weight = jnp.where(hit, weights[k : k + 1, :], weight)
    token = lax.broadcasted_iota(jnp.int32, (tokens, tokens), 0)
    other = lax.broadcasted_iota(jnp.int32, (tokens, tokens), 1)
    earlier = (token // seqs == other // seqs) & (token < other)
    rank = jnp.dot(member.astype(bf16), jnp.where(earlier, 1.0, 0.0).astype(bf16), preferred_element_type=f32)
    sender = (lax.broadcasted_iota(jnp.int32, (near, tokens), 1) // seqs * slots).astype(f32)
    place = jnp.where(member > 0, sender + rank, -1.0)
    place_ref[...] = place
    weight_ref[...] = weight
    row = lax.broadcasted_iota(jnp.int32, (per_expert, tokens), 0).astype(f32)
    for expert in range(near):
        choice[expert * per_expert : (expert + 1) * per_expert, :] = jnp.where(
            row == place[expert : expert + 1, :], 1.0, 0.0
        ).astype(bf16)
    chosen = jnp.dot(choice[...], flat[...], preferred_element_type=f32).astype(bf16)
    chosen = chosen.reshape(near, per_expert, piece)
    for y in range(n_y):
        chosen_ref[:, y] = chosen


def choose(rows, near, n_y, slots, top, seqs):
    n_z, depth, _ = rows.shape
    piece = (depth - 8) // seqs * 128
    tokens = n_z * seqs
    vmem = pl.BlockSpec(memory_space=pltpu.VMEM)
    return pl.pallas_call(
        functools.partial(choose_kernel, top, slots),
        in_specs=[vmem],
        out_specs=[vmem] * 3,
        out_shape=[
            jax.ShapeDtypeStruct((near, n_y, n_z * slots, piece), jnp.bfloat16),
            jax.ShapeDtypeStruct((near, tokens), jnp.float32),
            jax.ShapeDtypeStruct((near, tokens), jnp.float32),
        ],
        scratch_shapes=[
            pltpu.VMEM((tokens, piece), jnp.bfloat16),
            pltpu.VMEM((near * n_z * slots, tokens), jnp.bfloat16),
        ],
        compiler_params=pltpu.CompilerParams(vmem_limit_bytes=12 << 20),
    )(rows)


def combine_kernel(returned_ref, place_ref, weight_ref, out_ref, summed, choice):
    f32, bf16 = jnp.float32, jnp.bfloat16
    near, n_y, per_expert, piece = returned_ref.shape
    n_z, seqs, _ = out_ref.shape
    tokens = n_z * seqs
    total = near * per_expert
    row = lax.broadcasted_iota(jnp.int32, (per_expert, tokens), 0).astype(f32)
    for expert in range(near):
        at = slice(expert * per_expert, (expert + 1) * per_expert)
        result = jnp.sum(returned_ref[expert].astype(f32), axis=0).astype(bf16)
        summed[at, :] = result
        summed[total + expert * per_expert : total + (expert + 1) * per_expert, :] = result
        weight = jnp.where(
            row == place_ref[expert : expert + 1, :], weight_ref[expert : expert + 1, :], 0.0
        )
        high = weight.astype(bf16)
        choice[at, :] = high
        choice[total + expert * per_expert : total + (expert + 1) * per_expert, :] = (
            weight - high.astype(f32)
        ).astype(bf16)
    combined = lax.dot_general(
        choice[...], summed[...], (((0,), (0,)), ((), ())), preferred_element_type=f32
    )
    out_ref[...] = combined.astype(bf16).reshape(n_z, seqs, piece)


def combine(returned, place, weight, n_z):
    near, n_y, per_expert, piece = returned.shape
    tokens = place.shape[1]
    vmem = pl.BlockSpec(memory_space=pltpu.VMEM)
    return pl.pallas_call(
        combine_kernel,
        in_specs=[vmem] * 3,
        out_specs=vmem,
        out_shape=jax.ShapeDtypeStruct((n_z, tokens // n_z, piece), jnp.bfloat16),
        scratch_shapes=[
            pltpu.VMEM((2 * near * per_expert, piece), jnp.bfloat16),
            pltpu.VMEM((2 * near * per_expert, tokens), jnp.bfloat16),
        ],
        compiler_params=pltpu.CompilerParams(vmem_limit_bytes=12 << 20),
    )(returned, place, weight)


def on_device(
    hidden_in,
    state_in,
    receptance,
    key_in,
    value_in,
    learn_in,
    decay_in,
    decay_base,
    norm_gain,
    out_weight,
    routed_gain,
    expert_gate,
    expert_up,
    expert_down,
    route_ids,
    route_weights,
):
    n_y, n_zq = lax.axis_size("y"), lax.axis_size("zq")
    near = lax.axis_size(("zp", "x", "c"))
    seqs, width = hidden_in.shape
    quarter = width // n_y
    per_expert = n_zq * SLOTS

    product, new_state = heads_update(
        n_y, state_in, receptance, key_in, value_in, learn_in, decay_in, decay_base, norm_gain, out_weight
    )
    arrived = exchange(product, "y")
    parcels, own_residual = pack(arrived, hidden_in, routed_gain, route_ids, route_weights, n_zq)
    rows = exchange(parcels, "zq")
    chosen, place, weight = choose(rows, near, n_y, SLOTS, route_ids.shape[1], seqs)
    got = exchange(chosen.reshape(near * n_y, per_expert, quarter), NEAR_AXES)
    back = experts(got.reshape(near, n_y, per_expert, quarter), expert_gate, expert_up, expert_down)
    returned = exchange(back.reshape(near * n_y, per_expert, quarter), NEAR_AXES)
    combined = combine(returned.reshape(near, n_y, per_expert, quarter), place, weight, n_zq)
    routed = exchange(combined, "zq").astype(jnp.float32).sum(axis=0)
    result = (own_residual + routed).astype(jnp.bfloat16)
    spread = exchange(jnp.broadcast_to(result, (n_y, seqs, quarter)), "y")
    return (spread.transpose(1, 0, 2).reshape(seqs, width), new_state)


def solution(mesh):
    near_mesh = Mesh(mesh.devices.reshape(8, 2, 4, 2, 4), ("zq", "zp", "x", "c", "y"))
    in_specs = (
        P(EP, None),
        P(EP, "y", None, None),
        P(EP, "y"),
        P(EP, "y"),
        P(EP, "y"),
        P(EP, "y"),
        P(EP, "y"),
        P("y"),
        P("y"),
        P("y", None),
        P(),
        P(EP, None, "y"),
        P(EP, None, "y"),
        P(EP, "y", None),
        P(EP, None),
        P(EP, None),
    )
    out_specs = (P(EP, None), P(EP, "y", None, None))
    return jax.shard_map(
        on_device, mesh=near_mesh, in_specs=in_specs, out_specs=out_specs, check_vma=False
    )
```

```python
import functools
import math
import jax
import jax.numpy as jnp
import numpy as np
from jax import lax
from jax.experimental import pallas as pl
from jax.experimental.pallas import tpu as pltpu
from jax.sharding import Mesh, PartitionSpec as P

EPSILON = 1e-06
GROUP_EPSILON = 0.00064
SEQ_STEP = 8
SLOTS = 2
NEAR_AXES = ("zp", "x", "c", "y")
EP = ("zq", "zp", "x", "c")


def exchange(pieces, axes):
    return lax.all_to_all(pieces, axes, split_axis=0, concat_axis=0, tiled=True)


def two_parts(values):
    high = values.astype(jnp.bfloat16)
    return high, (values - high.astype(jnp.float32)).astype(jnp.bfloat16)


def heads_kernel(
    copies,
    state_ref,
    reading_ref,
    key_ref,
    value_ref,
    learn_ref,
    decay_ref,
    base_ref,
    gain_ref,
    weight_ref,
    new_state_ref,
    out_ref,
    state_here,
    new_here,
    inputs,
    decay_here,
    vectors,
    weight_here,
    rows,
    read,
    joined,
    parts,
    sums,
    arrived,
    stored,
):
    f32, bf16 = jnp.float32, jnp.bfloat16
    seqs, heads, size, _ = state_here.shape
    channels = heads * size
    pairs = heads // 2
    pair_width = 2 * size
    steps = seqs // SEQ_STEP

    def state_load(step):
        at = pl.ds(step * SEQ_STEP, SEQ_STEP)
        return pltpu.make_async_copy(state_ref.at[at], state_here.at[at], arrived.at[step])

    def state_store(step):
        at = pl.ds(step * SEQ_STEP, SEQ_STEP)
        return pltpu.make_async_copy(new_here.at[at], new_state_ref.at[at], stored.at[step])

    small = [
        pltpu.make_async_copy(source, target, arrived.at[steps + number])
        for number, (source, target) in enumerate(
            (
                (key_ref, inputs.at[0]),
                (learn_ref, inputs.at[1]),
                (decay_ref, decay_here),
                (base_ref, vectors.at[0]),
                (reading_ref, inputs.at[2]),
                (value_ref, inputs.at[3]),
                (gain_ref, vectors.at[1]),
            )
        )
    ]
    weight_load = pltpu.make_async_copy(weight_ref, weight_here, arrived.at[steps + len(small)])
    for load in small:
        load.start()
    for step in range(steps):
        state_load(step).start()
    weight_load.start()

    square = (pair_width, pair_width)
    same_head = (
        lax.broadcasted_iota(jnp.int32, square, 0) // size
        == lax.broadcasted_iota(jnp.int32, square, 1) // size
    )
    ones = jnp.where(same_head, 1.0, 0.0).astype(bf16)

    def head_sums(values):
        return sum(jnp.dot(part, ones, preferred_element_type=f32) for part in two_parts(values))

    for load in small:
        load.wait()
    keys = inputs[0].astype(f32)
    learning = jax.nn.sigmoid(inputs[1].astype(f32))
    decay = jnp.exp(-math.exp(-0.5) * jax.nn.sigmoid(vectors[0] + decay_here[...]))
    for pair in range(pairs):
        at = slice(pair * pair_width, (pair + 1) * pair_width)
        key = keys[:, at]
        unit = key * lax.rsqrt(head_sums(key * key) + EPSILON)
        rows[0, pair] = unit
        rows[1, pair] = decay[:, at]
        rows[2, pair] = unit * learning[:, at]
        rows[3, pair] = key
        rows[4, pair] = inputs[2, :, at].astype(f32)
        rows[5, pair] = inputs[3, :, at].astype(f32)

    blocks = [
        (local, pair, slice((local * pairs + pair) * size, (local * pairs + pair + 1) * size))
        for local in range(SEQ_STEP)
        for pair in range(pairs)
    ]
    on_diagonal = lax.broadcasted_iota(jnp.int32, (size, pair_width), 0) == (
        lax.broadcasted_iota(jnp.int32, (size, pair_width), 1) % size
    )
    head_of = lax.broadcasted_iota(jnp.int32, (2 * 8, pair_width), 0) // 8
    pick = jnp.where(
        head_of == lax.broadcasted_iota(jnp.int32, (2 * 8, pair_width), 1) // size, 1.0, 0.0
    ).astype(bf16)

    for step in range(steps):
        first = step * SEQ_STEP

        def row(which, local, pair):
            return rows[which, pair, first + local : first + local + 1, :]

        state_load(step).wait()
        for local, pair, at in blocks:
            parts[step, 2, at, :] = jnp.where(on_diagonal, row(5, local, pair), 0.0).astype(bf16)
            state = jnp.concatenate(
                [state_here[first + local, 2 * pair], state_here[first + local, 2 * pair + 1]], axis=1
            )
            joined[step, at, :] = state
            parts[step, 0, at, :], parts[step, 1, at, :] = two_parts(state * row(0, local, pair))
        sums[step, 0] = jnp.dot(parts[step, 0], ones, preferred_element_type=f32) + jnp.dot(
            parts[step, 1], ones, preferred_element_type=f32
        )
        sums[step, 1] = jnp.dot(parts[step, 2], ones, preferred_element_type=f32)
        for local, pair, at in blocks:
            new = (
                joined[step, at, :] * row(1, local, pair)
                - sums[step, 0, at, :] * row(2, local, pair)
                + sums[step, 1, at, :] * row(3, local, pair)
            )
            new_here[first + local, 2 * pair] = new[:, 0:size]
            new_here[first + local, 2 * pair + 1] = new[:, size:pair_width]
            parts[step, 0, at, :], parts[step, 1, at, :] = two_parts(new * row(4, local, pair))
        state_store(step).start()

    dims = (((1,), (1,)), ((), ()))
    lines = [[], []]
    for step in range(steps):
        found = lax.dot_general(pick, parts[step, 0], dims, preferred_element_type=f32)
        found += lax.dot_general(pick, parts[step, 1], dims, preferred_element_type=f32)
        for which in range(2):
            for local in range(SEQ_STEP):
                at = slice(local * pairs * size, (local + 1) * pairs * size)
                lines[which].append(found[which * 8 : which * 8 + 1, at])
    for which in range(2):
        read[which] = jnp.concatenate(lines[which], axis=0)

    mixed = []
    for pair in range(pairs):
        at = slice(pair * size, (pair + 1) * size)
        live = jnp.concatenate([read[0, :, at], read[1, :, at]], axis=1)
        live = live - head_sums(live) * (1.0 / size)
        spread = head_sums(jnp.square(live)) * (1.0 / size)
        gain = vectors[1, :, pair * pair_width : (pair + 1) * pair_width]
        mixed.append(live * lax.rsqrt(spread + GROUP_EPSILON) * gain)
    mixed = jnp.concatenate(mixed, axis=1).astype(bf16)
    weight_load.wait()
    product = jnp.dot(mixed, weight_here[...], preferred_element_type=f32).astype(bf16)
    for copy in range(copies):
        out_ref[copy] = product
    for step in range(steps):
        state_store(step).wait()


def heads_update(copies, state_in, receptance, key_in, value_in, learn_in, decay_in, decay_base, norm_gain, out_weight):
    seqs, heads, size, _ = state_in.shape
    width = out_weight.shape[1]
    channels = heads * size
    steps = seqs // SEQ_STEP
    step_rows = SEQ_STEP * heads // 2 * size
    any_space = pl.BlockSpec(memory_space=pl.ANY)
    new_state, product = pl.pallas_call(
        functools.partial(heads_kernel, copies),
        in_specs=[any_space] * 9,
        out_specs=[any_space, pl.BlockSpec(memory_space=pltpu.VMEM)],
        out_shape=[
            jax.ShapeDtypeStruct(state_in.shape, jnp.float32),
            pltpu.VMEM((copies, seqs, width), jnp.bfloat16),
        ],
        scratch_shapes=[
            pltpu.VMEM(state_in.shape, jnp.float32),
            pltpu.VMEM(state_in.shape, jnp.float32),
            pltpu.VMEM((4, seqs, channels), jnp.bfloat16),
            pltpu.VMEM((seqs, channels), jnp.float32),
            pltpu.VMEM((2, 1, channels), jnp.float32),
            pltpu.VMEM((channels, width), jnp.bfloat16),
            pltpu.VMEM((6, heads // 2, seqs, 2 * size), jnp.float32),
            pltpu.VMEM((2, seqs, channels // 2), jnp.float32),
            pltpu.VMEM((steps, step_rows, 2 * size), jnp.float32),
            pltpu.VMEM((steps, 3, step_rows, 2 * size), jnp.bfloat16),
            pltpu.VMEM((steps, 2, step_rows, 2 * size), jnp.float32),
            pltpu.SemaphoreType.DMA((steps + 8,)),
            pltpu.SemaphoreType.DMA((steps,)),
        ],
        compiler_params=pltpu.CompilerParams(vmem_limit_bytes=60 << 20),
        cost_estimate=pl.CostEstimate(flops=20_000_000, bytes_accessed=5_000_000, transcendentals=20_000),
    )(
        state_in,
        receptance,
        key_in,
        value_in,
        learn_in,
        decay_in,
        decay_base.reshape(1, channels),
        norm_gain.reshape(1, channels),
        out_weight,
    )
    return product, new_state


def expert_kernel(got_ref, gate_ref, up_ref, down_ref, out_ref, flat):
    f32 = jnp.float32
    senders, n_y, rows, quarter = got_ref.shape
    for y in range(n_y):
        flat[:, y * quarter : (y + 1) * quarter] = got_ref[:, y].reshape(senders * rows, quarter)
    units = gate_ref.shape[2]
    weights = jnp.concatenate([gate_ref[0], up_ref[0]], axis=1)
    half = senders * rows // 2
    hidden = []
    for first in (0, half):
        both = jnp.dot(flat[first : first + half], weights, preferred_element_type=f32)
        gate, upward = both[:, :units], both[:, units:]
        hidden.append((gate * jax.nn.sigmoid(gate) * upward).astype(jnp.bfloat16))
    hidden = jnp.concatenate(hidden, axis=0)
    for y in range(n_y):
        partial = jnp.dot(
            hidden, down_ref[0, :, y * quarter : (y + 1) * quarter], preferred_element_type=f32
        )
        out_ref[:, y] = partial.astype(jnp.bfloat16).reshape(senders, rows, quarter)


def experts(got, expert_gate, expert_up, expert_down):
    senders, n_y, rows, quarter = got.shape
    vmem = pl.BlockSpec(memory_space=pltpu.VMEM)
    return pl.pallas_call(
        expert_kernel,
        in_specs=[vmem] * 4,
        out_specs=vmem,
        out_shape=jax.ShapeDtypeStruct(got.shape, jnp.bfloat16),
        scratch_shapes=[pltpu.VMEM((senders * rows, n_y * quarter), jnp.bfloat16)],
        compiler_params=pltpu.CompilerParams(vmem_limit_bytes=12 << 20),
        cost_estimate=pl.CostEstimate(flops=400_000_000, bytes_accessed=4_000_000, transcendentals=40_000),
    )(got, expert_gate, expert_up, expert_down)


def pack_kernel(
    arrived_ref, hidden_ref, gain_ref, ids_ref, weights_ref, parcels_ref, own_ref
):
    f32, bf16 = jnp.float32, jnp.bfloat16
    seqs, width = hidden_ref.shape
    quarter = own_ref.shape[1]
    top = ids_ref.shape[0]
    attention = jnp.sum(arrived_ref[...].astype(f32), axis=0).astype(bf16)
    residual = hidden_ref[...].astype(f32) + attention.astype(f32)
    scale = lax.rsqrt(jnp.mean(residual * residual, axis=1, keepdims=True) + EPSILON)
    at = pl.ds(pl.multiple_of(lax.axis_index("y") * quarter, quarter), quarter)
    attention = jnp.sum(arrived_ref[:, :, at].astype(f32), axis=0).astype(bf16)
    residual = hidden_ref[:, at].astype(f32) + attention.astype(f32)
    own_ref[...] = residual
    normed = (residual * scale * gain_ref[:, at]).astype(bf16)

    weights = weights_ref[...]
    routing = jnp.zeros((8, 128), f32)
    parts = [ids_ref[...].astype(f32)]
    for _ in range(3):
        part = weights.astype(bf16).astype(f32)
        parts.append(part)
        weights = weights - part
    routing = jnp.concatenate(
        [jnp.pad(part, ((0, 8 - top), (0, 0))) for part in parts]
        + [jnp.zeros((8, 128 - len(parts) * seqs), f32)],
        axis=1,
    ).astype(bf16)
    chunks = quarter // 128
    for z in range(parcels_ref.shape[0]):
        for chunk in range(chunks):
            parcels_ref[z, chunk * seqs : (chunk + 1) * seqs, :] = normed[
                :, chunk * 128 : (chunk + 1) * 128
            ]
        parcels_ref[z, chunks * seqs : chunks * seqs + 8, :] = routing


def pack(arrived, hidden_in, routed_gain, route_ids, route_weights, n_z):
    n_y, seqs, width = arrived.shape
    quarter = width // n_y
    vmem = pl.BlockSpec(memory_space=pltpu.VMEM)
    return pl.pallas_call(
        pack_kernel,
        in_specs=[vmem] * 5,
        out_specs=[vmem] * 2,
        out_shape=[
            jax.ShapeDtypeStruct((n_z, quarter // 128 * seqs + 8, 128), jnp.bfloat16),
            jax.ShapeDtypeStruct((seqs, quarter), jnp.float32),
        ],
        compiler_params=pltpu.CompilerParams(vmem_limit_bytes=8 << 20),
    )(arrived, hidden_in, routed_gain.reshape(1, width), route_ids.T, route_weights.T)


def choose_kernel(top, slots, rows_ref, chosen_ref, place_ref, weight_ref, flat, choice):
    f32, bf16 = jnp.float32, jnp.bfloat16
    n_z = rows_ref.shape[0]
    seqs = flat.shape[0] // n_z
    near, n_y, per_expert, piece = chosen_ref.shape
    tokens = n_z * seqs
    chunks = piece // 128
    sender_of = lax.broadcasted_iota(jnp.int32, (8, 128), 1) // seqs
    groups = tokens // 128
    per_group = 128 // seqs
    spread = [[jnp.zeros((8, 128), f32) for _ in range(groups)] for _ in range(4)]
    for z in range(n_z):
        for chunk in range(chunks):
            flat[z * seqs : (z + 1) * seqs, chunk * 128 : (chunk + 1) * 128] = rows_ref[
                z, chunk * seqs : (chunk + 1) * seqs, :
            ]
        routing = rows_ref[z, chunks * seqs : chunks * seqs + 8, :].astype(f32)
        group, place = divmod(z, per_group)
        for which in range(4):
            turn = (place - which) * seqs % 128
            moved = routing if turn == 0 else pltpu.roll(routing, turn, 1)
            spread[which][group] = jnp.where(sender_of == place, moved, spread[which][group])
    ids, high, middle, low = [jnp.concatenate(part, axis=1) for part in spread]
    weights = high + middle + low
    named = (
        lax.axis_index("zq") * near + lax.broadcasted_iota(jnp.int32, (near, tokens), 0)
    ).astype(f32)
    member = jnp.zeros((near, tokens), f32)
    weight = jnp.zeros((near, tokens), f32)
    for k in range(top):
        hit = named == ids[k : k + 1, :]
        member = jnp.where(hit, 1.0, member)
        weight = jnp.where(hit, weights[k : k + 1, :], weight)
    token = lax.broadcasted_iota(jnp.int32, (tokens, tokens), 0)
    other = lax.broadcasted_iota(jnp.int32, (tokens, tokens), 1)
    earlier = (token // seqs == other // seqs) & (token < other)
    rank = jnp.dot(member.astype(bf16), jnp.where(earlier, 1.0, 0.0).astype(bf16), preferred_element_type=f32)
    sender = (lax.broadcasted_iota(jnp.int32, (near, tokens), 1) // seqs * slots).astype(f32)
    place = jnp.where(member > 0, sender + rank, -1.0)
    place_ref[...] = place
    weight_ref[...] = weight
    row = lax.broadcasted_iota(jnp.int32, (per_expert, tokens), 0).astype(f32)
    for expert in range(near):
        choice[expert * per_expert : (expert + 1) * per_expert, :] = jnp.where(
            row == place[expert : expert + 1, :], 1.0, 0.0
        ).astype(bf16)
    chosen = jnp.dot(choice[...], flat[...], preferred_element_type=f32).astype(bf16)
    chosen = chosen.reshape(near, per_expert, piece)
    for y in range(n_y):
        chosen_ref[:, y] = chosen


def choose(rows, near, n_y, slots, top, seqs):
    n_z, depth, _ = rows.shape
    piece = (depth - 8) // seqs * 128
    tokens = n_z * seqs
    vmem = pl.BlockSpec(memory_space=pltpu.VMEM)
    return pl.pallas_call(
        functools.partial(choose_kernel, top, slots),
        in_specs=[vmem],
        out_specs=[vmem] * 3,
        out_shape=[
            jax.ShapeDtypeStruct((near, n_y, n_z * slots, piece), jnp.bfloat16),
            jax.ShapeDtypeStruct((near, tokens), jnp.float32),
            jax.ShapeDtypeStruct((near, tokens), jnp.float32),
        ],
        scratch_shapes=[
            pltpu.VMEM((tokens, piece), jnp.bfloat16),
            pltpu.VMEM((near * n_z * slots, tokens), jnp.bfloat16),
        ],
        compiler_params=pltpu.CompilerParams(vmem_limit_bytes=12 << 20),
    )(rows)


def combine_kernel(returned_ref, place_ref, weight_ref, out_ref, summed, choice):
    f32, bf16 = jnp.float32, jnp.bfloat16
    near, n_y, per_expert, piece = returned_ref.shape
    n_z, seqs, _ = out_ref.shape
    tokens = n_z * seqs
    total = near * per_expert
    row = lax.broadcasted_iota(jnp.int32, (per_expert, tokens), 0).astype(f32)
    for expert in range(near):
        at = slice(expert * per_expert, (expert + 1) * per_expert)
        result = jnp.sum(returned_ref[expert].astype(f32), axis=0).astype(bf16)
        summed[at, :] = result
        summed[total + expert * per_expert : total + (expert + 1) * per_expert, :] = result
        weight = jnp.where(
            row == place_ref[expert : expert + 1, :], weight_ref[expert : expert + 1, :], 0.0
        )
        high = weight.astype(bf16)
        choice[at, :] = high
        choice[total + expert * per_expert : total + (expert + 1) * per_expert, :] = (
            weight - high.astype(f32)
        ).astype(bf16)
    combined = lax.dot_general(
        choice[...], summed[...], (((0,), (0,)), ((), ())), preferred_element_type=f32
    )
    out_ref[...] = combined.astype(bf16).reshape(n_z, seqs, piece)


def combine(returned, place, weight, n_z):
    near, n_y, per_expert, piece = returned.shape
    tokens = place.shape[1]
    vmem = pl.BlockSpec(memory_space=pltpu.VMEM)
    return pl.pallas_call(
        combine_kernel,
        in_specs=[vmem] * 3,
        out_specs=vmem,
        out_shape=jax.ShapeDtypeStruct((n_z, tokens // n_z, piece), jnp.bfloat16),
        scratch_shapes=[
            pltpu.VMEM((2 * near * per_expert, piece), jnp.bfloat16),
            pltpu.VMEM((2 * near * per_expert, tokens), jnp.bfloat16),
        ],
        compiler_params=pltpu.CompilerParams(vmem_limit_bytes=12 << 20),
    )(returned, place, weight)


def on_device(
    hidden_in,
    state_in,
    receptance,
    key_in,
    value_in,
    learn_in,
    decay_in,
    decay_base,
    norm_gain,
    out_weight,
    routed_gain,
    expert_gate,
    expert_up,
    expert_down,
    route_ids,
    route_weights,
):
    n_y, n_zq = lax.axis_size("y"), lax.axis_size("zq")
    near = lax.axis_size(("zp", "x", "c"))
    seqs, width = hidden_in.shape
    quarter = width // n_y
    per_expert = n_zq * SLOTS

    product, new_state = heads_update(
        n_y, state_in, receptance, key_in, value_in, learn_in, decay_in, decay_base, norm_gain, out_weight
    )
    arrived = exchange(product, "y")
    parcels, own_residual = pack(arrived, hidden_in, routed_gain, route_ids, route_weights, n_zq)
    rows = exchange(parcels, "zq")
    chosen, place, weight = choose(rows, near, n_y, SLOTS, route_ids.shape[1], seqs)
    got = exchange(chosen.reshape(near * n_y, per_expert, quarter), NEAR_AXES)
    back = experts(got.reshape(near, n_y, per_expert, quarter), expert_gate, expert_up, expert_down)
    returned = exchange(back.reshape(near * n_y, per_expert, quarter), NEAR_AXES)
    combined = combine(returned.reshape(near, n_y, per_expert, quarter), place, weight, n_zq)
    routed = exchange(combined, "zq").astype(jnp.float32).sum(axis=0)
    result = (own_residual + routed).astype(jnp.bfloat16)
    spread = exchange(jnp.broadcast_to(result, (n_y, seqs, quarter)), "y")
    return (spread.transpose(1, 0, 2).reshape(seqs, width), new_state)


def solution(mesh):
    near_mesh = Mesh(mesh.devices.reshape(8, 2, 4, 2, 4), ("zq", "zp", "x", "c", "y"))
    in_specs = (
        P(EP, None),
        P(EP, "y", None, None),
        P(EP, "y"),
        P(EP, "y"),
        P(EP, "y"),
        P(EP, "y"),
        P(EP, "y"),
        P("y"),
        P("y"),
        P("y", None),
        P(),
        P(EP, None, "y"),
        P(EP, None, "y"),
        P(EP, "y", None),
        P(EP, None),
        P(EP, None),
    )
    out_specs = (P(EP, None), P(EP, "y", None, None))
    return jax.shard_map(
        on_device, mesh=near_mesh, in_specs=in_specs, out_specs=out_specs, check_vma=False
    )
```

```python
import functools
import math
import jax
import jax.numpy as jnp
import numpy as np
from jax import lax
from jax.experimental import pallas as pl
from jax.experimental.pallas import tpu as pltpu
from jax.sharding import Mesh, PartitionSpec as P

EPSILON = 1e-06
GROUP_EPSILON = 0.00064
SEQ_STEP = 8
SLOTS = 2
NEAR_AXES = ("zp", "x", "c", "y")
EP = ("zq", "zp", "x", "c")


def exchange(pieces, axes):
    return lax.all_to_all(pieces, axes, split_axis=0, concat_axis=0, tiled=True)


def two_parts(values):
    high = values.astype(jnp.bfloat16)
    return high, (values - high.astype(jnp.float32)).astype(jnp.bfloat16)


def heads_kernel(
    owners,
    state_ref,
    reading_ref,
    key_ref,
    value_ref,
    learn_ref,
    decay_ref,
    base_ref,
    gain_ref,
    weight_ref,
    new_state_ref,
    out_ref,
    state_here,
    new_here,
    inputs,
    decay_here,
    vectors,
    weight_here,
    rows,
    read,
    joined,
    parts,
    sums,
    arrived,
    stored,
):
    f32, bf16 = jnp.float32, jnp.bfloat16
    seqs, heads, size, _ = state_here.shape
    channels = heads * size
    pairs = heads // 2
    pair_width = 2 * size
    steps = seqs // SEQ_STEP

    def state_load(step):
        at = pl.ds(step * SEQ_STEP, SEQ_STEP)
        return pltpu.make_async_copy(state_ref.at[at], state_here.at[at], arrived.at[step])

    def state_store(step):
        at = pl.ds(step * SEQ_STEP, SEQ_STEP)
        return pltpu.make_async_copy(new_here.at[at], new_state_ref.at[at], stored.at[step])

    small = [
        pltpu.make_async_copy(source, target, arrived.at[steps + number])
        for number, (source, target) in enumerate(
            (
                (key_ref, inputs.at[0]),
                (learn_ref, inputs.at[1]),
                (decay_ref, decay_here),
                (base_ref, vectors.at[0]),
                (reading_ref, inputs.at[2]),
                (value_ref, inputs.at[3]),
                (gain_ref, vectors.at[1]),
            )
        )
    ]
    weight_load = pltpu.make_async_copy(weight_ref, weight_here, arrived.at[steps + len(small)])
    for load in small:
        load.start()
    for step in range(steps):
        state_load(step).start()
    weight_load.start()

    square = (pair_width, pair_width)
    same_head = (
        lax.broadcasted_iota(jnp.int32, square, 0) // size
        == lax.broadcasted_iota(jnp.int32, square, 1) // size
    )
    ones = jnp.where(same_head, 1.0, 0.0).astype(bf16)

    def head_sums(values):
        return sum(jnp.dot(part, ones, preferred_element_type=f32) for part in two_parts(values))

    for load in small:
        load.wait()
    keys = inputs[0].astype(f32)
    learning = jax.nn.sigmoid(inputs[1].astype(f32))
    decay = jnp.exp(-math.exp(-0.5) * jax.nn.sigmoid(vectors[0] + decay_here[...]))
    for pair in range(pairs):
        at = slice(pair * pair_width, (pair + 1) * pair_width)
        key = keys[:, at]
        unit = key * lax.rsqrt(head_sums(key * key) + EPSILON)
        rows[0, pair] = unit
        rows[1, pair] = decay[:, at]
        rows[2, pair] = unit * learning[:, at]
        rows[3, pair] = key
        rows[4, pair] = inputs[2, :, at].astype(f32)
        rows[5, pair] = inputs[3, :, at].astype(f32)

    blocks = [
        (local, pair, slice((local * pairs + pair) * size, (local * pairs + pair + 1) * size))
        for local in range(SEQ_STEP)
        for pair in range(pairs)
    ]
    on_diagonal = lax.broadcasted_iota(jnp.int32, (size, pair_width), 0) == (
        lax.broadcasted_iota(jnp.int32, (size, pair_width), 1) % size
    )
    head_of = lax.broadcasted_iota(jnp.int32, (2 * 8, pair_width), 0) // 8
    pick = jnp.where(
        head_of == lax.broadcasted_iota(jnp.int32, (2 * 8, pair_width), 1) // size, 1.0, 0.0
    ).astype(bf16)

    for step in range(steps):
        first = step * SEQ_STEP

        def row(which, local, pair):
            return rows[which, pair, first + local : first + local + 1, :]

        state_load(step).wait()
        for local, pair, at in blocks:
            parts[step, 2, at, :] = jnp.where(on_diagonal, row(5, local, pair), 0.0).astype(bf16)
            state = jnp.concatenate(
                [state_here[first + local, 2 * pair], state_here[first + local, 2 * pair + 1]], axis=1
            )
            joined[step, at, :] = state
            parts[step, 0, at, :], parts[step, 1, at, :] = two_parts(state * row(0, local, pair))
        sums[step, 0] = jnp.dot(parts[step, 0], ones, preferred_element_type=f32) + jnp.dot(
            parts[step, 1], ones, preferred_element_type=f32
        )
        sums[step, 1] = jnp.dot(parts[step, 2], ones, preferred_element_type=f32)
        for local, pair, at in blocks:
            new = (
                joined[step, at, :] * row(1, local, pair)
                - sums[step, 0, at, :] * row(2, local, pair)
                + sums[step, 1, at, :] * row(3, local, pair)
            )
            new_here[first + local, 2 * pair] = new[:, 0:size]
            new_here[first + local, 2 * pair + 1] = new[:, size:pair_width]
            parts[step, 0, at, :], parts[step, 1, at, :] = two_parts(new * row(4, local, pair))
        state_store(step).start()

    dims = (((1,), (1,)), ((), ()))
    lines = [[], []]
    for step in range(steps):
        found = lax.dot_general(pick, parts[step, 0], dims, preferred_element_type=f32)
        found += lax.dot_general(pick, parts[step, 1], dims, preferred_element_type=f32)
        for which in range(2):
            for local in range(SEQ_STEP):
                at = slice(local * pairs * size, (local + 1) * pairs * size)
                lines[which].append(found[which * 8 : which * 8 + 1, at])
    for which in range(2):
        read[which] = jnp.concatenate(lines[which], axis=0)

    mixed = []
    for pair in range(pairs):
        at = slice(pair * size, (pair + 1) * size)
        live = jnp.concatenate([read[0, :, at], read[1, :, at]], axis=1)
        live = live - head_sums(live) * (1.0 / size)
        spread = head_sums(jnp.square(live)) * (1.0 / size)
        gain = vectors[1, :, pair * pair_width : (pair + 1) * pair_width]
        mixed.append(live * lax.rsqrt(spread + GROUP_EPSILON) * gain)
    mixed = jnp.concatenate(mixed, axis=1).astype(bf16)
    weight_load.wait()
    product = jnp.dot(mixed, weight_here[...], preferred_element_type=f32).astype(bf16)
    quarter = out_ref.shape[2]
    for owner in range(owners):
        out_ref[owner] = product[:, owner * quarter : (owner + 1) * quarter]
    for step in range(steps):
        state_store(step).wait()


def heads_update(owners, state_in, receptance, key_in, value_in, learn_in, decay_in, decay_base, norm_gain, out_weight):
    seqs, heads, size, _ = state_in.shape
    width = out_weight.shape[1]
    channels = heads * size
    steps = seqs // SEQ_STEP
    step_rows = SEQ_STEP * heads // 2 * size
    any_space = pl.BlockSpec(memory_space=pl.ANY)
    new_state, product = pl.pallas_call(
        functools.partial(heads_kernel, owners),
        in_specs=[any_space] * 9,
        out_specs=[any_space, pl.BlockSpec(memory_space=pltpu.VMEM)],
        out_shape=[
            jax.ShapeDtypeStruct(state_in.shape, jnp.float32),
            pltpu.VMEM((owners, seqs, width // owners), jnp.bfloat16),
        ],
        scratch_shapes=[
            pltpu.VMEM(state_in.shape, jnp.float32),
            pltpu.VMEM(state_in.shape, jnp.float32),
            pltpu.VMEM((4, seqs, channels), jnp.bfloat16),
            pltpu.VMEM((seqs, channels), jnp.float32),
            pltpu.VMEM((2, 1, channels), jnp.float32),
            pltpu.VMEM((channels, width), jnp.bfloat16),
            pltpu.VMEM((6, heads // 2, seqs, 2 * size), jnp.float32),
            pltpu.VMEM((2, seqs, channels // 2), jnp.float32),
            pltpu.VMEM((steps, step_rows, 2 * size), jnp.float32),
            pltpu.VMEM((steps, 3, step_rows, 2 * size), jnp.bfloat16),
            pltpu.VMEM((steps, 2, step_rows, 2 * size), jnp.float32),
            pltpu.SemaphoreType.DMA((steps + 8,)),
            pltpu.SemaphoreType.DMA((steps,)),
        ],
        compiler_params=pltpu.CompilerParams(vmem_limit_bytes=60 << 20),
        cost_estimate=pl.CostEstimate(flops=20_000_000, bytes_accessed=5_000_000, transcendentals=20_000),
    )(
        state_in,
        receptance,
        key_in,
        value_in,
        learn_in,
        decay_in,
        decay_base.reshape(1, channels),
        norm_gain.reshape(1, channels),
        out_weight,
    )
    return product, new_state


def expert_kernel(got_ref, gain_ref, gate_ref, up_ref, down_ref, out_ref, flat):
    f32 = jnp.float32
    senders, n_y, rows, quarter = got_ref.shape
    power = jnp.zeros((senders * rows, 128), f32)
    for y in range(n_y):
        flat[:, y * quarter : (y + 1) * quarter] = got_ref[:, y].reshape(senders * rows, quarter)
        for first in range(y * quarter, (y + 1) * quarter, 128):
            at = slice(first, first + 128)
            original = flat[:, at].astype(f32) * (1.0 / gain_ref[:, at])
            power += original * original
    mean = jnp.sum(power, axis=1, keepdims=True) * (1.0 / (n_y * quarter))
    scale = lax.rsqrt(mean + EPSILON)
    units = gate_ref.shape[2]
    weights = jnp.concatenate([gate_ref[0], up_ref[0]], axis=1)
    half = senders * rows // 2
    hidden = []
    for first in (0, half):
        both = jnp.dot(flat[first : first + half], weights, preferred_element_type=f32)
        both = both * scale[first : first + half]
        gate, upward = both[:, :units], both[:, units:]
        hidden.append((gate * jax.nn.sigmoid(gate) * upward).astype(jnp.bfloat16))
    hidden = jnp.concatenate(hidden, axis=0)
    for y in range(n_y):
        partial = jnp.dot(
            hidden, down_ref[0, :, y * quarter : (y + 1) * quarter], preferred_element_type=f32
        )
        out_ref[:, y] = partial.astype(jnp.bfloat16).reshape(senders, rows, quarter)


def experts(got, routed_gain, expert_gate, expert_up, expert_down):
    senders, n_y, rows, quarter = got.shape
    vmem = pl.BlockSpec(memory_space=pltpu.VMEM)
    return pl.pallas_call(
        expert_kernel,
        in_specs=[vmem] * 5,
        out_specs=vmem,
        out_shape=jax.ShapeDtypeStruct(got.shape, jnp.bfloat16),
        scratch_shapes=[pltpu.VMEM((senders * rows, n_y * quarter), jnp.bfloat16)],
        compiler_params=pltpu.CompilerParams(vmem_limit_bytes=12 << 20),
        cost_estimate=pl.CostEstimate(flops=400_000_000, bytes_accessed=4_000_000, transcendentals=40_000),
    )(got, routed_gain.reshape(1, n_y * quarter), expert_gate, expert_up, expert_down)


def pack_kernel(
    arrived_ref, hidden_ref, gain_ref, ids_ref, weights_ref, parcels_ref, own_ref
):
    f32, bf16 = jnp.float32, jnp.bfloat16
    seqs, quarter = own_ref.shape
    top = ids_ref.shape[0]
    at = pl.ds(pl.multiple_of(lax.axis_index("y") * quarter, quarter), quarter)
    attention = jnp.sum(arrived_ref[...].astype(f32), axis=0).astype(bf16)
    residual = hidden_ref[:, at].astype(f32) + attention.astype(f32)
    own_ref[...] = residual
    gained = (residual * gain_ref[:, at]).astype(bf16)

    weights = weights_ref[...]
    routing = jnp.zeros((8, 128), f32)
    parts = [ids_ref[...].astype(f32)]
    for _ in range(3):
        part = weights.astype(bf16).astype(f32)
        parts.append(part)
        weights = weights - part
    routing = jnp.concatenate(
        [jnp.pad(part, ((0, 8 - top), (0, 0))) for part in parts]
        + [jnp.zeros((8, 128 - len(parts) * seqs), f32)],
        axis=1,
    ).astype(bf16)
    chunks = quarter // 128
    for z in range(parcels_ref.shape[0]):
        for chunk in range(chunks):
            parcels_ref[z, chunk * seqs : (chunk + 1) * seqs, :] = gained[
                :, chunk * 128 : (chunk + 1) * 128
            ]
        parcels_ref[z, chunks * seqs : chunks * seqs + 8, :] = routing


def pack(arrived, hidden_in, routed_gain, route_ids, route_weights, n_z):
    n_y, seqs, quarter = arrived.shape
    width = n_y * quarter
    vmem = pl.BlockSpec(memory_space=pltpu.VMEM)
    return pl.pallas_call(
        pack_kernel,
        in_specs=[vmem] * 5,
        out_specs=[vmem] * 2,
        out_shape=[
            jax.ShapeDtypeStruct((n_z, quarter // 128 * seqs + 8, 128), jnp.bfloat16),
            jax.ShapeDtypeStruct((seqs, quarter), jnp.float32),
        ],
        compiler_params=pltpu.CompilerParams(vmem_limit_bytes=8 << 20),
    )(arrived, hidden_in, routed_gain.reshape(1, width), route_ids.T, route_weights.T)


def choose_kernel(top, slots, rows_ref, chosen_ref, place_ref, weight_ref, flat, choice):
    f32, bf16 = jnp.float32, jnp.bfloat16
    n_z = rows_ref.shape[0]
    seqs = flat.shape[0] // n_z
    near, n_y, per_expert, piece = chosen_ref.shape
    tokens = n_z * seqs
    chunks = piece // 128
    sender_of = lax.broadcasted_iota(jnp.int32, (8, 128), 1) // seqs
    groups = tokens // 128
    per_group = 128 // seqs
    spread = [[jnp.zeros((8, 128), f32) for _ in range(groups)] for _ in range(4)]
    for z in range(n_z):
        for chunk in range(chunks):
            flat[z * seqs : (z + 1) * seqs, chunk * 128 : (chunk + 1) * 128] = rows_ref[
                z, chunk * seqs : (chunk + 1) * seqs, :
            ]
        routing = rows_ref[z, chunks * seqs : chunks * seqs + 8, :].astype(f32)
        group, place = divmod(z, per_group)
        for which in range(4):
            turn = (place - which) * seqs % 128
            moved = routing if turn == 0 else pltpu.roll(routing, turn, 1)
            spread[which][group] = jnp.where(sender_of == place, moved, spread[which][group])
    ids, high, middle, low = [jnp.concatenate(part, axis=1) for part in spread]
    weights = high + middle + low
    named = (
        lax.axis_index("zq") * near + lax.broadcasted_iota(jnp.int32, (near, tokens), 0)
    ).astype(f32)
    member = jnp.zeros((near, tokens), f32)
    weight = jnp.zeros((near, tokens), f32)
    for k in range(top):
        hit = named == ids[k : k + 1, :]
        member = jnp.where(hit, 1.0, member)
        weight = jnp.where(hit, weights[k : k + 1, :], weight)
    token = lax.broadcasted_iota(jnp.int32, (tokens, tokens), 0)
    other = lax.broadcasted_iota(jnp.int32, (tokens, tokens), 1)
    earlier = (token // seqs == other // seqs) & (token < other)
    rank = jnp.dot(member.astype(bf16), jnp.where(earlier, 1.0, 0.0).astype(bf16), preferred_element_type=f32)
    sender = (lax.broadcasted_iota(jnp.int32, (near, tokens), 1) // seqs * slots).astype(f32)
    place = jnp.where(member > 0, sender + rank, -1.0)
    place_ref[...] = place
    weight_ref[...] = weight
    row = lax.broadcasted_iota(jnp.int32, (per_expert, tokens), 0).astype(f32)
    for expert in range(near):
        choice[expert * per_expert : (expert + 1) * per_expert, :] = jnp.where(
            row == place[expert : expert + 1, :], 1.0, 0.0
        ).astype(bf16)
    chosen = jnp.dot(choice[...], flat[...], preferred_element_type=f32).astype(bf16)
    chosen = chosen.reshape(near, per_expert, piece)
    for y in range(n_y):
        chosen_ref[:, y] = chosen


def choose(rows, near, n_y, slots, top, seqs):
    n_z, depth, _ = rows.shape
    piece = (depth - 8) // seqs * 128
    tokens = n_z * seqs
    vmem = pl.BlockSpec(memory_space=pltpu.VMEM)
    return pl.pallas_call(
        functools.partial(choose_kernel, top, slots),
        in_specs=[vmem],
        out_specs=[vmem] * 3,
        out_shape=[
            jax.ShapeDtypeStruct((near, n_y, n_z * slots, piece), jnp.bfloat16),
            jax.ShapeDtypeStruct((near, tokens), jnp.float32),
            jax.ShapeDtypeStruct((near, tokens), jnp.float32),
        ],
        scratch_shapes=[
            pltpu.VMEM((tokens, piece), jnp.bfloat16),
            pltpu.VMEM((near * n_z * slots, tokens), jnp.bfloat16),
        ],
        compiler_params=pltpu.CompilerParams(vmem_limit_bytes=12 << 20),
    )(rows)


def combine_kernel(returned_ref, place_ref, weight_ref, out_ref, summed, choice):
    f32, bf16 = jnp.float32, jnp.bfloat16
    near, n_y, per_expert, piece = returned_ref.shape
    n_z, seqs, _ = out_ref.shape
    tokens = n_z * seqs
    total = near * per_expert
    row = lax.broadcasted_iota(jnp.int32, (per_expert, tokens), 0).astype(f32)
    for expert in range(near):
        at = slice(expert * per_expert, (expert + 1) * per_expert)
        result = jnp.sum(returned_ref[expert].astype(f32), axis=0).astype(bf16)
        summed[at, :] = result
        summed[total + expert * per_expert : total + (expert + 1) * per_expert, :] = result
        weight = jnp.where(
            row == place_ref[expert : expert + 1, :], weight_ref[expert : expert + 1, :], 0.0
        )
        high = weight.astype(bf16)
        choice[at, :] = high
        choice[total + expert * per_expert : total + (expert + 1) * per_expert, :] = (
            weight - high.astype(f32)
        ).astype(bf16)
    combined = lax.dot_general(
        choice[...], summed[...], (((0,), (0,)), ((), ())), preferred_element_type=f32
    )
    out_ref[...] = combined.astype(bf16).reshape(n_z, seqs, piece)


def combine(returned, place, weight, n_z):
    near, n_y, per_expert, piece = returned.shape
    tokens = place.shape[1]
    vmem = pl.BlockSpec(memory_space=pltpu.VMEM)
    return pl.pallas_call(
        combine_kernel,
        in_specs=[vmem] * 3,
        out_specs=vmem,
        out_shape=jax.ShapeDtypeStruct((n_z, tokens // n_z, piece), jnp.bfloat16),
        scratch_shapes=[
            pltpu.VMEM((2 * near * per_expert, piece), jnp.bfloat16),
            pltpu.VMEM((2 * near * per_expert, tokens), jnp.bfloat16),
        ],
        compiler_params=pltpu.CompilerParams(vmem_limit_bytes=12 << 20),
    )(returned, place, weight)


def on_device(
    hidden_in,
    state_in,
    receptance,
    key_in,
    value_in,
    learn_in,
    decay_in,
    decay_base,
    norm_gain,
    out_weight,
    routed_gain,
    expert_gate,
    expert_up,
    expert_down,
    route_ids,
    route_weights,
):
    n_y, n_zq = lax.axis_size("y"), lax.axis_size("zq")
    near = lax.axis_size(("zp", "x", "c"))
    seqs, width = hidden_in.shape
    quarter = width // n_y
    per_expert = n_zq * SLOTS

    product, new_state = heads_update(
        n_y, state_in, receptance, key_in, value_in, learn_in, decay_in, decay_base, norm_gain, out_weight
    )
    arrived = exchange(product, "y")
    parcels, own_residual = pack(arrived, hidden_in, routed_gain, route_ids, route_weights, n_zq)
    rows = exchange(parcels, "zq")
    chosen, place, weight = choose(rows, near, n_y, SLOTS, route_ids.shape[1], seqs)
    got = exchange(chosen.reshape(near * n_y, per_expert, quarter), NEAR_AXES)
    back = experts(got.reshape(near, n_y, per_expert, quarter), routed_gain, expert_gate, expert_up, expert_down)
    returned = exchange(back.reshape(near * n_y, per_expert, quarter), NEAR_AXES)
    combined = combine(returned.reshape(near, n_y, per_expert, quarter), place, weight, n_zq)
    routed = exchange(combined, "zq").astype(jnp.float32).sum(axis=0)
    result = (own_residual + routed).astype(jnp.bfloat16)
    spread = exchange(jnp.broadcast_to(result, (n_y, seqs, quarter)), "y")
    return (spread.transpose(1, 0, 2).reshape(seqs, width), new_state)


def solution(mesh):
    near_mesh = Mesh(mesh.devices.reshape(8, 2, 4, 2, 4), ("zq", "zp", "x", "c", "y"))
    in_specs = (
        P(EP, None),
        P(EP, "y", None, None),
        P(EP, "y"),
        P(EP, "y"),
        P(EP, "y"),
        P(EP, "y"),
        P(EP, "y"),
        P("y"),
        P("y"),
        P("y", None),
        P(),
        P(EP, None, "y"),
        P(EP, None, "y"),
        P(EP, "y", None),
        P(EP, None),
        P(EP, None),
    )
    out_specs = (P(EP, None), P(EP, "y", None, None))
    return jax.shard_map(
        on_device, mesh=near_mesh, in_specs=in_specs, out_specs=out_specs, check_vma=False
    )
```

```python
import functools
import math
import jax
import jax.numpy as jnp
import numpy as np
from jax import lax
from jax.experimental import pallas as pl
from jax.experimental.pallas import tpu as pltpu
from jax.sharding import Mesh, PartitionSpec as P

EPSILON = 1e-06
GROUP_EPSILON = 0.00064
SEQ_STEP = 8
SLOTS = 2
NEAR_AXES = ("zp", "x", "c", "y")
EP = ("zq", "zp", "x", "c")


def exchange(pieces, axes):
    return lax.all_to_all(pieces, axes, split_axis=0, concat_axis=0, tiled=True)


def two_parts(values):
    high = values.astype(jnp.bfloat16)
    return high, (values - high.astype(jnp.float32)).astype(jnp.bfloat16)


def heads_kernel(
    owners,
    state_ref,
    reading_ref,
    key_ref,
    value_ref,
    learn_ref,
    decay_ref,
    base_ref,
    gain_ref,
    weight_ref,
    new_state_ref,
    out_ref,
    late_ref,
    state_here,
    early,
    inputs,
    decay_here,
    vectors,
    weight_here,
    rows,
    read,
    joined,
    parts,
    sums,
    arrived,
    stored,
):
    f32, bf16 = jnp.float32, jnp.bfloat16
    seqs, heads, size, _ = state_here.shape
    channels = heads * size
    pairs = heads // 2
    pair_width = 2 * size
    steps = 2

    def state_load(step):
        at = pl.ds(step * SEQ_STEP, SEQ_STEP)
        return pltpu.make_async_copy(state_ref.at[at], state_here.at[at], arrived.at[step])

    store = pltpu.make_async_copy(early, new_state_ref.at[pl.ds(0, SEQ_STEP)], stored)

    small = [
        pltpu.make_async_copy(source, target, arrived.at[steps + number])
        for number, (source, target) in enumerate(
            (
                (key_ref, inputs.at[0]),
                (learn_ref, inputs.at[1]),
                (decay_ref, decay_here),
                (base_ref, vectors.at[0]),
                (reading_ref, inputs.at[2]),
                (value_ref, inputs.at[3]),
                (gain_ref, vectors.at[1]),
            )
        )
    ]
    weight_load = pltpu.make_async_copy(weight_ref, weight_here, arrived.at[steps + len(small)])
    for load in small:
        load.start()
    for step in range(steps):
        state_load(step).start()
    weight_load.start()

    square = (pair_width, pair_width)
    same_head = (
        lax.broadcasted_iota(jnp.int32, square, 0) // size
        == lax.broadcasted_iota(jnp.int32, square, 1) // size
    )
    ones = jnp.where(same_head, 1.0, 0.0).astype(bf16)

    def head_sums(values):
        return sum(jnp.dot(part, ones, preferred_element_type=f32) for part in two_parts(values))

    for load in small:
        load.wait()
    keys = inputs[0].astype(f32)
    learning = jax.nn.sigmoid(inputs[1].astype(f32))
    decay = jnp.exp(-math.exp(-0.5) * jax.nn.sigmoid(vectors[0] + decay_here[...]))
    for pair in range(pairs):
        at = slice(pair * pair_width, (pair + 1) * pair_width)
        key = keys[:, at]
        unit = key * lax.rsqrt(head_sums(key * key) + EPSILON)
        rows[0, pair] = unit
        rows[1, pair] = decay[:, at]
        rows[2, pair] = unit * learning[:, at]
        rows[3, pair] = key
        rows[4, pair] = inputs[2, :, at].astype(f32)
        rows[5, pair] = inputs[3, :, at].astype(f32)

    blocks = [
        (local, pair, slice((local * pairs + pair) * size, (local * pairs + pair + 1) * size))
        for local in range(SEQ_STEP)
        for pair in range(pairs)
    ]
    on_diagonal = lax.broadcasted_iota(jnp.int32, (size, pair_width), 0) == (
        lax.broadcasted_iota(jnp.int32, (size, pair_width), 1) % size
    )
    head_of = lax.broadcasted_iota(jnp.int32, (2 * 8, pair_width), 0) // 8
    pick = jnp.where(
        head_of == lax.broadcasted_iota(jnp.int32, (2 * 8, pair_width), 1) // size, 1.0, 0.0
    ).astype(bf16)

    for step in range(steps):
        first = step * SEQ_STEP

        def row(which, local, pair):
            return rows[which, pair, first + local : first + local + 1, :]

        state_load(step).wait()
        for local, pair, at in blocks:
            parts[step, 2, at, :] = jnp.where(on_diagonal, row(5, local, pair), 0.0).astype(bf16)
            state = jnp.concatenate(
                [state_here[first + local, 2 * pair], state_here[first + local, 2 * pair + 1]], axis=1
            )
            joined[step, at, :] = state
            parts[step, 0, at, :], parts[step, 1, at, :] = two_parts(state * row(0, local, pair))
        sums[step, 0] = jnp.dot(parts[step, 0], ones, preferred_element_type=f32) + jnp.dot(
            parts[step, 1], ones, preferred_element_type=f32
        )
        sums[step, 1] = jnp.dot(parts[step, 2], ones, preferred_element_type=f32)
        for local, pair, at in blocks:
            new = (
                joined[step, at, :] * row(1, local, pair)
                - sums[step, 0, at, :] * row(2, local, pair)
                + sums[step, 1, at, :] * row(3, local, pair)
            )
            target = early if step == 0 else late_ref
            target[local, 2 * pair] = new[:, 0:size]
            target[local, 2 * pair + 1] = new[:, size:pair_width]
            parts[step, 0, at, :], parts[step, 1, at, :] = two_parts(new * row(4, local, pair))
        if step == 0:
            store.start()

    dims = (((1,), (1,)), ((), ()))
    lines = [[], []]
    for step in range(steps):
        found = lax.dot_general(pick, parts[step, 0], dims, preferred_element_type=f32)
        found += lax.dot_general(pick, parts[step, 1], dims, preferred_element_type=f32)
        for which in range(2):
            for local in range(SEQ_STEP):
                at = slice(local * pairs * size, (local + 1) * pairs * size)
                lines[which].append(found[which * 8 : which * 8 + 1, at])
    for which in range(2):
        read[which] = jnp.concatenate(lines[which], axis=0)

    mixed = []
    for pair in range(pairs):
        at = slice(pair * size, (pair + 1) * size)
        live = jnp.concatenate([read[0, :, at], read[1, :, at]], axis=1)
        live = live - head_sums(live) * (1.0 / size)
        spread = head_sums(jnp.square(live)) * (1.0 / size)
        gain = vectors[1, :, pair * pair_width : (pair + 1) * pair_width]
        mixed.append(live * lax.rsqrt(spread + GROUP_EPSILON) * gain)
    mixed = jnp.concatenate(mixed, axis=1).astype(bf16)
    weight_load.wait()
    product = jnp.dot(mixed, weight_here[...], preferred_element_type=f32).astype(bf16)
    quarter = out_ref.shape[2]
    for owner in range(owners):
        out_ref[owner] = product[:, owner * quarter : (owner + 1) * quarter]
    store.wait()


def heads_update(owners, state_in, receptance, key_in, value_in, learn_in, decay_in, decay_base, norm_gain, out_weight):
    seqs, heads, size, _ = state_in.shape
    width = out_weight.shape[1]
    channels = heads * size
    steps = 2
    step_rows = SEQ_STEP * heads // 2 * size
    any_space = pl.BlockSpec(memory_space=pl.ANY)
    half_shape = (SEQ_STEP, heads, size, size)
    new_state, product, late = pl.pallas_call(
        functools.partial(heads_kernel, owners),
        in_specs=[any_space] * 9,
        out_specs=[any_space] + [pl.BlockSpec(memory_space=pltpu.VMEM)] * 2,
        out_shape=[
            jax.ShapeDtypeStruct(state_in.shape, jnp.float32),
            pltpu.VMEM((owners, seqs, width // owners), jnp.bfloat16),
            pltpu.VMEM(half_shape, jnp.float32),
        ],
        scratch_shapes=[
            pltpu.VMEM(state_in.shape, jnp.float32),
            pltpu.VMEM(half_shape, jnp.float32),
            pltpu.VMEM((4, seqs, channels), jnp.bfloat16),
            pltpu.VMEM((seqs, channels), jnp.float32),
            pltpu.VMEM((2, 1, channels), jnp.float32),
            pltpu.VMEM((channels, width), jnp.bfloat16),
            pltpu.VMEM((6, heads // 2, seqs, 2 * size), jnp.float32),
            pltpu.VMEM((2, seqs, channels // 2), jnp.float32),
            pltpu.VMEM((steps, step_rows, 2 * size), jnp.float32),
            pltpu.VMEM((steps, 3, step_rows, 2 * size), jnp.bfloat16),
            pltpu.VMEM((steps, 2, step_rows, 2 * size), jnp.float32),
            pltpu.SemaphoreType.DMA((steps + 8,)),
            pltpu.SemaphoreType.DMA,
        ],
        compiler_params=pltpu.CompilerParams(vmem_limit_bytes=60 << 20),
        cost_estimate=pl.CostEstimate(flops=20_000_000, bytes_accessed=5_000_000, transcendentals=20_000),
    )(
        state_in,
        receptance,
        key_in,
        value_in,
        learn_in,
        decay_in,
        decay_base.reshape(1, channels),
        norm_gain.reshape(1, channels),
        out_weight,
    )
    return product, new_state, late


def expert_kernel(
    got_ref, gain_ref, gate_ref, up_ref, down_ref, late_ref, state_ref, out_ref, new_state_ref, flat, stored
):
    f32 = jnp.float32
    store = pltpu.make_async_copy(
        late_ref, new_state_ref.at[pl.ds(SEQ_STEP, SEQ_STEP)], stored
    )
    store.start()
    senders, n_y, rows, quarter = got_ref.shape
    power = jnp.zeros((senders * rows, 128), f32)
    for y in range(n_y):
        flat[:, y * quarter : (y + 1) * quarter] = got_ref[:, y].reshape(senders * rows, quarter)
        for first in range(y * quarter, (y + 1) * quarter, 128):
            at = slice(first, first + 128)
            original = flat[:, at].astype(f32) * (1.0 / gain_ref[:, at])
            power += original * original
    mean = jnp.sum(power, axis=1, keepdims=True) * (1.0 / (n_y * quarter))
    scale = lax.rsqrt(mean + EPSILON)
    units = gate_ref.shape[2]
    weights = jnp.concatenate([gate_ref[0], up_ref[0]], axis=1)
    half = senders * rows // 2
    hidden = []
    for first in (0, half):
        both = jnp.dot(flat[first : first + half], weights, preferred_element_type=f32)
        both = both * scale[first : first + half]
        gate, upward = both[:, :units], both[:, units:]
        hidden.append((gate * jax.nn.sigmoid(gate) * upward).astype(jnp.bfloat16))
    hidden = jnp.concatenate(hidden, axis=0)
    for y in range(n_y):
        partial = jnp.dot(
            hidden, down_ref[0, :, y * quarter : (y + 1) * quarter], preferred_element_type=f32
        )
        out_ref[:, y] = partial.astype(jnp.bfloat16).reshape(senders, rows, quarter)
    store.wait()


def experts(got, routed_gain, expert_gate, expert_up, expert_down, late, new_state):
    senders, n_y, rows, quarter = got.shape
    vmem = pl.BlockSpec(memory_space=pltpu.VMEM)
    return pl.pallas_call(
        expert_kernel,
        in_specs=[vmem] * 6 + [pl.BlockSpec(memory_space=pl.ANY)],
        out_specs=[vmem, pl.BlockSpec(memory_space=pl.ANY)],
        out_shape=[
            jax.ShapeDtypeStruct(got.shape, jnp.bfloat16),
            jax.ShapeDtypeStruct(new_state.shape, new_state.dtype),
        ],
        input_output_aliases={6: 1},
        scratch_shapes=[
            pltpu.VMEM((senders * rows, n_y * quarter), jnp.bfloat16),
            pltpu.SemaphoreType.DMA,
        ],
        compiler_params=pltpu.CompilerParams(vmem_limit_bytes=12 << 20),
        cost_estimate=pl.CostEstimate(flops=400_000_000, bytes_accessed=4_000_000, transcendentals=40_000),
    )(got, routed_gain.reshape(1, n_y * quarter), expert_gate, expert_up, expert_down, late, new_state)


def pack_kernel(
    arrived_ref, hidden_ref, gain_ref, ids_ref, weights_ref, parcels_ref, own_ref
):
    f32, bf16 = jnp.float32, jnp.bfloat16
    seqs, quarter = own_ref.shape
    top = ids_ref.shape[0]
    at = pl.ds(pl.multiple_of(lax.axis_index("y") * quarter, quarter), quarter)
    attention = jnp.sum(arrived_ref[...].astype(f32), axis=0).astype(bf16)
    residual = hidden_ref[:, at].astype(f32) + attention.astype(f32)
    own_ref[...] = residual
    gained = (residual * gain_ref[:, at]).astype(bf16)

    weights = weights_ref[...]
    routing = jnp.zeros((8, 128), f32)
    parts = [ids_ref[...].astype(f32)]
    for _ in range(3):
        part = weights.astype(bf16).astype(f32)
        parts.append(part)
        weights = weights - part
    routing = jnp.concatenate(
        [jnp.pad(part, ((0, 8 - top), (0, 0))) for part in parts]
        + [jnp.zeros((8, 128 - len(parts) * seqs), f32)],
        axis=1,
    ).astype(bf16)
    chunks = quarter // 128
    for z in range(parcels_ref.shape[0]):
        for chunk in range(chunks):
            parcels_ref[z, chunk * seqs : (chunk + 1) * seqs, :] = gained[
                :, chunk * 128 : (chunk + 1) * 128
            ]
        parcels_ref[z, chunks * seqs : chunks * seqs + 8, :] = routing


def pack(arrived, hidden_in, routed_gain, route_ids, route_weights, n_z):
    n_y, seqs, quarter = arrived.shape
    width = n_y * quarter
    vmem = pl.BlockSpec(memory_space=pltpu.VMEM)
    return pl.pallas_call(
        pack_kernel,
        in_specs=[vmem] * 5,
        out_specs=[vmem] * 2,
        out_shape=[
            jax.ShapeDtypeStruct((n_z, quarter // 128 * seqs + 8, 128), jnp.bfloat16),
            jax.ShapeDtypeStruct((seqs, quarter), jnp.float32),
        ],
        compiler_params=pltpu.CompilerParams(vmem_limit_bytes=8 << 20),
    )(arrived, hidden_in, routed_gain.reshape(1, width), route_ids.T, route_weights.T)


def choose_kernel(top, slots, rows_ref, chosen_ref, place_ref, weight_ref, flat, choice):
    f32, bf16 = jnp.float32, jnp.bfloat16
    n_z = rows_ref.shape[0]
    seqs = flat.shape[0] // n_z
    near, n_y, per_expert, piece = chosen_ref.shape
    tokens = n_z * seqs
    chunks = piece // 128
    sender_of = lax.broadcasted_iota(jnp.int32, (8, 128), 1) // seqs
    groups = tokens // 128
    per_group = 128 // seqs
    spread = [[jnp.zeros((8, 128), f32) for _ in range(groups)] for _ in range(4)]
    for z in range(n_z):
        for chunk in range(chunks):
            flat[z * seqs : (z + 1) * seqs, chunk * 128 : (chunk + 1) * 128] = rows_ref[
                z, chunk * seqs : (chunk + 1) * seqs, :
            ]
        routing = rows_ref[z, chunks * seqs : chunks * seqs + 8, :].astype(f32)
        group, place = divmod(z, per_group)
        for which in range(4):
            turn = (place - which) * seqs % 128
            moved = routing if turn == 0 else pltpu.roll(routing, turn, 1)
            spread[which][group] = jnp.where(sender_of == place, moved, spread[which][group])
    ids, high, middle, low = [jnp.concatenate(part, axis=1) for part in spread]
    weights = high + middle + low
    named = (
        lax.axis_index("zq") * near + lax.broadcasted_iota(jnp.int32, (near, tokens), 0)
    ).astype(f32)
    member = jnp.zeros((near, tokens), f32)
    weight = jnp.zeros((near, tokens), f32)
    for k in range(top):
        hit = named == ids[k : k + 1, :]
        member = jnp.where(hit, 1.0, member)
        weight = jnp.where(hit, weights[k : k + 1, :], weight)
    token = lax.broadcasted_iota(jnp.int32, (tokens, tokens), 0)
    other = lax.broadcasted_iota(jnp.int32, (tokens, tokens), 1)
    earlier = (token // seqs == other // seqs) & (token < other)
    rank = jnp.dot(member.astype(bf16), jnp.where(earlier, 1.0, 0.0).astype(bf16), preferred_element_type=f32)
    sender = (lax.broadcasted_iota(jnp.int32, (near, tokens), 1) // seqs * slots).astype(f32)
    place = jnp.where(member > 0, sender + rank, -1.0)
    place_ref[...] = place
    weight_ref[...] = weight
    row = lax.broadcasted_iota(jnp.int32, (per_expert, tokens), 0).astype(f32)
    for expert in range(near):
        choice[expert * per_expert : (expert + 1) * per_expert, :] = jnp.where(
            row == place[expert : expert + 1, :], 1.0, 0.0
        ).astype(bf16)
    chosen = jnp.dot(choice[...], flat[...], preferred_element_type=f32).astype(bf16)
    chosen = chosen.reshape(near, per_expert, piece)
    for y in range(n_y):
        chosen_ref[:, y] = chosen


def choose(rows, near, n_y, slots, top, seqs):
    n_z, depth, _ = rows.shape
    piece = (depth - 8) // seqs * 128
    tokens = n_z * seqs
    vmem = pl.BlockSpec(memory_space=pltpu.VMEM)
    return pl.pallas_call(
        functools.partial(choose_kernel, top, slots),
        in_specs=[vmem],
        out_specs=[vmem] * 3,
        out_shape=[
            jax.ShapeDtypeStruct((near, n_y, n_z * slots, piece), jnp.bfloat16),
            jax.ShapeDtypeStruct((near, tokens), jnp.float32),
            jax.ShapeDtypeStruct((near, tokens), jnp.float32),
        ],
        scratch_shapes=[
            pltpu.VMEM((tokens, piece), jnp.bfloat16),
            pltpu.VMEM((near * n_z * slots, tokens), jnp.bfloat16),
        ],
        compiler_params=pltpu.CompilerParams(vmem_limit_bytes=12 << 20),
    )(rows)


def combine_kernel(returned_ref, place_ref, weight_ref, out_ref, summed, choice):
    f32, bf16 = jnp.float32, jnp.bfloat16
    near, n_y, per_expert, piece = returned_ref.shape
    n_z, seqs, _ = out_ref.shape
    tokens = n_z * seqs
    total = near * per_expert
    row = lax.broadcasted_iota(jnp.int32, (per_expert, tokens), 0).astype(f32)
    for expert in range(near):
        at = slice(expert * per_expert, (expert + 1) * per_expert)
        result = jnp.sum(returned_ref[expert].astype(f32), axis=0).astype(bf16)
        summed[at, :] = result
        summed[total + expert * per_expert : total + (expert + 1) * per_expert, :] = result
        weight = jnp.where(
            row == place_ref[expert : expert + 1, :], weight_ref[expert : expert + 1, :], 0.0
        )
        high = weight.astype(bf16)
        choice[at, :] = high
        choice[total + expert * per_expert : total + (expert + 1) * per_expert, :] = (
            weight - high.astype(f32)
        ).astype(bf16)
    combined = lax.dot_general(
        choice[...], summed[...], (((0,), (0,)), ((), ())), preferred_element_type=f32
    )
    out_ref[...] = combined.astype(bf16).reshape(n_z, seqs, piece)


def combine(returned, place, weight, n_z):
    near, n_y, per_expert, piece = returned.shape
    tokens = place.shape[1]
    vmem = pl.BlockSpec(memory_space=pltpu.VMEM)
    return pl.pallas_call(
        combine_kernel,
        in_specs=[vmem] * 3,
        out_specs=vmem,
        out_shape=jax.ShapeDtypeStruct((n_z, tokens // n_z, piece), jnp.bfloat16),
        scratch_shapes=[
            pltpu.VMEM((2 * near * per_expert, piece), jnp.bfloat16),
            pltpu.VMEM((2 * near * per_expert, tokens), jnp.bfloat16),
        ],
        compiler_params=pltpu.CompilerParams(vmem_limit_bytes=12 << 20),
    )(returned, place, weight)


def on_device(
    hidden_in,
    state_in,
    receptance,
    key_in,
    value_in,
    learn_in,
    decay_in,
    decay_base,
    norm_gain,
    out_weight,
    routed_gain,
    expert_gate,
    expert_up,
    expert_down,
    route_ids,
    route_weights,
):
    n_y, n_zq = lax.axis_size("y"), lax.axis_size("zq")
    near = lax.axis_size(("zp", "x", "c"))
    seqs, width = hidden_in.shape
    quarter = width // n_y
    per_expert = n_zq * SLOTS

    product, new_state, late = heads_update(
        n_y, state_in, receptance, key_in, value_in, learn_in, decay_in, decay_base, norm_gain, out_weight
    )
    arrived = exchange(product, "y")
    parcels, own_residual = pack(arrived, hidden_in, routed_gain, route_ids, route_weights, n_zq)
    rows = exchange(parcels, "zq")
    chosen, place, weight = choose(rows, near, n_y, SLOTS, route_ids.shape[1], seqs)
    got = exchange(chosen.reshape(near * n_y, per_expert, quarter), NEAR_AXES)
    got = got.reshape(near, n_y, per_expert, quarter)
    back, new_state = experts(got, routed_gain, expert_gate, expert_up, expert_down, late, new_state)
    returned = exchange(back.reshape(near * n_y, per_expert, quarter), NEAR_AXES)
    combined = combine(returned.reshape(near, n_y, per_expert, quarter), place, weight, n_zq)
    routed = exchange(combined, "zq").astype(jnp.float32).sum(axis=0)
    result = (own_residual + routed).astype(jnp.bfloat16)
    spread = exchange(jnp.broadcast_to(result, (n_y, seqs, quarter)), "y")
    return (spread.transpose(1, 0, 2).reshape(seqs, width), new_state)


def solution(mesh):
    near_mesh = Mesh(mesh.devices.reshape(8, 2, 4, 2, 4), ("zq", "zp", "x", "c", "y"))
    in_specs = (
        P(EP, None),
        P(EP, "y", None, None),
        P(EP, "y"),
        P(EP, "y"),
        P(EP, "y"),
        P(EP, "y"),
        P(EP, "y"),
        P("y"),
        P("y"),
        P("y", None),
        P(),
        P(EP, None, "y"),
        P(EP, None, "y"),
        P(EP, "y", None),
        P(EP, None),
        P(EP, None),
    )
    out_specs = (P(EP, None), P(EP, "y", None, None))
    return jax.shard_map(
        on_device, mesh=near_mesh, in_specs=in_specs, out_specs=out_specs, check_vma=False
    )
```

```python
import functools
import math
import jax
import jax.numpy as jnp
import numpy as np
from jax import lax
from jax.experimental import pallas as pl
from jax.experimental.pallas import tpu as pltpu
from jax.sharding import Mesh, PartitionSpec as P

EPSILON = 1e-06
GROUP_EPSILON = 0.00064
SEQ_STEP = 8
SLOTS = 2
NEAR_AXES = ("zp", "x", "c", "y")
EP = ("zq", "zp", "x", "c")


def exchange(pieces, axes):
    return lax.all_to_all(pieces, axes, split_axis=0, concat_axis=0, tiled=True)


def two_parts(values):
    high = values.astype(jnp.bfloat16)
    return high, (values - high.astype(jnp.float32)).astype(jnp.bfloat16)


def routing_rows(ids, shares):
    f32, bf16 = jnp.float32, jnp.bfloat16
    top, seqs = ids.shape
    lane = lax.broadcasted_iota(jnp.int32, (8, 128), 1)
    ids = jnp.pad(ids, ((0, 8 - top), (0, 128 - seqs)))
    again = jnp.zeros((8, 128), jnp.int32)
    for k in range(top):
        line = jnp.broadcast_to(ids[k : k + 1], (8, 128))
        for back in range(1, seqs):
            same = (pltpu.roll(line, back, 1) == ids) & (lane >= back)
            again = jnp.where(same, 128, again)
    parts = [(ids + again)[:, :seqs].astype(f32)]
    shares = jnp.pad(shares, ((0, 8 - top), (0, 0)))
    for _ in range(3):
        part = shares.astype(bf16).astype(f32)
        parts.append(part)
        shares = shares - part
    parts.append(jnp.zeros((8, 128 - len(parts) * seqs), f32))
    return jnp.concatenate(parts, axis=1).astype(bf16)


def heads_kernel(
    owners,
    state_ref,
    reading_ref,
    key_ref,
    value_ref,
    learn_ref,
    decay_ref,
    base_ref,
    gain_ref,
    weight_ref,
    ids_ref,
    shares_ref,
    new_state_ref,
    out_ref,
    late_ref,
    routing_ref,
    state_here,
    early,
    inputs,
    decay_here,
    vectors,
    ids_here,
    shares_here,
    weight_here,
    rows,
    read,
    joined,
    parts,
    sums,
    arrived,
    stored,
):
    f32, bf16 = jnp.float32, jnp.bfloat16
    seqs, heads, size, _ = state_here.shape
    channels = heads * size
    pairs = heads // 2
    pair_width = 2 * size
    steps = 2

    def state_load(step):
        at = pl.ds(step * SEQ_STEP, SEQ_STEP)
        return pltpu.make_async_copy(state_ref.at[at], state_here.at[at], arrived.at[step])

    store = pltpu.make_async_copy(early, new_state_ref.at[pl.ds(0, SEQ_STEP)], stored)

    small = [
        pltpu.make_async_copy(source, target, arrived.at[steps + number])
        for number, (source, target) in enumerate(
            (
                (key_ref, inputs.at[0]),
                (learn_ref, inputs.at[1]),
                (decay_ref, decay_here),
                (base_ref, vectors.at[0]),
                (reading_ref, inputs.at[2]),
                (value_ref, inputs.at[3]),
                (gain_ref, vectors.at[1]),
                (ids_ref, ids_here),
                (shares_ref, shares_here),
            )
        )
    ]
    weight_load = pltpu.make_async_copy(weight_ref, weight_here, arrived.at[steps + len(small)])
    for load in small:
        load.start()
    for step in range(steps):
        state_load(step).start()
    weight_load.start()

    square = (pair_width, pair_width)
    same_head = (
        lax.broadcasted_iota(jnp.int32, square, 0) // size
        == lax.broadcasted_iota(jnp.int32, square, 1) // size
    )
    ones = jnp.where(same_head, 1.0, 0.0).astype(bf16)

    def head_sums(values):
        return sum(jnp.dot(part, ones, preferred_element_type=f32) for part in two_parts(values))

    for load in small:
        load.wait()
    keys = inputs[0].astype(f32)
    learning = jax.nn.sigmoid(inputs[1].astype(f32))
    decay = jnp.exp(-math.exp(-0.5) * jax.nn.sigmoid(vectors[0] + decay_here[...]))
    for pair in range(pairs):
        at = slice(pair * pair_width, (pair + 1) * pair_width)
        key = keys[:, at]
        unit = key * lax.rsqrt(head_sums(key * key) + EPSILON)
        rows[0, pair] = unit
        rows[1, pair] = decay[:, at]
        rows[2, pair] = unit * learning[:, at]
        rows[3, pair] = key
        rows[4, pair] = inputs[2, :, at].astype(f32)
        rows[5, pair] = inputs[3, :, at].astype(f32)

    routing_ref[...] = routing_rows(ids_here[...], shares_here[...])

    blocks = [
        (local, pair, slice((local * pairs + pair) * size, (local * pairs + pair + 1) * size))
        for local in range(SEQ_STEP)
        for pair in range(pairs)
    ]
    on_diagonal = lax.broadcasted_iota(jnp.int32, (size, pair_width), 0) == (
        lax.broadcasted_iota(jnp.int32, (size, pair_width), 1) % size
    )
    head_of = lax.broadcasted_iota(jnp.int32, (2 * 8, pair_width), 0) // 8
    pick = jnp.where(
        head_of == lax.broadcasted_iota(jnp.int32, (2 * 8, pair_width), 1) // size, 1.0, 0.0
    ).astype(bf16)

    for step in range(steps):
        first = step * SEQ_STEP

        def row(which, local, pair):
            return rows[which, pair, first + local : first + local + 1, :]

        state_load(step).wait()
        for local, pair, at in blocks:
            parts[step, 2, at, :] = jnp.where(on_diagonal, row(5, local, pair), 0.0).astype(bf16)
            state = jnp.concatenate(
                [state_here[first + local, 2 * pair], state_here[first + local, 2 * pair + 1]], axis=1
            )
            joined[step, at, :] = state
            parts[step, 0, at, :], parts[step, 1, at, :] = two_parts(state * row(0, local, pair))
        sums[step, 0] = jnp.dot(parts[step, 0], ones, preferred_element_type=f32) + jnp.dot(
            parts[step, 1], ones, preferred_element_type=f32
        )
        sums[step, 1] = jnp.dot(parts[step, 2], ones, preferred_element_type=f32)
        for local, pair, at in blocks:
            new = (
                joined[step, at, :] * row(1, local, pair)
                - sums[step, 0, at, :] * row(2, local, pair)
                + sums[step, 1, at, :] * row(3, local, pair)
            )
            target = early if step == 0 else late_ref
            target[local, 2 * pair] = new[:, 0:size]
            target[local, 2 * pair + 1] = new[:, size:pair_width]
            parts[step, 0, at, :], parts[step, 1, at, :] = two_parts(new * row(4, local, pair))
        if step == 0:
            store.start()

    dims = (((1,), (1,)), ((), ()))
    lines = [[], []]
    for step in range(steps):
        found = lax.dot_general(pick, parts[step, 0], dims, preferred_element_type=f32)
        found += lax.dot_general(pick, parts[step, 1], dims, preferred_element_type=f32)
        for which in range(2):
            for local in range(SEQ_STEP):
                at = slice(local * pairs * size, (local + 1) * pairs * size)
                lines[which].append(found[which * 8 : which * 8 + 1, at])
    for which in range(2):
        read[which] = jnp.concatenate(lines[which], axis=0)

    mixed = []
    for pair in range(pairs):
        at = slice(pair * size, (pair + 1) * size)
        live = jnp.concatenate([read[0, :, at], read[1, :, at]], axis=1)
        live = live - head_sums(live) * (1.0 / size)
        spread = head_sums(jnp.square(live)) * (1.0 / size)
        gain = vectors[1, :, pair * pair_width : (pair + 1) * pair_width]
        mixed.append(live * lax.rsqrt(spread + GROUP_EPSILON) * gain)
    mixed = jnp.concatenate(mixed, axis=1).astype(bf16)
    weight_load.wait()
    product = jnp.dot(mixed, weight_here[...], preferred_element_type=f32).astype(bf16)
    quarter = out_ref.shape[2]
    for owner in range(owners):
        out_ref[owner] = product[:, owner * quarter : (owner + 1) * quarter]
    store.wait()


def heads_update(owners, state_in, receptance, key_in, value_in, learn_in, decay_in, decay_base, norm_gain, out_weight, route_ids, route_weights):
    seqs, heads, size, _ = state_in.shape
    width = out_weight.shape[1]
    channels = heads * size
    steps = 2
    step_rows = SEQ_STEP * heads // 2 * size
    any_space = pl.BlockSpec(memory_space=pl.ANY)
    half_shape = (SEQ_STEP, heads, size, size)
    top = route_ids.shape[1]
    new_state, product, late, routing = pl.pallas_call(
        functools.partial(heads_kernel, owners),
        in_specs=[any_space] * 11,
        out_specs=[any_space] + [pl.BlockSpec(memory_space=pltpu.VMEM)] * 3,
        out_shape=[
            jax.ShapeDtypeStruct(state_in.shape, jnp.float32),
            pltpu.VMEM((owners, seqs, width // owners), jnp.bfloat16),
            pltpu.VMEM(half_shape, jnp.float32),
            pltpu.VMEM((8, 128), jnp.bfloat16),
        ],
        scratch_shapes=[
            pltpu.VMEM(state_in.shape, jnp.float32),
            pltpu.VMEM(half_shape, jnp.float32),
            pltpu.VMEM((4, seqs, channels), jnp.bfloat16),
            pltpu.VMEM((seqs, channels), jnp.float32),
            pltpu.VMEM((2, 1, channels), jnp.float32),
            pltpu.VMEM((top, seqs), jnp.int32),
            pltpu.VMEM((top, seqs), jnp.float32),
            pltpu.VMEM((channels, width), jnp.bfloat16),
            pltpu.VMEM((6, heads // 2, seqs, 2 * size), jnp.float32),
            pltpu.VMEM((2, seqs, channels // 2), jnp.float32),
            pltpu.VMEM((steps, step_rows, 2 * size), jnp.float32),
            pltpu.VMEM((steps, 3, step_rows, 2 * size), jnp.bfloat16),
            pltpu.VMEM((steps, 2, step_rows, 2 * size), jnp.float32),
            pltpu.SemaphoreType.DMA((steps + 10,)),
            pltpu.SemaphoreType.DMA,
        ],
        compiler_params=pltpu.CompilerParams(vmem_limit_bytes=60 << 20),
        cost_estimate=pl.CostEstimate(flops=20_000_000, bytes_accessed=5_000_000, transcendentals=20_000),
    )(
        state_in,
        receptance,
        key_in,
        value_in,
        learn_in,
        decay_in,
        decay_base.reshape(1, channels),
        norm_gain.reshape(1, channels),
        out_weight,
        route_ids.T,
        route_weights.T,
    )
    return product, new_state, late, routing


def expert_kernel(
    got_ref, gain_ref, gate_ref, up_ref, down_ref, late_ref, state_ref, out_ref, new_state_ref, flat, stored
):
    f32 = jnp.float32
    store = pltpu.make_async_copy(
        late_ref, new_state_ref.at[pl.ds(SEQ_STEP, SEQ_STEP)], stored
    )
    store.start()
    senders, n_y, rows, quarter = got_ref.shape
    power = jnp.zeros((senders * rows, 128), f32)
    for y in range(n_y):
        flat[:, y * quarter : (y + 1) * quarter] = got_ref[:, y].reshape(senders * rows, quarter)
        for first in range(y * quarter, (y + 1) * quarter, 128):
            at = slice(first, first + 128)
            original = flat[:, at].astype(f32) * (1.0 / gain_ref[:, at])
            power += original * original
    mean = jnp.sum(power, axis=1, keepdims=True) * (1.0 / (n_y * quarter))
    scale = lax.rsqrt(mean + EPSILON)
    units = gate_ref.shape[2]
    weights = jnp.concatenate([gate_ref[0], up_ref[0]], axis=1)
    half = senders * rows // 2
    hidden = []
    for first in (0, half):
        both = jnp.dot(flat[first : first + half], weights, preferred_element_type=f32)
        both = both * scale[first : first + half]
        gate, upward = both[:, :units], both[:, units:]
        hidden.append((gate * jax.nn.sigmoid(gate) * upward).astype(jnp.bfloat16))
    hidden = jnp.concatenate(hidden, axis=0)
    for y in range(n_y):
        partial = jnp.dot(
            hidden, down_ref[0, :, y * quarter : (y + 1) * quarter], preferred_element_type=f32
        )
        out_ref[:, y] = partial.astype(jnp.bfloat16).reshape(senders, rows, quarter)
    store.wait()


def experts(got, routed_gain, expert_gate, expert_up, expert_down, late, new_state):
    senders, n_y, rows, quarter = got.shape
    vmem = pl.BlockSpec(memory_space=pltpu.VMEM)
    return pl.pallas_call(
        expert_kernel,
        in_specs=[vmem] * 6 + [pl.BlockSpec(memory_space=pl.ANY)],
        out_specs=[vmem, pl.BlockSpec(memory_space=pl.ANY)],
        out_shape=[
            jax.ShapeDtypeStruct(got.shape, jnp.bfloat16),
            jax.ShapeDtypeStruct(new_state.shape, new_state.dtype),
        ],
        input_output_aliases={6: 1},
        scratch_shapes=[
            pltpu.VMEM((senders * rows, n_y * quarter), jnp.bfloat16),
            pltpu.SemaphoreType.DMA,
        ],
        compiler_params=pltpu.CompilerParams(vmem_limit_bytes=12 << 20),
        cost_estimate=pl.CostEstimate(flops=400_000_000, bytes_accessed=4_000_000, transcendentals=40_000),
    )(got, routed_gain.reshape(1, n_y * quarter), expert_gate, expert_up, expert_down, late, new_state)


def pack_kernel(
    arrived_ref, hidden_ref, gain_ref, routing_ref, parcels_ref, own_ref
):
    f32, bf16 = jnp.float32, jnp.bfloat16
    seqs, quarter = own_ref.shape
    at = pl.ds(pl.multiple_of(lax.axis_index("y") * quarter, quarter), quarter)
    attention = jnp.sum(arrived_ref[...].astype(f32), axis=0).astype(bf16)
    residual = hidden_ref[:, at].astype(f32) + attention.astype(f32)
    own_ref[...] = residual
    gained = (residual * gain_ref[:, at]).astype(bf16)

    chunks = quarter // 128
    for z in range(parcels_ref.shape[0]):
        for chunk in range(chunks):
            parcels_ref[z, chunk * seqs : (chunk + 1) * seqs, :] = gained[
                :, chunk * 128 : (chunk + 1) * 128
            ]
        parcels_ref[z, chunks * seqs : chunks * seqs + 8, :] = routing_ref[...]


def pack(arrived, hidden_in, routed_gain, routing, n_z):
    n_y, seqs, quarter = arrived.shape
    width = n_y * quarter
    vmem = pl.BlockSpec(memory_space=pltpu.VMEM)
    return pl.pallas_call(
        pack_kernel,
        in_specs=[vmem] * 4,
        out_specs=[vmem] * 2,
        out_shape=[
            jax.ShapeDtypeStruct((n_z, quarter // 128 * seqs + 8, 128), jnp.bfloat16),
            jax.ShapeDtypeStruct((seqs, quarter), jnp.float32),
        ],
        compiler_params=pltpu.CompilerParams(vmem_limit_bytes=8 << 20),
    )(arrived, hidden_in, routed_gain.reshape(1, width), routing)


def choose_kernel(top, slots, rows_ref, chosen_ref, place_ref, weight_ref, flat, choice):
    f32, bf16 = jnp.float32, jnp.bfloat16
    n_z = rows_ref.shape[0]
    seqs = flat.shape[0] // n_z
    near, n_y, per_expert, piece = chosen_ref.shape
    tokens = n_z * seqs
    chunks = piece // 128
    sender_of = lax.broadcasted_iota(jnp.int32, (8, 128), 1) // seqs
    groups = tokens // 128
    per_group = 128 // seqs
    spread = [[jnp.zeros((8, 128), f32) for _ in range(groups)] for _ in range(4)]
    for z in range(n_z):
        for chunk in range(chunks):
            flat[z * seqs : (z + 1) * seqs, chunk * 128 : (chunk + 1) * 128] = rows_ref[
                z, chunk * seqs : (chunk + 1) * seqs, :
            ]
        routing = rows_ref[z, chunks * seqs : chunks * seqs + 8, :].astype(f32)
        group, place = divmod(z, per_group)
        for which in range(4):
            turn = (place - which) * seqs % 128
            moved = routing if turn == 0 else pltpu.roll(routing, turn, 1)
            spread[which][group] = jnp.where(sender_of == place, moved, spread[which][group])
    ids, high, middle, low = [jnp.concatenate(part, axis=1) for part in spread]
    weights = high + middle + low
    named = (
        lax.axis_index("zq") * near + lax.broadcasted_iota(jnp.int32, (near, tokens), 0)
    ).astype(f32)
    sender = (lax.broadcasted_iota(jnp.int32, (near, tokens), 1) // seqs * slots).astype(f32)
    place = jnp.full((near, tokens), -1.0, f32)
    weight = jnp.zeros((near, tokens), f32)
    for k in range(top):
        for slot in range(slots):
            hit = named + 128.0 * slot == ids[k : k + 1, :]
            place = jnp.where(hit, sender + slot, place)
            weight = jnp.where(hit, weights[k : k + 1, :], weight)
    place_ref[...] = place
    weight_ref[...] = weight
    row = lax.broadcasted_iota(jnp.int32, (per_expert, tokens), 0).astype(f32)
    for expert in range(near):
        choice[expert * per_expert : (expert + 1) * per_expert, :] = jnp.where(
            row == place[expert : expert + 1, :], 1.0, 0.0
        ).astype(bf16)
    chosen = jnp.dot(choice[...], flat[...], preferred_element_type=f32).astype(bf16)
    chosen = chosen.reshape(near, per_expert, piece)
    for y in range(n_y):
        chosen_ref[:, y] = chosen


def choose(rows, near, n_y, slots, top, seqs):
    n_z, depth, _ = rows.shape
    piece = (depth - 8) // seqs * 128
    tokens = n_z * seqs
    vmem = pl.BlockSpec(memory_space=pltpu.VMEM)
    return pl.pallas_call(
        functools.partial(choose_kernel, top, slots),
        in_specs=[vmem],
        out_specs=[vmem] * 3,
        out_shape=[
            jax.ShapeDtypeStruct((near, n_y, n_z * slots, piece), jnp.bfloat16),
            jax.ShapeDtypeStruct((near, tokens), jnp.float32),
            jax.ShapeDtypeStruct((near, tokens), jnp.float32),
        ],
        scratch_shapes=[
            pltpu.VMEM((tokens, piece), jnp.bfloat16),
            pltpu.VMEM((near * n_z * slots, tokens), jnp.bfloat16),
        ],
        compiler_params=pltpu.CompilerParams(vmem_limit_bytes=12 << 20),
    )(rows)


def combine_kernel(returned_ref, place_ref, weight_ref, out_ref, summed, choice):
    f32, bf16 = jnp.float32, jnp.bfloat16
    near, n_y, per_expert, piece = returned_ref.shape
    n_z, seqs, _ = out_ref.shape
    tokens = n_z * seqs
    total = near * per_expert
    row = lax.broadcasted_iota(jnp.int32, (per_expert, tokens), 0).astype(f32)
    for expert in range(near):
        at = slice(expert * per_expert, (expert + 1) * per_expert)
        result = jnp.sum(returned_ref[expert].astype(f32), axis=0).astype(bf16)
        summed[at, :] = result
        summed[total + expert * per_expert : total + (expert + 1) * per_expert, :] = result
        weight = jnp.where(
            row == place_ref[expert : expert + 1, :], weight_ref[expert : expert + 1, :], 0.0
        )
        high = weight.astype(bf16)
        choice[at, :] = high
        choice[total + expert * per_expert : total + (expert + 1) * per_expert, :] = (
            weight - high.astype(f32)
        ).astype(bf16)
    combined = lax.dot_general(
        choice[...], summed[...], (((0,), (0,)), ((), ())), preferred_element_type=f32
    )
    out_ref[...] = combined.astype(bf16).reshape(n_z, seqs, piece)


def combine(returned, place, weight, n_z):
    near, n_y, per_expert, piece = returned.shape
    tokens = place.shape[1]
    vmem = pl.BlockSpec(memory_space=pltpu.VMEM)
    return pl.pallas_call(
        combine_kernel,
        in_specs=[vmem] * 3,
        out_specs=vmem,
        out_shape=jax.ShapeDtypeStruct((n_z, tokens // n_z, piece), jnp.bfloat16),
        scratch_shapes=[
            pltpu.VMEM((2 * near * per_expert, piece), jnp.bfloat16),
            pltpu.VMEM((2 * near * per_expert, tokens), jnp.bfloat16),
        ],
        compiler_params=pltpu.CompilerParams(vmem_limit_bytes=12 << 20),
    )(returned, place, weight)


def on_device(
    hidden_in,
    state_in,
    receptance,
    key_in,
    value_in,
    learn_in,
    decay_in,
    decay_base,
    norm_gain,
    out_weight,
    routed_gain,
    expert_gate,
    expert_up,
    expert_down,
    route_ids,
    route_weights,
):
    n_y, n_zq = lax.axis_size("y"), lax.axis_size("zq")
    near = lax.axis_size(("zp", "x", "c"))
    seqs, width = hidden_in.shape
    quarter = width // n_y
    per_expert = n_zq * SLOTS

    product, new_state, late, routing = heads_update(
        n_y, state_in, receptance, key_in, value_in, learn_in, decay_in, decay_base, norm_gain, out_weight,
        route_ids, route_weights,
    )
    arrived = exchange(product, "y")
    parcels, own_residual = pack(arrived, hidden_in, routed_gain, routing, n_zq)
    rows = exchange(parcels, "zq")
    chosen, place, weight = choose(rows, near, n_y, SLOTS, route_ids.shape[1], seqs)
    got = exchange(chosen.reshape(near * n_y, per_expert, quarter), NEAR_AXES)
    got = got.reshape(near, n_y, per_expert, quarter)
    back, new_state = experts(got, routed_gain, expert_gate, expert_up, expert_down, late, new_state)
    returned = exchange(back.reshape(near * n_y, per_expert, quarter), NEAR_AXES)
    combined = combine(returned.reshape(near, n_y, per_expert, quarter), place, weight, n_zq)
    routed = exchange(combined, "zq").astype(jnp.float32).sum(axis=0)
    result = (own_residual + routed).astype(jnp.bfloat16)
    spread = exchange(jnp.broadcast_to(result, (n_y, seqs, quarter)), "y")
    return (spread.transpose(1, 0, 2).reshape(seqs, width), new_state)


def solution(mesh):
    near_mesh = Mesh(mesh.devices.reshape(8, 2, 4, 2, 4), ("zq", "zp", "x", "c", "y"))
    in_specs = (
        P(EP, None),
        P(EP, "y", None, None),
        P(EP, "y"),
        P(EP, "y"),
        P(EP, "y"),
        P(EP, "y"),
        P(EP, "y"),
        P("y"),
        P("y"),
        P("y", None),
        P(),
        P(EP, None, "y"),
        P(EP, None, "y"),
        P(EP, "y", None),
        P(EP, None),
        P(EP, None),
    )
    out_specs = (P(EP, None), P(EP, "y", None, None))
    return jax.shard_map(
        on_device, mesh=near_mesh, in_specs=in_specs, out_specs=out_specs, check_vma=False
    )
```

```python
import functools
import math
import jax
import jax.numpy as jnp
import numpy as np
from jax import lax
from jax.experimental import pallas as pl
from jax.experimental.pallas import tpu as pltpu
from jax.sharding import Mesh, PartitionSpec as P

EPSILON = 1e-06
GROUP_EPSILON = 0.00064
SEQ_STEP = 8
SLOTS = 2
NEAR_AXES = ("zp", "x", "c", "y")
EP = ("zq", "zp", "x", "c")


def exchange(pieces, axes):
    return lax.all_to_all(pieces, axes, split_axis=0, concat_axis=0, tiled=True)


def two_parts(values):
    high = values.astype(jnp.bfloat16)
    return high, (values - high.astype(jnp.float32)).astype(jnp.bfloat16)


def routing_rows(ids, shares):
    f32, bf16 = jnp.float32, jnp.bfloat16
    top, seqs = ids.shape
    lane = lax.broadcasted_iota(jnp.int32, (8, 128), 1)
    ids = jnp.pad(ids, ((0, 8 - top), (0, 128 - seqs)))
    again = jnp.zeros((8, 128), jnp.int32)
    for k in range(top):
        line = jnp.broadcast_to(ids[k : k + 1], (8, 128))
        for back in range(1, seqs):
            same = (pltpu.roll(line, back, 1) == ids) & (lane >= back)
            again = jnp.where(same, 128, again)
    parts = [(ids + again)[:, :seqs].astype(f32)]
    shares = jnp.pad(shares, ((0, 8 - top), (0, 0)))
    for _ in range(3):
        part = shares.astype(bf16).astype(f32)
        parts.append(part)
        shares = shares - part
    parts.append(jnp.zeros((8, 128 - len(parts) * seqs), f32))
    return jnp.concatenate(parts, axis=1).astype(bf16)


def heads_kernel(
    owners,
    state_ref,
    reading_ref,
    key_ref,
    value_ref,
    learn_ref,
    decay_ref,
    base_ref,
    gain_ref,
    weight_ref,
    ids_ref,
    shares_ref,
    new_state_ref,
    out_ref,
    late_ref,
    routing_ref,
    state_here,
    early,
    inputs,
    decay_here,
    vectors,
    ids_here,
    shares_here,
    weight_here,
    rows,
    read,
    joined,
    parts,
    sums,
    arrived,
    stored,
):
    f32, bf16 = jnp.float32, jnp.bfloat16
    seqs, heads, size, _ = state_here.shape
    channels = heads * size
    pairs = heads // 2
    pair_width = 2 * size
    steps = 2

    def state_load(step):
        at = pl.ds(step * SEQ_STEP, SEQ_STEP)
        return pltpu.make_async_copy(state_ref.at[at], state_here.at[at], arrived.at[step])

    store = pltpu.make_async_copy(early, new_state_ref.at[pl.ds(0, SEQ_STEP)], stored)

    small = [
        pltpu.make_async_copy(source, target, arrived.at[steps + number])
        for number, (source, target) in enumerate(
            (
                (key_ref, inputs.at[0]),
                (learn_ref, inputs.at[1]),
                (decay_ref, decay_here),
                (base_ref, vectors.at[0]),
                (reading_ref, inputs.at[2]),
                (value_ref, inputs.at[3]),
                (gain_ref, vectors.at[1]),
                (ids_ref, ids_here),
                (shares_ref, shares_here),
            )
        )
    ]
    weight_load = pltpu.make_async_copy(weight_ref, weight_here, arrived.at[steps + len(small)])
    for load in small:
        load.start()
    for step in range(steps):
        state_load(step).start()
    weight_load.start()

    square = (pair_width, pair_width)
    same_head = (
        lax.broadcasted_iota(jnp.int32, square, 0) // size
        == lax.broadcasted_iota(jnp.int32, square, 1) // size
    )
    ones = jnp.where(same_head, 1.0, 0.0).astype(bf16)

    def head_sums(values):
        return sum(jnp.dot(part, ones, preferred_element_type=f32) for part in two_parts(values))

    for load in small:
        load.wait()
    keys = inputs[0].astype(f32)
    learning = jax.nn.sigmoid(inputs[1].astype(f32))
    decay = jnp.exp(-math.exp(-0.5) * jax.nn.sigmoid(vectors[0] + decay_here[...]))
    for pair in range(pairs):
        at = slice(pair * pair_width, (pair + 1) * pair_width)
        key = keys[:, at]
        unit = key * lax.rsqrt(head_sums(key * key) + EPSILON)
        rows[0, pair] = unit
        rows[1, pair] = decay[:, at]
        rows[2, pair] = unit * learning[:, at]
        rows[3, pair] = key
        rows[4, pair] = inputs[2, :, at].astype(f32)
        rows[5, pair] = inputs[3, :, at].astype(f32)

    routing_ref[...] = routing_rows(ids_here[...], shares_here[...])

    blocks = [
        (local, pair, slice((local * pairs + pair) * size, (local * pairs + pair + 1) * size))
        for local in range(SEQ_STEP)
        for pair in range(pairs)
    ]
    on_diagonal = lax.broadcasted_iota(jnp.int32, (size, pair_width), 0) == (
        lax.broadcasted_iota(jnp.int32, (size, pair_width), 1) % size
    )
    head_of = lax.broadcasted_iota(jnp.int32, (2 * 8, pair_width), 0) // 8
    pick = jnp.where(
        head_of == lax.broadcasted_iota(jnp.int32, (2 * 8, pair_width), 1) // size, 1.0, 0.0
    ).astype(bf16)

    for step in range(steps):
        first = step * SEQ_STEP

        def row(which, local, pair):
            return rows[which, pair, first + local : first + local + 1, :]

        state_load(step).wait()
        for local, pair, at in blocks:
            parts[step, 2, at, :] = jnp.where(on_diagonal, row(5, local, pair), 0.0).astype(bf16)
            state = jnp.concatenate(
                [state_here[first + local, 2 * pair], state_here[first + local, 2 * pair + 1]], axis=1
            )
            joined[step, at, :] = state
            parts[step, 0, at, :], parts[step, 1, at, :] = two_parts(state * row(0, local, pair))
        sums[step, 0] = jnp.dot(parts[step, 0], ones, preferred_element_type=f32) + jnp.dot(
            parts[step, 1], ones, preferred_element_type=f32
        )
        sums[step, 1] = jnp.dot(parts[step, 2], ones, preferred_element_type=f32)
        for local, pair, at in blocks:
            new = (
                joined[step, at, :] * row(1, local, pair)
                - sums[step, 0, at, :] * row(2, local, pair)
                + sums[step, 1, at, :] * row(3, local, pair)
            )
            target = early if step == 0 else late_ref
            target[local, 2 * pair] = new[:, 0:size]
            target[local, 2 * pair + 1] = new[:, size:pair_width]
            parts[step, 0, at, :], parts[step, 1, at, :] = two_parts(new * row(4, local, pair))
        if step == 0:
            store.start()

    dims = (((1,), (1,)), ((), ()))
    lines = [[], []]
    for step in range(steps):
        found = lax.dot_general(pick, parts[step, 0], dims, preferred_element_type=f32)
        found += lax.dot_general(pick, parts[step, 1], dims, preferred_element_type=f32)
        for which in range(2):
            for local in range(SEQ_STEP):
                at = slice(local * pairs * size, (local + 1) * pairs * size)
                lines[which].append(found[which * 8 : which * 8 + 1, at])
    for which in range(2):
        read[which] = jnp.concatenate(lines[which], axis=0)

    mixed = []
    for pair in range(pairs):
        at = slice(pair * size, (pair + 1) * size)
        live = jnp.concatenate(
            [
                read[which, :, at] - jnp.mean(read[which, :, at], axis=1, keepdims=True)
                for which in range(2)
            ],
            axis=1,
        )
        spread = head_sums(jnp.square(live)) * (1.0 / size)
        gain = vectors[1, :, pair * pair_width : (pair + 1) * pair_width]
        mixed.append(live * lax.rsqrt(spread + GROUP_EPSILON) * gain)
    mixed = jnp.concatenate(mixed, axis=1).astype(bf16)
    weight_load.wait()
    product = jnp.dot(mixed, weight_here[...], preferred_element_type=f32).astype(bf16)
    quarter = out_ref.shape[2]
    for owner in range(owners):
        out_ref[owner] = product[:, owner * quarter : (owner + 1) * quarter]
    store.wait()


def heads_update(owners, state_in, receptance, key_in, value_in, learn_in, decay_in, decay_base, norm_gain, out_weight, route_ids, route_weights):
    seqs, heads, size, _ = state_in.shape
    width = out_weight.shape[1]
    channels = heads * size
    steps = 2
    step_rows = SEQ_STEP * heads // 2 * size
    any_space = pl.BlockSpec(memory_space=pl.ANY)
    half_shape = (SEQ_STEP, heads, size, size)
    top = route_ids.shape[1]
    new_state, product, late, routing = pl.pallas_call(
        functools.partial(heads_kernel, owners),
        in_specs=[any_space] * 11,
        out_specs=[any_space] + [pl.BlockSpec(memory_space=pltpu.VMEM)] * 3,
        out_shape=[
            jax.ShapeDtypeStruct(state_in.shape, jnp.float32),
            pltpu.VMEM((owners, seqs, width // owners), jnp.bfloat16),
            pltpu.VMEM(half_shape, jnp.float32),
            pltpu.VMEM((8, 128), jnp.bfloat16),
        ],
        scratch_shapes=[
            pltpu.VMEM(state_in.shape, jnp.float32),
            pltpu.VMEM(half_shape, jnp.float32),
            pltpu.VMEM((4, seqs, channels), jnp.bfloat16),
            pltpu.VMEM((seqs, channels), jnp.float32),
            pltpu.VMEM((2, 1, channels), jnp.float32),
            pltpu.VMEM((top, seqs), jnp.int32),
            pltpu.VMEM((top, seqs), jnp.float32),
            pltpu.VMEM((channels, width), jnp.bfloat16),
            pltpu.VMEM((6, heads // 2, seqs, 2 * size), jnp.float32),
            pltpu.VMEM((2, seqs, channels // 2), jnp.float32),
            pltpu.VMEM((steps, step_rows, 2 * size), jnp.float32),
            pltpu.VMEM((steps, 3, step_rows, 2 * size), jnp.bfloat16),
            pltpu.VMEM((steps, 2, step_rows, 2 * size), jnp.float32),
            pltpu.SemaphoreType.DMA((steps + 10,)),
            pltpu.SemaphoreType.DMA,
        ],
        compiler_params=pltpu.CompilerParams(vmem_limit_bytes=60 << 20),
        cost_estimate=pl.CostEstimate(flops=20_000_000, bytes_accessed=5_000_000, transcendentals=20_000),
    )(
        state_in,
        receptance,
        key_in,
        value_in,
        learn_in,
        decay_in,
        decay_base.reshape(1, channels),
        norm_gain.reshape(1, channels),
        out_weight,
        route_ids.T,
        route_weights.T,
    )
    return product, new_state, late, routing


def expert_kernel(
    got_ref, gain_ref, gate_ref, up_ref, down_ref, late_ref, state_ref, out_ref, new_state_ref, flat, stored
):
    f32 = jnp.float32
    store = pltpu.make_async_copy(
        late_ref, new_state_ref.at[pl.ds(SEQ_STEP, SEQ_STEP)], stored
    )
    store.start()
    senders, n_y, rows, quarter = got_ref.shape
    power = jnp.zeros((senders * rows, 128), f32)
    for y in range(n_y):
        flat[:, y * quarter : (y + 1) * quarter] = got_ref[:, y].reshape(senders * rows, quarter)
        for first in range(y * quarter, (y + 1) * quarter, 128):
            at = slice(first, first + 128)
            original = flat[:, at].astype(f32) * (1.0 / gain_ref[:, at])
            power += original * original
    mean = jnp.sum(power, axis=1, keepdims=True) * (1.0 / (n_y * quarter))
    scale = lax.rsqrt(mean + EPSILON)
    units = gate_ref.shape[2]
    weights = jnp.concatenate([gate_ref[0], up_ref[0]], axis=1)
    half = senders * rows // 2
    hidden = []
    for first in (0, half):
        both = jnp.dot(flat[first : first + half], weights, preferred_element_type=f32)
        both = both * scale[first : first + half]
        gate, upward = both[:, :units], both[:, units:]
        hidden.append((gate * jax.nn.sigmoid(gate) * upward).astype(jnp.bfloat16))
    hidden = jnp.concatenate(hidden, axis=0)
    for y in range(n_y):
        partial = jnp.dot(
            hidden, down_ref[0, :, y * quarter : (y + 1) * quarter], preferred_element_type=f32
        )
        out_ref[:, y] = partial.astype(jnp.bfloat16).reshape(senders, rows, quarter)
    store.wait()


def experts(got, routed_gain, expert_gate, expert_up, expert_down, late, new_state):
    senders, n_y, rows, quarter = got.shape
    vmem = pl.BlockSpec(memory_space=pltpu.VMEM)
    return pl.pallas_call(
        expert_kernel,
        in_specs=[vmem] * 6 + [pl.BlockSpec(memory_space=pl.ANY)],
        out_specs=[vmem, pl.BlockSpec(memory_space=pl.ANY)],
        out_shape=[
            jax.ShapeDtypeStruct(got.shape, jnp.bfloat16),
            jax.ShapeDtypeStruct(new_state.shape, new_state.dtype),
        ],
        input_output_aliases={6: 1},
        scratch_shapes=[
            pltpu.VMEM((senders * rows, n_y * quarter), jnp.bfloat16),
            pltpu.SemaphoreType.DMA,
        ],
        compiler_params=pltpu.CompilerParams(vmem_limit_bytes=12 << 20),
        cost_estimate=pl.CostEstimate(flops=400_000_000, bytes_accessed=4_000_000, transcendentals=40_000),
    )(got, routed_gain.reshape(1, n_y * quarter), expert_gate, expert_up, expert_down, late, new_state)


def pack_kernel(
    arrived_ref, hidden_ref, gain_ref, routing_ref, parcels_ref, own_ref
):
    f32, bf16 = jnp.float32, jnp.bfloat16
    seqs, quarter = own_ref.shape
    at = pl.ds(pl.multiple_of(lax.axis_index("y") * quarter, quarter), quarter)
    attention = jnp.sum(arrived_ref[...].astype(f32), axis=0).astype(bf16)
    residual = hidden_ref[:, at].astype(f32) + attention.astype(f32)
    own_ref[...] = residual
    gained = (residual * gain_ref[:, at]).astype(bf16)

    chunks = quarter // 128
    for z in range(parcels_ref.shape[0]):
        for chunk in range(chunks):
            parcels_ref[z, chunk * seqs : (chunk + 1) * seqs, :] = gained[
                :, chunk * 128 : (chunk + 1) * 128
            ]
        parcels_ref[z, chunks * seqs : chunks * seqs + 8, :] = routing_ref[...]


def pack(arrived, hidden_in, routed_gain, routing, n_z):
    n_y, seqs, quarter = arrived.shape
    width = n_y * quarter
    vmem = pl.BlockSpec(memory_space=pltpu.VMEM)
    return pl.pallas_call(
        pack_kernel,
        in_specs=[vmem] * 4,
        out_specs=[vmem] * 2,
        out_shape=[
            jax.ShapeDtypeStruct((n_z, quarter // 128 * seqs + 8, 128), jnp.bfloat16),
            jax.ShapeDtypeStruct((seqs, quarter), jnp.float32),
        ],
        compiler_params=pltpu.CompilerParams(vmem_limit_bytes=8 << 20),
    )(arrived, hidden_in, routed_gain.reshape(1, width), routing)


def choose_kernel(top, slots, rows_ref, chosen_ref, place_ref, weight_ref, flat, choice):
    f32, bf16 = jnp.float32, jnp.bfloat16
    n_z = rows_ref.shape[0]
    seqs = flat.shape[0] // n_z
    near, n_y, per_expert, piece = chosen_ref.shape
    tokens = n_z * seqs
    chunks = piece // 128
    sender_of = lax.broadcasted_iota(jnp.int32, (8, 128), 1) // seqs
    groups = tokens // 128
    per_group = 128 // seqs
    spread = [[jnp.zeros((8, 128), f32) for _ in range(groups)] for _ in range(4)]
    for z in range(n_z):
        for chunk in range(chunks):
            flat[z * seqs : (z + 1) * seqs, chunk * 128 : (chunk + 1) * 128] = rows_ref[
                z, chunk * seqs : (chunk + 1) * seqs, :
            ]
        routing = rows_ref[z, chunks * seqs : chunks * seqs + 8, :].astype(f32)
        group, place = divmod(z, per_group)
        for which in range(4):
            turn = (place - which) * seqs % 128
            moved = routing if turn == 0 else pltpu.roll(routing, turn, 1)
            spread[which][group] = jnp.where(sender_of == place, moved, spread[which][group])
    ids, high, middle, low = [jnp.concatenate(part, axis=1) for part in spread]
    weights = high + middle + low
    named = (
        lax.axis_index("zq") * near + lax.broadcasted_iota(jnp.int32, (near, tokens), 0)
    ).astype(f32)
    sender = (lax.broadcasted_iota(jnp.int32, (near, tokens), 1) // seqs * slots).astype(f32)
    place = jnp.full((near, tokens), -1.0, f32)
    weight = jnp.zeros((near, tokens), f32)
    for k in range(top):
        for slot in range(slots):
            hit = named + 128.0 * slot == ids[k : k + 1, :]
            place = jnp.where(hit, sender + slot, place)
            weight = jnp.where(hit, weights[k : k + 1, :], weight)
    place_ref[...] = place
    weight_ref[...] = weight
    row = lax.broadcasted_iota(jnp.int32, (per_expert, tokens), 0).astype(f32)
    for expert in range(near):
        choice[expert * per_expert : (expert + 1) * per_expert, :] = jnp.where(
            row == place[expert : expert + 1, :], 1.0, 0.0
        ).astype(bf16)
    chosen = jnp.dot(choice[...], flat[...], preferred_element_type=f32).astype(bf16)
    chosen = chosen.reshape(near, per_expert, piece)
    for y in range(n_y):
        chosen_ref[:, y] = chosen


def choose(rows, near, n_y, slots, top, seqs):
    n_z, depth, _ = rows.shape
    piece = (depth - 8) // seqs * 128
    tokens = n_z * seqs
    vmem = pl.BlockSpec(memory_space=pltpu.VMEM)
    return pl.pallas_call(
        functools.partial(choose_kernel, top, slots),
        in_specs=[vmem],
        out_specs=[vmem] * 3,
        out_shape=[
            jax.ShapeDtypeStruct((near, n_y, n_z * slots, piece), jnp.bfloat16),
            jax.ShapeDtypeStruct((near, tokens), jnp.float32),
            jax.ShapeDtypeStruct((near, tokens), jnp.float32),
        ],
        scratch_shapes=[
            pltpu.VMEM((tokens, piece), jnp.bfloat16),
            pltpu.VMEM((near * n_z * slots, tokens), jnp.bfloat16),
        ],
        compiler_params=pltpu.CompilerParams(vmem_limit_bytes=12 << 20),
    )(rows)


def combine_kernel(returned_ref, place_ref, weight_ref, out_ref, summed, choice):
    f32, bf16 = jnp.float32, jnp.bfloat16
    near, n_y, per_expert, piece = returned_ref.shape
    n_z, seqs, _ = out_ref.shape
    tokens = n_z * seqs
    total = near * per_expert
    row = lax.broadcasted_iota(jnp.int32, (per_expert, tokens), 0).astype(f32)
    for expert in range(near):
        at = slice(expert * per_expert, (expert + 1) * per_expert)
        result = jnp.sum(returned_ref[expert].astype(f32), axis=0).astype(bf16)
        summed[at, :] = result
        summed[total + expert * per_expert : total + (expert + 1) * per_expert, :] = result
        weight = jnp.where(
            row == place_ref[expert : expert + 1, :], weight_ref[expert : expert + 1, :], 0.0
        )
        high = weight.astype(bf16)
        choice[at, :] = high
        choice[total + expert * per_expert : total + (expert + 1) * per_expert, :] = (
            weight - high.astype(f32)
        ).astype(bf16)
    combined = lax.dot_general(
        choice[...], summed[...], (((0,), (0,)), ((), ())), preferred_element_type=f32
    )
    out_ref[...] = combined.astype(bf16).reshape(n_z, seqs, piece)


def combine(returned, place, weight, n_z):
    near, n_y, per_expert, piece = returned.shape
    tokens = place.shape[1]
    vmem = pl.BlockSpec(memory_space=pltpu.VMEM)
    return pl.pallas_call(
        combine_kernel,
        in_specs=[vmem] * 3,
        out_specs=vmem,
        out_shape=jax.ShapeDtypeStruct((n_z, tokens // n_z, piece), jnp.bfloat16),
        scratch_shapes=[
            pltpu.VMEM((2 * near * per_expert, piece), jnp.bfloat16),
            pltpu.VMEM((2 * near * per_expert, tokens), jnp.bfloat16),
        ],
        compiler_params=pltpu.CompilerParams(vmem_limit_bytes=12 << 20),
    )(returned, place, weight)


def on_device(
    hidden_in,
    state_in,
    receptance,
    key_in,
    value_in,
    learn_in,
    decay_in,
    decay_base,
    norm_gain,
    out_weight,
    routed_gain,
    expert_gate,
    expert_up,
    expert_down,
    route_ids,
    route_weights,
):
    n_y, n_zq = lax.axis_size("y"), lax.axis_size("zq")
    near = lax.axis_size(("zp", "x", "c"))
    seqs, width = hidden_in.shape
    quarter = width // n_y
    per_expert = n_zq * SLOTS

    product, new_state, late, routing = heads_update(
        n_y, state_in, receptance, key_in, value_in, learn_in, decay_in, decay_base, norm_gain, out_weight,
        route_ids, route_weights,
    )
    arrived = exchange(product, "y")
    parcels, own_residual = pack(arrived, hidden_in, routed_gain, routing, n_zq)
    rows = exchange(parcels, "zq")
    chosen, place, weight = choose(rows, near, n_y, SLOTS, route_ids.shape[1], seqs)
    got = exchange(chosen.reshape(near * n_y, per_expert, quarter), NEAR_AXES)
    got = got.reshape(near, n_y, per_expert, quarter)
    back, new_state = experts(got, routed_gain, expert_gate, expert_up, expert_down, late, new_state)
    returned = exchange(back.reshape(near * n_y, per_expert, quarter), NEAR_AXES)
    combined = combine(returned.reshape(near, n_y, per_expert, quarter), place, weight, n_zq)
    routed = exchange(combined, "zq").astype(jnp.float32).sum(axis=0)
    result = (own_residual + routed).astype(jnp.bfloat16)
    spread = exchange(jnp.broadcast_to(result, (n_y, seqs, quarter)), "y")
    return (spread.transpose(1, 0, 2).reshape(seqs, width), new_state)


def solution(mesh):
    near_mesh = Mesh(mesh.devices.reshape(8, 2, 4, 2, 4), ("zq", "zp", "x", "c", "y"))
    in_specs = (
        P(EP, None),
        P(EP, "y", None, None),
        P(EP, "y"),
        P(EP, "y"),
        P(EP, "y"),
        P(EP, "y"),
        P(EP, "y"),
        P("y"),
        P("y"),
        P("y", None),
        P(),
        P(EP, None, "y"),
        P(EP, None, "y"),
        P(EP, "y", None),
        P(EP, None),
        P(EP, None),
    )
    out_specs = (P(EP, None), P(EP, "y", None, None))
    return jax.shard_map(
        on_device, mesh=near_mesh, in_specs=in_specs, out_specs=out_specs, check_vma=False
    )
```

```python
import functools
import math
import jax
import jax.numpy as jnp
import numpy as np
from jax import lax
from jax.experimental import pallas as pl
from jax.experimental.pallas import tpu as pltpu
from jax.sharding import Mesh, PartitionSpec as P

EPSILON = 1e-06
GROUP_EPSILON = 0.00064
SEQ_STEP = 8
SEQ_COPY = 4
SLOTS = 2
NEAR_AXES = ("zp", "x", "c", "y")
EP = ("zq", "zp", "x", "c")


def exchange(pieces, axes):
    return lax.all_to_all(pieces, axes, split_axis=0, concat_axis=0, tiled=True)


def two_parts(values):
    high = values.astype(jnp.bfloat16)
    return high, (values - high.astype(jnp.float32)).astype(jnp.bfloat16)


def routing_rows(ids, shares):
    f32, bf16 = jnp.float32, jnp.bfloat16
    top, seqs = ids.shape
    lane = lax.broadcasted_iota(jnp.int32, (8, 128), 1)
    ids = jnp.pad(ids, ((0, 8 - top), (0, 128 - seqs)))
    again = jnp.zeros((8, 128), jnp.int32)
    for k in range(top):
        line = jnp.broadcast_to(ids[k : k + 1], (8, 128))
        for back in range(1, seqs):
            same = (pltpu.roll(line, back, 1) == ids) & (lane >= back)
            again = jnp.where(same, 128, again)
    parts = [(ids + again)[:, :seqs].astype(f32)]
    shares = jnp.pad(shares, ((0, 8 - top), (0, 0)))
    for _ in range(3):
        part = shares.astype(bf16).astype(f32)
        parts.append(part)
        shares = shares - part
    parts.append(jnp.zeros((8, 128 - len(parts) * seqs), f32))
    return jnp.concatenate(parts, axis=1).astype(bf16)


def heads_kernel(
    owners,
    state_ref,
    reading_ref,
    key_ref,
    value_ref,
    learn_ref,
    decay_ref,
    base_ref,
    gain_ref,
    weight_ref,
    ids_ref,
    shares_ref,
    new_state_ref,
    out_ref,
    late_ref,
    routing_ref,
    state_here,
    early,
    inputs,
    decay_here,
    vectors,
    ids_here,
    shares_here,
    weight_here,
    rows,
    read,
    joined,
    parts,
    sums,
    arrived,
    stored,
):
    f32, bf16 = jnp.float32, jnp.bfloat16
    seqs, heads, size, _ = state_here.shape
    channels = heads * size
    pairs = heads // 2
    pair_width = 2 * size
    steps = 2

    chunks = seqs // SEQ_COPY

    def state_load(chunk):
        at = pl.ds(chunk * SEQ_COPY, SEQ_COPY)
        return pltpu.make_async_copy(state_ref.at[at], state_here.at[at], arrived.at[chunk])

    store = pltpu.make_async_copy(early, new_state_ref.at[pl.ds(0, SEQ_STEP)], stored)

    small = [
        pltpu.make_async_copy(source, target, arrived.at[chunks + number])
        for number, (source, target) in enumerate(
            (
                (key_ref, inputs.at[0]),
                (learn_ref, inputs.at[1]),
                (decay_ref, decay_here),
                (base_ref, vectors.at[0]),
                (reading_ref, inputs.at[2]),
                (value_ref, inputs.at[3]),
                (gain_ref, vectors.at[1]),
                (ids_ref, ids_here),
                (shares_ref, shares_here),
            )
        )
    ]
    weight_load = pltpu.make_async_copy(weight_ref, weight_here, arrived.at[chunks + len(small)])
    for load in small:
        load.start()
    for chunk in range(chunks):
        state_load(chunk).start()
    weight_load.start()

    square = (pair_width, pair_width)
    same_head = (
        lax.broadcasted_iota(jnp.int32, square, 0) // size
        == lax.broadcasted_iota(jnp.int32, square, 1) // size
    )
    ones = jnp.where(same_head, 1.0, 0.0).astype(bf16)

    def head_sums(values):
        return sum(jnp.dot(part, ones, preferred_element_type=f32) for part in two_parts(values))

    for load in small:
        load.wait()
    keys = inputs[0].astype(f32)
    learning = jax.nn.sigmoid(inputs[1].astype(f32))
    decay = jnp.exp(-math.exp(-0.5) * jax.nn.sigmoid(vectors[0] + decay_here[...]))
    for pair in range(pairs):
        at = slice(pair * pair_width, (pair + 1) * pair_width)
        key = keys[:, at]
        unit = key * lax.rsqrt(head_sums(key * key) + EPSILON)
        rows[0, pair] = unit
        rows[1, pair] = decay[:, at]
        rows[2, pair] = unit * learning[:, at]
        rows[3, pair] = key
        rows[4, pair] = inputs[2, :, at].astype(f32)
        rows[5, pair] = inputs[3, :, at].astype(f32)

    routing_ref[...] = routing_rows(ids_here[...], shares_here[...])

    blocks = [
        (local, pair, slice((local * pairs + pair) * size, (local * pairs + pair + 1) * size))
        for local in range(SEQ_STEP)
        for pair in range(pairs)
    ]
    on_diagonal = lax.broadcasted_iota(jnp.int32, (size, pair_width), 0) == (
        lax.broadcasted_iota(jnp.int32, (size, pair_width), 1) % size
    )
    head_of = lax.broadcasted_iota(jnp.int32, (2 * 8, pair_width), 0) // 8
    pick = jnp.where(
        head_of == lax.broadcasted_iota(jnp.int32, (2 * 8, pair_width), 1) // size, 1.0, 0.0
    ).astype(bf16)

    for step in range(steps):
        first = step * SEQ_STEP

        def row(which, local, pair):
            return rows[which, pair, first + local : first + local + 1, :]

        for local, pair, at in blocks:
            if pair == 0 and local % SEQ_COPY == 0:
                state_load((first + local) // SEQ_COPY).wait()
            parts[step, 2, at, :] = jnp.where(on_diagonal, row(5, local, pair), 0.0).astype(bf16)
            state = jnp.concatenate(
                [state_here[first + local, 2 * pair], state_here[first + local, 2 * pair + 1]], axis=1
            )
            joined[step, at, :] = state
            parts[step, 0, at, :], parts[step, 1, at, :] = two_parts(state * row(0, local, pair))
        sums[step, 0] = jnp.dot(parts[step, 0], ones, preferred_element_type=f32) + jnp.dot(
            parts[step, 1], ones, preferred_element_type=f32
        )
        sums[step, 1] = jnp.dot(parts[step, 2], ones, preferred_element_type=f32)
        for local, pair, at in blocks:
            new = (
                joined[step, at, :] * row(1, local, pair)
                - sums[step, 0, at, :] * row(2, local, pair)
                + sums[step, 1, at, :] * row(3, local, pair)
            )
            target = early if step == 0 else late_ref
            target[local, 2 * pair] = new[:, 0:size]
            target[local, 2 * pair + 1] = new[:, size:pair_width]
            parts[step, 0, at, :], parts[step, 1, at, :] = two_parts(new * row(4, local, pair))
        if step == 0:
            store.start()

    dims = (((1,), (1,)), ((), ()))
    lines = [[], []]
    for step in range(steps):
        found = lax.dot_general(pick, parts[step, 0], dims, preferred_element_type=f32)
        found += lax.dot_general(pick, parts[step, 1], dims, preferred_element_type=f32)
        for which in range(2):
            for local in range(SEQ_STEP):
                at = slice(local * pairs * size, (local + 1) * pairs * size)
                lines[which].append(found[which * 8 : which * 8 + 1, at])
    for which in range(2):
        read[which] = jnp.concatenate(lines[which], axis=0)

    mixed = []
    for pair in range(pairs):
        at = slice(pair * size, (pair + 1) * size)
        live = jnp.concatenate(
            [
                read[which, :, at] - jnp.mean(read[which, :, at], axis=1, keepdims=True)
                for which in range(2)
            ],
            axis=1,
        )
        spread = head_sums(jnp.square(live)) * (1.0 / size)
        gain = vectors[1, :, pair * pair_width : (pair + 1) * pair_width]
        mixed.append(live * lax.rsqrt(spread + GROUP_EPSILON) * gain)
    mixed = jnp.concatenate(mixed, axis=1).astype(bf16)
    weight_load.wait()
    product = jnp.dot(mixed, weight_here[...], preferred_element_type=f32).astype(bf16)
    quarter = out_ref.shape[2]
    for owner in range(owners):
        out_ref[owner] = product[:, owner * quarter : (owner + 1) * quarter]
    store.wait()


def heads_update(owners, state_in, receptance, key_in, value_in, learn_in, decay_in, decay_base, norm_gain, out_weight, route_ids, route_weights):
    seqs, heads, size, _ = state_in.shape
    width = out_weight.shape[1]
    channels = heads * size
    steps = 2
    step_rows = SEQ_STEP * heads // 2 * size
    any_space = pl.BlockSpec(memory_space=pl.ANY)
    half_shape = (SEQ_STEP, heads, size, size)
    top = route_ids.shape[1]
    new_state, product, late, routing = pl.pallas_call(
        functools.partial(heads_kernel, owners),
        in_specs=[any_space] * 11,
        out_specs=[any_space] + [pl.BlockSpec(memory_space=pltpu.VMEM)] * 3,
        out_shape=[
            jax.ShapeDtypeStruct(state_in.shape, jnp.float32),
            pltpu.VMEM((owners, seqs, width // owners), jnp.bfloat16),
            pltpu.VMEM(half_shape, jnp.float32),
            pltpu.VMEM((8, 128), jnp.bfloat16),
        ],
        scratch_shapes=[
            pltpu.VMEM(state_in.shape, jnp.float32),
            pltpu.VMEM(half_shape, jnp.float32),
            pltpu.VMEM((4, seqs, channels), jnp.bfloat16),
            pltpu.VMEM((seqs, channels), jnp.float32),
            pltpu.VMEM((2, 1, channels), jnp.float32),
            pltpu.VMEM((top, seqs), jnp.int32),
            pltpu.VMEM((top, seqs), jnp.float32),
            pltpu.VMEM((channels, width), jnp.bfloat16),
            pltpu.VMEM((6, heads // 2, seqs, 2 * size), jnp.float32),
            pltpu.VMEM((2, seqs, channels // 2), jnp.float32),
            pltpu.VMEM((steps, step_rows, 2 * size), jnp.float32),
            pltpu.VMEM((steps, 3, step_rows, 2 * size), jnp.bfloat16),
            pltpu.VMEM((steps, 2, step_rows, 2 * size), jnp.float32),
            pltpu.SemaphoreType.DMA((seqs // SEQ_COPY + 10,)),
            pltpu.SemaphoreType.DMA,
        ],
        compiler_params=pltpu.CompilerParams(vmem_limit_bytes=60 << 20),
        cost_estimate=pl.CostEstimate(flops=20_000_000, bytes_accessed=5_000_000, transcendentals=20_000),
    )(
        state_in,
        receptance,
        key_in,
        value_in,
        learn_in,
        decay_in,
        decay_base.reshape(1, channels),
        norm_gain.reshape(1, channels),
        out_weight,
        route_ids.T,
        route_weights.T,
    )
    return product, new_state, late, routing


def expert_kernel(
    got_ref, gain_ref, gate_ref, up_ref, down_ref, late_ref, state_ref, out_ref, new_state_ref, flat, stored
):
    f32 = jnp.float32
    store = pltpu.make_async_copy(
        late_ref, new_state_ref.at[pl.ds(SEQ_STEP, SEQ_STEP)], stored
    )
    store.start()
    senders, n_y, rows, quarter = got_ref.shape
    power = jnp.zeros((senders * rows, 128), f32)
    for y in range(n_y):
        flat[:, y * quarter : (y + 1) * quarter] = got_ref[:, y].reshape(senders * rows, quarter)
        for first in range(y * quarter, (y + 1) * quarter, 128):
            at = slice(first, first + 128)
            original = flat[:, at].astype(f32) * (1.0 / gain_ref[:, at])
            power += original * original
    mean = jnp.sum(power, axis=1, keepdims=True) * (1.0 / (n_y * quarter))
    scale = lax.rsqrt(mean + EPSILON)
    units = gate_ref.shape[2]
    weights = jnp.concatenate([gate_ref[0], up_ref[0]], axis=1)
    half = senders * rows // 2
    hidden = []
    for first in (0, half):
        both = jnp.dot(flat[first : first + half], weights, preferred_element_type=f32)
        both = both * scale[first : first + half]
        gate, upward = both[:, :units], both[:, units:]
        hidden.append((gate * jax.nn.sigmoid(gate) * upward).astype(jnp.bfloat16))
    hidden = jnp.concatenate(hidden, axis=0)
    for y in range(n_y):
        partial = jnp.dot(
            hidden, down_ref[0, :, y * quarter : (y + 1) * quarter], preferred_element_type=f32
        )
        out_ref[:, y] = partial.astype(jnp.bfloat16).reshape(senders, rows, quarter)
    store.wait()


def experts(got, routed_gain, expert_gate, expert_up, expert_down, late, new_state):
    senders, n_y, rows, quarter = got.shape
    vmem = pl.BlockSpec(memory_space=pltpu.VMEM)
    return pl.pallas_call(
        expert_kernel,
        in_specs=[vmem] * 6 + [pl.BlockSpec(memory_space=pl.ANY)],
        out_specs=[vmem, pl.BlockSpec(memory_space=pl.ANY)],
        out_shape=[
            jax.ShapeDtypeStruct(got.shape, jnp.bfloat16),
            jax.ShapeDtypeStruct(new_state.shape, new_state.dtype),
        ],
        input_output_aliases={6: 1},
        scratch_shapes=[
            pltpu.VMEM((senders * rows, n_y * quarter), jnp.bfloat16),
            pltpu.SemaphoreType.DMA,
        ],
        compiler_params=pltpu.CompilerParams(vmem_limit_bytes=12 << 20),
        cost_estimate=pl.CostEstimate(flops=400_000_000, bytes_accessed=4_000_000, transcendentals=40_000),
    )(got, routed_gain.reshape(1, n_y * quarter), expert_gate, expert_up, expert_down, late, new_state)


def pack_kernel(
    arrived_ref, hidden_ref, gain_ref, routing_ref, parcels_ref, own_ref
):
    f32, bf16 = jnp.float32, jnp.bfloat16
    seqs, quarter = own_ref.shape
    at = pl.ds(pl.multiple_of(lax.axis_index("y") * quarter, quarter), quarter)
    attention = jnp.sum(arrived_ref[...].astype(f32), axis=0).astype(bf16)
    residual = hidden_ref[:, at].astype(f32) + attention.astype(f32)
    own_ref[...] = residual
    gained = (residual * gain_ref[:, at]).astype(bf16)

    chunks = quarter // 128
    for z in range(parcels_ref.shape[0]):
        for chunk in range(chunks):
            parcels_ref[z, chunk * seqs : (chunk + 1) * seqs, :] = gained[
                :, chunk * 128 : (chunk + 1) * 128
            ]
        parcels_ref[z, chunks * seqs : chunks * seqs + 8, :] = routing_ref[...]


def pack(arrived, hidden_in, routed_gain, routing, n_z):
    n_y, seqs, quarter = arrived.shape
    width = n_y * quarter
    vmem = pl.BlockSpec(memory_space=pltpu.VMEM)
    return pl.pallas_call(
        pack_kernel,
        in_specs=[vmem] * 4,
        out_specs=[vmem] * 2,
        out_shape=[
            jax.ShapeDtypeStruct((n_z, quarter // 128 * seqs + 8, 128), jnp.bfloat16),
            jax.ShapeDtypeStruct((seqs, quarter), jnp.float32),
        ],
        compiler_params=pltpu.CompilerParams(vmem_limit_bytes=8 << 20),
    )(arrived, hidden_in, routed_gain.reshape(1, width), routing)


def choose_kernel(top, slots, rows_ref, chosen_ref, place_ref, weight_ref, flat, choice):
    f32, bf16 = jnp.float32, jnp.bfloat16
    n_z = rows_ref.shape[0]
    seqs = flat.shape[0] // n_z
    near, n_y, per_expert, piece = chosen_ref.shape
    tokens = n_z * seqs
    chunks = piece // 128
    sender_of = lax.broadcasted_iota(jnp.int32, (8, 128), 1) // seqs
    groups = tokens // 128
    per_group = 128 // seqs
    spread = [[jnp.zeros((8, 128), f32) for _ in range(groups)] for _ in range(4)]
    for z in range(n_z):
        for chunk in range(chunks):
            flat[z * seqs : (z + 1) * seqs, chunk * 128 : (chunk + 1) * 128] = rows_ref[
                z, chunk * seqs : (chunk + 1) * seqs, :
            ]
        routing = rows_ref[z, chunks * seqs : chunks * seqs + 8, :].astype(f32)
        group, place = divmod(z, per_group)
        for which in range(4):
            turn = (place - which) * seqs % 128
            moved = routing if turn == 0 else pltpu.roll(routing, turn, 1)
            spread[which][group] = jnp.where(sender_of == place, moved, spread[which][group])
    ids, high, middle, low = [jnp.concatenate(part, axis=1) for part in spread]
    weights = high + middle + low
    named = (
        lax.axis_index("zq") * near + lax.broadcasted_iota(jnp.int32, (near, tokens), 0)
    ).astype(f32)
    sender = (lax.broadcasted_iota(jnp.int32, (near, tokens), 1) // seqs * slots).astype(f32)
    place = jnp.full((near, tokens), -1.0, f32)
    weight = jnp.zeros((near, tokens), f32)
    for k in range(top):
        for slot in range(slots):
            hit = named + 128.0 * slot == ids[k : k + 1, :]
            place = jnp.where(hit, sender + slot, place)
            weight = jnp.where(hit, weights[k : k + 1, :], weight)
    place_ref[...] = place
    weight_ref[...] = weight
    row = lax.broadcasted_iota(jnp.int32, (per_expert, tokens), 0).astype(f32)
    for expert in range(near):
        choice[expert * per_expert : (expert + 1) * per_expert, :] = jnp.where(
            row == place[expert : expert + 1, :], 1.0, 0.0
        ).astype(bf16)
    chosen = jnp.dot(choice[...], flat[...], preferred_element_type=f32).astype(bf16)
    chosen = chosen.reshape(near, per_expert, piece)
    for y in range(n_y):
        chosen_ref[:, y] = chosen


def choose(rows, near, n_y, slots, top, seqs):
    n_z, depth, _ = rows.shape
    piece = (depth - 8) // seqs * 128
    tokens = n_z * seqs
    vmem = pl.BlockSpec(memory_space=pltpu.VMEM)
    return pl.pallas_call(
        functools.partial(choose_kernel, top, slots),
        in_specs=[vmem],
        out_specs=[vmem] * 3,
        out_shape=[
            jax.ShapeDtypeStruct((near, n_y, n_z * slots, piece), jnp.bfloat16),
            jax.ShapeDtypeStruct((near, tokens), jnp.float32),
            jax.ShapeDtypeStruct((near, tokens), jnp.float32),
        ],
        scratch_shapes=[
            pltpu.VMEM((tokens, piece), jnp.bfloat16),
            pltpu.VMEM((near * n_z * slots, tokens), jnp.bfloat16),
        ],
        compiler_params=pltpu.CompilerParams(vmem_limit_bytes=12 << 20),
    )(rows)


def combine_kernel(returned_ref, place_ref, weight_ref, out_ref, summed, choice):
    f32, bf16 = jnp.float32, jnp.bfloat16
    near, n_y, per_expert, piece = returned_ref.shape
    n_z, seqs, _ = out_ref.shape
    tokens = n_z * seqs
    total = near * per_expert
    row = lax.broadcasted_iota(jnp.int32, (per_expert, tokens), 0).astype(f32)
    for expert in range(near):
        at = slice(expert * per_expert, (expert + 1) * per_expert)
        result = jnp.sum(returned_ref[expert].astype(f32), axis=0).astype(bf16)
        summed[at, :] = result
        summed[total + expert * per_expert : total + (expert + 1) * per_expert, :] = result
        weight = jnp.where(
            row == place_ref[expert : expert + 1, :], weight_ref[expert : expert + 1, :], 0.0
        )
        high = weight.astype(bf16)
        choice[at, :] = high
        choice[total + expert * per_expert : total + (expert + 1) * per_expert, :] = (
            weight - high.astype(f32)
        ).astype(bf16)
    combined = lax.dot_general(
        choice[...], summed[...], (((0,), (0,)), ((), ())), preferred_element_type=f32
    )
    out_ref[...] = combined.astype(bf16).reshape(n_z, seqs, piece)


def combine(returned, place, weight, n_z):
    near, n_y, per_expert, piece = returned.shape
    tokens = place.shape[1]
    vmem = pl.BlockSpec(memory_space=pltpu.VMEM)
    return pl.pallas_call(
        combine_kernel,
        in_specs=[vmem] * 3,
        out_specs=vmem,
        out_shape=jax.ShapeDtypeStruct((n_z, tokens // n_z, piece), jnp.bfloat16),
        scratch_shapes=[
            pltpu.VMEM((2 * near * per_expert, piece), jnp.bfloat16),
            pltpu.VMEM((2 * near * per_expert, tokens), jnp.bfloat16),
        ],
        compiler_params=pltpu.CompilerParams(vmem_limit_bytes=12 << 20),
    )(returned, place, weight)


def on_device(
    hidden_in,
    state_in,
    receptance,
    key_in,
    value_in,
    learn_in,
    decay_in,
    decay_base,
    norm_gain,
    out_weight,
    routed_gain,
    expert_gate,
    expert_up,
    expert_down,
    route_ids,
    route_weights,
):
    n_y, n_zq = lax.axis_size("y"), lax.axis_size("zq")
    near = lax.axis_size(("zp", "x", "c"))
    seqs, width = hidden_in.shape
    quarter = width // n_y
    per_expert = n_zq * SLOTS

    product, new_state, late, routing = heads_update(
        n_y, state_in, receptance, key_in, value_in, learn_in, decay_in, decay_base, norm_gain, out_weight,
        route_ids, route_weights,
    )
    arrived = exchange(product, "y")
    parcels, own_residual = pack(arrived, hidden_in, routed_gain, routing, n_zq)
    rows = exchange(parcels, "zq")
    chosen, place, weight = choose(rows, near, n_y, SLOTS, route_ids.shape[1], seqs)
    got = exchange(chosen.reshape(near * n_y, per_expert, quarter), NEAR_AXES)
    got = got.reshape(near, n_y, per_expert, quarter)
    back, new_state = experts(got, routed_gain, expert_gate, expert_up, expert_down, late, new_state)
    returned = exchange(back.reshape(near * n_y, per_expert, quarter), NEAR_AXES)
    combined = combine(returned.reshape(near, n_y, per_expert, quarter), place, weight, n_zq)
    routed = exchange(combined, "zq").astype(jnp.float32).sum(axis=0)
    result = (own_residual + routed).astype(jnp.bfloat16)
    spread = exchange(jnp.broadcast_to(result, (n_y, seqs, quarter)), "y")
    return (spread.transpose(1, 0, 2).reshape(seqs, width), new_state)


def solution(mesh):
    near_mesh = Mesh(mesh.devices.reshape(8, 2, 4, 2, 4), ("zq", "zp", "x", "c", "y"))
    in_specs = (
        P(EP, None),
        P(EP, "y", None, None),
        P(EP, "y"),
        P(EP, "y"),
        P(EP, "y"),
        P(EP, "y"),
        P(EP, "y"),
        P("y"),
        P("y"),
        P("y", None),
        P(),
        P(EP, None, "y"),
        P(EP, None, "y"),
        P(EP, "y", None),
        P(EP, None),
        P(EP, None),
    )
    out_specs = (P(EP, None), P(EP, "y", None, None))
    return jax.shard_map(
        on_device, mesh=near_mesh, in_specs=in_specs, out_specs=out_specs, check_vma=False
    )
```

```python
import functools
import math
import jax
import jax.numpy as jnp
import numpy as np
from jax import lax
from jax.experimental import pallas as pl
from jax.experimental.pallas import tpu as pltpu
from jax.sharding import Mesh, PartitionSpec as P

EPSILON = 1e-06
GROUP_EPSILON = 0.00064
SEQ_STEP = 8
SEQ_COPY = 4
SLOTS = 2
NEAR_AXES = ("zp", "x", "c", "y")
EP = ("zq", "zp", "x", "c")


def exchange(pieces, axes):
    return lax.all_to_all(pieces, axes, split_axis=0, concat_axis=0, tiled=True)


def two_parts(values):
    high = values.astype(jnp.bfloat16)
    return high, (values - high.astype(jnp.float32)).astype(jnp.bfloat16)


def routing_rows(ids, shares):
    f32, bf16 = jnp.float32, jnp.bfloat16
    top, seqs = ids.shape
    lane = lax.broadcasted_iota(jnp.int32, (8, 128), 1)
    ids = jnp.pad(ids, ((0, 8 - top), (0, 128 - seqs)))
    again = jnp.zeros((8, 128), jnp.int32)
    for k in range(top):
        line = jnp.broadcast_to(ids[k : k + 1], (8, 128))
        for back in range(1, seqs):
            same = (pltpu.roll(line, back, 1) == ids) & (lane >= back)
            again = jnp.where(same, 128, again)
    parts = [(ids + again)[:, :seqs].astype(f32)]
    shares = jnp.pad(shares, ((0, 8 - top), (0, 0)))
    for _ in range(3):
        part = shares.astype(bf16).astype(f32)
        parts.append(part)
        shares = shares - part
    parts.append(jnp.zeros((8, 128 - len(parts) * seqs), f32))
    return jnp.concatenate(parts, axis=1).astype(bf16)


def heads_kernel(
    owners,
    state_ref,
    reading_ref,
    key_ref,
    value_ref,
    learn_ref,
    decay_ref,
    base_ref,
    gain_ref,
    weight_ref,
    ids_ref,
    shares_ref,
    new_state_ref,
    out_ref,
    late_ref,
    routing_ref,
    state_here,
    early,
    inputs,
    decay_here,
    vectors,
    ids_here,
    shares_here,
    weight_here,
    rows,
    read,
    joined,
    parts,
    sums,
    arrived,
    stored,
):
    f32, bf16 = jnp.float32, jnp.bfloat16
    seqs, heads, size, _ = state_here.shape
    channels = heads * size
    pairs = heads // 2
    pair_width = 2 * size
    steps = 2

    chunks = seqs // SEQ_COPY

    def state_load(chunk):
        at = pl.ds(chunk * SEQ_COPY, SEQ_COPY)
        return pltpu.make_async_copy(state_ref.at[at], state_here.at[at], arrived.at[chunk])

    store = pltpu.make_async_copy(early, new_state_ref.at[pl.ds(0, SEQ_STEP)], stored)

    small = [
        pltpu.make_async_copy(source, target, arrived.at[chunks + number])
        for number, (source, target) in enumerate(
            (
                (key_ref, inputs.at[0]),
                (learn_ref, inputs.at[1]),
                (decay_ref, decay_here),
                (base_ref, vectors.at[0]),
                (reading_ref, inputs.at[2]),
                (value_ref, inputs.at[3]),
                (gain_ref, vectors.at[1]),
                (ids_ref, ids_here),
                (shares_ref, shares_here),
            )
        )
    ]
    weight_load = pltpu.make_async_copy(weight_ref, weight_here, arrived.at[chunks + len(small)])
    state_load(0).start()
    for load in small:
        load.start()
    for chunk in range(1, chunks):
        state_load(chunk).start()
    weight_load.start()

    square = (pair_width, pair_width)
    same_head = (
        lax.broadcasted_iota(jnp.int32, square, 0) // size
        == lax.broadcasted_iota(jnp.int32, square, 1) // size
    )
    ones = jnp.where(same_head, 1.0, 0.0).astype(bf16)

    def head_sums(values):
        return sum(jnp.dot(part, ones, preferred_element_type=f32) for part in two_parts(values))

    for load in small:
        load.wait()
    keys = inputs[0].astype(f32)
    learning = jax.nn.sigmoid(inputs[1].astype(f32))
    decay = jnp.exp(-math.exp(-0.5) * jax.nn.sigmoid(vectors[0] + decay_here[...]))
    for pair in range(pairs):
        at = slice(pair * pair_width, (pair + 1) * pair_width)
        key = keys[:, at]
        unit = key * lax.rsqrt(head_sums(key * key) + EPSILON)
        rows[0, pair] = unit
        rows[1, pair] = decay[:, at]
        rows[2, pair] = unit * learning[:, at]
        rows[3, pair] = key
        rows[4, pair] = inputs[2, :, at].astype(f32)
        rows[5, pair] = inputs[3, :, at].astype(f32)

    routing_ref[...] = routing_rows(ids_here[...], shares_here[...])

    blocks = [
        (local, pair, slice((local * pairs + pair) * size, (local * pairs + pair + 1) * size))
        for local in range(SEQ_STEP)
        for pair in range(pairs)
    ]
    on_diagonal = lax.broadcasted_iota(jnp.int32, (size, pair_width), 0) == (
        lax.broadcasted_iota(jnp.int32, (size, pair_width), 1) % size
    )
    head_of = lax.broadcasted_iota(jnp.int32, (2 * 8, pair_width), 0) // 8
    pick = jnp.where(
        head_of == lax.broadcasted_iota(jnp.int32, (2 * 8, pair_width), 1) // size, 1.0, 0.0
    ).astype(bf16)

    for step in range(steps):
        first = step * SEQ_STEP

        def row(which, local, pair):
            return rows[which, pair, first + local : first + local + 1, :]

        for local, pair, at in blocks:
            if pair == 0 and local % SEQ_COPY == 0:
                state_load((first + local) // SEQ_COPY).wait()
            parts[step, 2, at, :] = jnp.where(on_diagonal, row(5, local, pair), 0.0).astype(bf16)
            state = jnp.concatenate(
                [state_here[first + local, 2 * pair], state_here[first + local, 2 * pair + 1]], axis=1
            )
            joined[step, at, :] = state
            parts[step, 0, at, :], parts[step, 1, at, :] = two_parts(state * row(0, local, pair))
        sums[step, 0] = jnp.dot(parts[step, 0], ones, preferred_element_type=f32) + jnp.dot(
            parts[step, 1], ones, preferred_element_type=f32
        )
        sums[step, 1] = jnp.dot(parts[step, 2], ones, preferred_element_type=f32)
        for local, pair, at in blocks:
            new = (
                joined[step, at, :] * row(1, local, pair)
                - sums[step, 0, at, :] * row(2, local, pair)
                + sums[step, 1, at, :] * row(3, local, pair)
            )
            target = early if step == 0 else late_ref
            target[local, 2 * pair] = new[:, 0:size]
            target[local, 2 * pair + 1] = new[:, size:pair_width]
            parts[step, 0, at, :], parts[step, 1, at, :] = two_parts(new * row(4, local, pair))
        if step == 0:
            store.start()

    dims = (((1,), (1,)), ((), ()))
    lines = [[], []]
    for step in range(steps):
        found = lax.dot_general(pick, parts[step, 0], dims, preferred_element_type=f32)
        found += lax.dot_general(pick, parts[step, 1], dims, preferred_element_type=f32)
        for which in range(2):
            for local in range(SEQ_STEP):
                at = slice(local * pairs * size, (local + 1) * pairs * size)
                lines[which].append(found[which * 8 : which * 8 + 1, at])
    for which in range(2):
        read[which] = jnp.concatenate(lines[which], axis=0)

    mixed = []
    for pair in range(pairs):
        at = slice(pair * size, (pair + 1) * size)
        live = jnp.concatenate(
            [
                read[which, :, at] - jnp.mean(read[which, :, at], axis=1, keepdims=True)
                for which in range(2)
            ],
            axis=1,
        )
        spread = head_sums(jnp.square(live)) * (1.0 / size)
        gain = vectors[1, :, pair * pair_width : (pair + 1) * pair_width]
        mixed.append(live * lax.rsqrt(spread + GROUP_EPSILON) * gain)
    mixed = jnp.concatenate(mixed, axis=1).astype(bf16)
    weight_load.wait()
    product = jnp.dot(mixed, weight_here[...], preferred_element_type=f32).astype(bf16)
    quarter = out_ref.shape[2]
    for owner in range(owners):
        out_ref[owner] = product[:, owner * quarter : (owner + 1) * quarter]
    store.wait()


def heads_update(owners, state_in, receptance, key_in, value_in, learn_in, decay_in, decay_base, norm_gain, out_weight, route_ids, route_weights):
    seqs, heads, size, _ = state_in.shape
    width = out_weight.shape[1]
    channels = heads * size
    steps = 2
    step_rows = SEQ_STEP * heads // 2 * size
    any_space = pl.BlockSpec(memory_space=pl.ANY)
    half_shape = (SEQ_STEP, heads, size, size)
    top = route_ids.shape[1]
    new_state, product, late, routing = pl.pallas_call(
        functools.partial(heads_kernel, owners),
        in_specs=[any_space] * 11,
        out_specs=[any_space] + [pl.BlockSpec(memory_space=pltpu.VMEM)] * 3,
        out_shape=[
            jax.ShapeDtypeStruct(state_in.shape, jnp.float32),
            pltpu.VMEM((owners, seqs, width // owners), jnp.bfloat16),
            pltpu.VMEM(half_shape, jnp.float32),
            pltpu.VMEM((8, 128), jnp.bfloat16),
        ],
        scratch_shapes=[
            pltpu.VMEM(state_in.shape, jnp.float32),
            pltpu.VMEM(half_shape, jnp.float32),
            pltpu.VMEM((4, seqs, channels), jnp.bfloat16),
            pltpu.VMEM((seqs, channels), jnp.float32),
            pltpu.VMEM((2, 1, channels), jnp.float32),
            pltpu.VMEM((top, seqs), jnp.int32),
            pltpu.VMEM((top, seqs), jnp.float32),
            pltpu.VMEM((channels, width), jnp.bfloat16),
            pltpu.VMEM((6, heads // 2, seqs, 2 * size), jnp.float32),
            pltpu.VMEM((2, seqs, channels // 2), jnp.float32),
            pltpu.VMEM((steps, step_rows, 2 * size), jnp.float32),
            pltpu.VMEM((steps, 3, step_rows, 2 * size), jnp.bfloat16),
            pltpu.VMEM((steps, 2, step_rows, 2 * size), jnp.float32),
            pltpu.SemaphoreType.DMA((seqs // SEQ_COPY + 10,)),
            pltpu.SemaphoreType.DMA,
        ],
        compiler_params=pltpu.CompilerParams(vmem_limit_bytes=60 << 20),
        cost_estimate=pl.CostEstimate(flops=20_000_000, bytes_accessed=5_000_000, transcendentals=20_000),
    )(
        state_in,
        receptance,
        key_in,
        value_in,
        learn_in,
        decay_in,
        decay_base.reshape(1, channels),
        norm_gain.reshape(1, channels),
        out_weight,
        route_ids.T,
        route_weights.T,
    )
    return product, new_state, late, routing


def expert_kernel(
    got_ref, gain_ref, gate_ref, up_ref, down_ref, late_ref, state_ref, out_ref, new_state_ref, flat, stored
):
    f32 = jnp.float32
    store = pltpu.make_async_copy(
        late_ref, new_state_ref.at[pl.ds(SEQ_STEP, SEQ_STEP)], stored
    )
    store.start()
    senders, n_y, rows, quarter = got_ref.shape
    power = jnp.zeros((senders * rows, 128), f32)
    for y in range(n_y):
        flat[:, y * quarter : (y + 1) * quarter] = got_ref[:, y].reshape(senders * rows, quarter)
        for first in range(y * quarter, (y + 1) * quarter, 128):
            at = slice(first, first + 128)
            original = flat[:, at].astype(f32) * (1.0 / gain_ref[:, at])
            power += original * original
    mean = jnp.sum(power, axis=1, keepdims=True) * (1.0 / (n_y * quarter))
    scale = lax.rsqrt(mean + EPSILON)
    units = gate_ref.shape[2]
    weights = jnp.concatenate([gate_ref[0], up_ref[0]], axis=1)
    half = senders * rows // 2
    hidden = []
    for first in (0, half):
        both = jnp.dot(flat[first : first + half], weights, preferred_element_type=f32)
        both = both * scale[first : first + half]
        gate, upward = both[:, :units], both[:, units:]
        hidden.append((gate * jax.nn.sigmoid(gate) * upward).astype(jnp.bfloat16))
    hidden = jnp.concatenate(hidden, axis=0)
    for y in range(n_y):
        partial = jnp.dot(
            hidden, down_ref[0, :, y * quarter : (y + 1) * quarter], preferred_element_type=f32
        )
        out_ref[:, y] = partial.astype(jnp.bfloat16).reshape(senders, rows, quarter)
    store.wait()


def experts(got, routed_gain, expert_gate, expert_up, expert_down, late, new_state):
    senders, n_y, rows, quarter = got.shape
    vmem = pl.BlockSpec(memory_space=pltpu.VMEM)
    return pl.pallas_call(
        expert_kernel,
        in_specs=[vmem] * 6 + [pl.BlockSpec(memory_space=pl.ANY)],
        out_specs=[vmem, pl.BlockSpec(memory_space=pl.ANY)],
        out_shape=[
            jax.ShapeDtypeStruct(got.shape, jnp.bfloat16),
            jax.ShapeDtypeStruct(new_state.shape, new_state.dtype),
        ],
        input_output_aliases={6: 1},
        scratch_shapes=[
            pltpu.VMEM((senders * rows, n_y * quarter), jnp.bfloat16),
            pltpu.SemaphoreType.DMA,
        ],
        compiler_params=pltpu.CompilerParams(vmem_limit_bytes=12 << 20),
        cost_estimate=pl.CostEstimate(flops=400_000_000, bytes_accessed=4_000_000, transcendentals=40_000),
    )(got, routed_gain.reshape(1, n_y * quarter), expert_gate, expert_up, expert_down, late, new_state)


def pack_kernel(
    arrived_ref, hidden_ref, gain_ref, routing_ref, parcels_ref, own_ref
):
    f32, bf16 = jnp.float32, jnp.bfloat16
    seqs, quarter = own_ref.shape
    at = pl.ds(pl.multiple_of(lax.axis_index("y") * quarter, quarter), quarter)
    attention = jnp.sum(arrived_ref[...].astype(f32), axis=0).astype(bf16)
    residual = hidden_ref[:, at].astype(f32) + attention.astype(f32)
    own_ref[...] = residual
    gained = (residual * gain_ref[:, at]).astype(bf16)

    chunks = quarter // 128
    for z in range(parcels_ref.shape[0]):
        for chunk in range(chunks):
            parcels_ref[z, chunk * seqs : (chunk + 1) * seqs, :] = gained[
                :, chunk * 128 : (chunk + 1) * 128
            ]
        parcels_ref[z, chunks * seqs : chunks * seqs + 8, :] = routing_ref[...]


def pack(arrived, hidden_in, routed_gain, routing, n_z):
    n_y, seqs, quarter = arrived.shape
    width = n_y * quarter
    vmem = pl.BlockSpec(memory_space=pltpu.VMEM)
    return pl.pallas_call(
        pack_kernel,
        in_specs=[vmem] * 4,
        out_specs=[vmem] * 2,
        out_shape=[
            jax.ShapeDtypeStruct((n_z, quarter // 128 * seqs + 8, 128), jnp.bfloat16),
            jax.ShapeDtypeStruct((seqs, quarter), jnp.float32),
        ],
        compiler_params=pltpu.CompilerParams(vmem_limit_bytes=8 << 20),
    )(arrived, hidden_in, routed_gain.reshape(1, width), routing)


def choose_kernel(top, slots, rows_ref, chosen_ref, place_ref, weight_ref, flat, choice):
    f32, bf16 = jnp.float32, jnp.bfloat16
    n_z = rows_ref.shape[0]
    seqs = flat.shape[0] // n_z
    near, n_y, per_expert, piece = chosen_ref.shape
    tokens = n_z * seqs
    chunks = piece // 128
    sender_of = lax.broadcasted_iota(jnp.int32, (8, 128), 1) // seqs
    groups = tokens // 128
    per_group = 128 // seqs
    spread = [[jnp.zeros((8, 128), f32) for _ in range(groups)] for _ in range(4)]
    for z in range(n_z):
        for chunk in range(chunks):
            flat[z * seqs : (z + 1) * seqs, chunk * 128 : (chunk + 1) * 128] = rows_ref[
                z, chunk * seqs : (chunk + 1) * seqs, :
            ]
        routing = rows_ref[z, chunks * seqs : chunks * seqs + 8, :].astype(f32)
        group, place = divmod(z, per_group)
        for which in range(4):
            turn = (place - which) * seqs % 128
            moved = routing if turn == 0 else pltpu.roll(routing, turn, 1)
            spread[which][group] = jnp.where(sender_of == place, moved, spread[which][group])
    ids, high, middle, low = [jnp.concatenate(part, axis=1) for part in spread]
    weights = high + middle + low
    named = (
        lax.axis_index("zq") * near + lax.broadcasted_iota(jnp.int32, (near, tokens), 0)
    ).astype(f32)
    sender = (lax.broadcasted_iota(jnp.int32, (near, tokens), 1) // seqs * slots).astype(f32)
    place = jnp.full((near, tokens), -1.0, f32)
    weight = jnp.zeros((near, tokens), f32)
    for k in range(top):
        for slot in range(slots):
            hit = named + 128.0 * slot == ids[k : k + 1, :]
            place = jnp.where(hit, sender + slot, place)
            weight = jnp.where(hit, weights[k : k + 1, :], weight)
    place_ref[...] = place
    weight_ref[...] = weight
    row = lax.broadcasted_iota(jnp.int32, (per_expert, tokens), 0).astype(f32)
    for expert in range(near):
        choice[expert * per_expert : (expert + 1) * per_expert, :] = jnp.where(
            row == place[expert : expert + 1, :], 1.0, 0.0
        ).astype(bf16)
    chosen = jnp.dot(choice[...], flat[...], preferred_element_type=f32).astype(bf16)
    chosen = chosen.reshape(near, per_expert, piece)
    for y in range(n_y):
        chosen_ref[:, y] = chosen


def choose(rows, near, n_y, slots, top, seqs):
    n_z, depth, _ = rows.shape
    piece = (depth - 8) // seqs * 128
    tokens = n_z * seqs
    vmem = pl.BlockSpec(memory_space=pltpu.VMEM)
    return pl.pallas_call(
        functools.partial(choose_kernel, top, slots),
        in_specs=[vmem],
        out_specs=[vmem] * 3,
        out_shape=[
            jax.ShapeDtypeStruct((near, n_y, n_z * slots, piece), jnp.bfloat16),
            jax.ShapeDtypeStruct((near, tokens), jnp.float32),
            jax.ShapeDtypeStruct((near, tokens), jnp.float32),
        ],
        scratch_shapes=[
            pltpu.VMEM((tokens, piece), jnp.bfloat16),
            pltpu.VMEM((near * n_z * slots, tokens), jnp.bfloat16),
        ],
        compiler_params=pltpu.CompilerParams(vmem_limit_bytes=12 << 20),
    )(rows)


def combine_kernel(returned_ref, place_ref, weight_ref, out_ref, summed, choice):
    f32, bf16 = jnp.float32, jnp.bfloat16
    near, n_y, per_expert, piece = returned_ref.shape
    n_z, seqs, _ = out_ref.shape
    tokens = n_z * seqs
    total = near * per_expert
    row = lax.broadcasted_iota(jnp.int32, (per_expert, tokens), 0).astype(f32)
    for expert in range(near):
        at = slice(expert * per_expert, (expert + 1) * per_expert)
        result = jnp.sum(returned_ref[expert].astype(f32), axis=0).astype(bf16)
        summed[at, :] = result
        summed[total + expert * per_expert : total + (expert + 1) * per_expert, :] = result
        weight = jnp.where(
            row == place_ref[expert : expert + 1, :], weight_ref[expert : expert + 1, :], 0.0
        )
        high = weight.astype(bf16)
        choice[at, :] = high
        choice[total + expert * per_expert : total + (expert + 1) * per_expert, :] = (
            weight - high.astype(f32)
        ).astype(bf16)
    combined = lax.dot_general(
        choice[...], summed[...], (((0,), (0,)), ((), ())), preferred_element_type=f32
    )
    out_ref[...] = combined.astype(bf16).reshape(n_z, seqs, piece)


def combine(returned, place, weight, n_z):
    near, n_y, per_expert, piece = returned.shape
    tokens = place.shape[1]
    vmem = pl.BlockSpec(memory_space=pltpu.VMEM)
    return pl.pallas_call(
        combine_kernel,
        in_specs=[vmem] * 3,
        out_specs=vmem,
        out_shape=jax.ShapeDtypeStruct((n_z, tokens // n_z, piece), jnp.bfloat16),
        scratch_shapes=[
            pltpu.VMEM((2 * near * per_expert, piece), jnp.bfloat16),
            pltpu.VMEM((2 * near * per_expert, tokens), jnp.bfloat16),
        ],
        compiler_params=pltpu.CompilerParams(vmem_limit_bytes=12 << 20),
    )(returned, place, weight)


def on_device(
    hidden_in,
    state_in,
    receptance,
    key_in,
    value_in,
    learn_in,
    decay_in,
    decay_base,
    norm_gain,
    out_weight,
    routed_gain,
    expert_gate,
    expert_up,
    expert_down,
    route_ids,
    route_weights,
):
    n_y, n_zq = lax.axis_size("y"), lax.axis_size("zq")
    near = lax.axis_size(("zp", "x", "c"))
    seqs, width = hidden_in.shape
    quarter = width // n_y
    per_expert = n_zq * SLOTS

    product, new_state, late, routing = heads_update(
        n_y, state_in, receptance, key_in, value_in, learn_in, decay_in, decay_base, norm_gain, out_weight,
        route_ids, route_weights,
    )
    arrived = exchange(product, "y")
    parcels, own_residual = pack(arrived, hidden_in, routed_gain, routing, n_zq)
    rows = exchange(parcels, "zq")
    chosen, place, weight = choose(rows, near, n_y, SLOTS, route_ids.shape[1], seqs)
    got = exchange(chosen.reshape(near * n_y, per_expert, quarter), NEAR_AXES)
    got = got.reshape(near, n_y, per_expert, quarter)
    back, new_state = experts(got, routed_gain, expert_gate, expert_up, expert_down, late, new_state)
    returned = exchange(back.reshape(near * n_y, per_expert, quarter), NEAR_AXES)
    combined = combine(returned.reshape(near, n_y, per_expert, quarter), place, weight, n_zq)
    routed = exchange(combined, "zq").astype(jnp.float32).sum(axis=0)
    result = (own_residual + routed).astype(jnp.bfloat16)
    spread = exchange(jnp.broadcast_to(result, (n_y, seqs, quarter)), "y")
    return (spread.transpose(1, 0, 2).reshape(seqs, width), new_state)


def solution(mesh):
    near_mesh = Mesh(mesh.devices.reshape(8, 2, 4, 2, 4), ("zq", "zp", "x", "c", "y"))
    in_specs = (
        P(EP, None),
        P(EP, "y", None, None),
        P(EP, "y"),
        P(EP, "y"),
        P(EP, "y"),
        P(EP, "y"),
        P(EP, "y"),
        P("y"),
        P("y"),
        P("y", None),
        P(),
        P(EP, None, "y"),
        P(EP, None, "y"),
        P(EP, "y", None),
        P(EP, None),
        P(EP, None),
    )
    out_specs = (P(EP, None), P(EP, "y", None, None))
    return jax.shard_map(
        on_device, mesh=near_mesh, in_specs=in_specs, out_specs=out_specs, check_vma=False
    )
```
